32 devices in a mesh: sp: 4 (over z), tp: 4 (over y, x), dp: 2 (over core).
Axes of the slice: x: 2, y: 2, z: 4, core: 2. Of those that a mesh axis runs over, the one named last changes fastest.
Arguments:
- latent_tokens: bfloat16 [4096, 2048], P(('dp', 'sp', 'tp')), parts along dimension 0, may hold values from -6 to 6
- condition: bfloat16 [4096], P(('dp', 'sp')), parts along dimension 0, may hold values from -6 to 6
- shift_weight: bfloat16 [2048, 2048], P('sp', 'tp'), may hold values from -0.125 to 0.125
- scale_weight: bfloat16 [2048, 2048], P('sp', 'tp'), may hold values from -0.125 to 0.125
- gate_weight: bfloat16 [2048, 2048], P('sp', 'tp'), may hold values from -0.125 to 0.125
- norm_gain: float32 [2048], replicated, may hold values from 0.1 to 1.9
- query_down: bfloat16 [2048, 512], replicated, may hold values from -0.125 to 0.125
- query_gain: float32 [512], replicated, may hold values from 0.1 to 1.9
- kv_down: bfloat16 [2048, 256], replicated, may hold values from -0.125 to 0.125
- kv_gain: float32 [256], replicated, may hold values from 0.1 to 1.9
- rope_down: bfloat16 [2048, 32], replicated, may hold values from -0.125 to 0.125
- query_up: bfloat16 [512, 1536], P(None, 'tp'), may hold values from -0.25 to 0.25
- key_up: bfloat16 [256, 1024], P(None, 'tp'), may hold values from -0.375 to 0.375
- value_up: bfloat16 [256, 1024], P(None, 'tp'), may hold values from -0.375 to 0.375
- query_norm_gain: float32 [96], replicated, may hold values from 0.47 to 16
- key_norm_gain: float32 [96], replicated, may hold values from 0.47 to 16
- out_weight: bfloat16 [1024, 2048], P('tp'), may hold values from -0.1875 to 0.1875
- context_latent: bfloat16 [2048, 256], P(('dp', 'sp')), parts along dimension 0, may hold values from -6 to 6
- context_rope: bfloat16 [2048, 32], P(('dp', 'sp')), parts along dimension 0, may hold values from -6 to 6
- context_lift: float32 [16], P('tp'), may hold values from 0 to 2
Outputs:
- output: bfloat16 [4096, 2048], P(('dp', 'sp', 'tp')), parts along dimension 0
The draws below stay inside these ranges and needn't reach their ends.
There are 2 independent parts, one for each index of `dp`. The reference program is written for one: setup_inputs(seed, part) draws one part's arguments, and reference() takes and returns one part's arrays. A program takes and returns all parts, laid end to end along the dimension named above; an argument that names none is the same for every part. Nothing has to cross between parts.
All inputs are finite; a program needn't handle non-finite values.
Results may differ from the reference program's by a relative error of at most 0.015.
The reference program's roundings to bfloat16 on the way count: a program that leaves them out, or rounds other values in their place, can miss the bound.
Values may be sent and summed in bfloat16 or wider, within the bound.
A program may use at most 128 MiB of HBM per device.

```python
import jax
import jax.numpy as jnp
from jax import lax

D_MODEL = 2048
HEADS = 16
NOPE_DIM = 64
ROPE_DIM = 32
VALUE_DIM = 64
QK_DIM = 96
Q_RANK = 512
KV_RANK = 256
GRID_W = 64
CONTEXT = 1024
TOKENS = 2048
N_TP = 4


def gain_draw(key, salt):
    own_key = jax.random.fold_in(key, salt)
    normal_values = jax.random.normal(own_key, (QK_DIM,), jnp.float32)
    return 1.7 * (1.0 + 0.18 * jnp.clip(normal_values, -4.0, 4.0))


def draw_query_norm_gain(key, part):
    return gain_draw(key, 31)


def draw_key_norm_gain(key, part):
    return gain_draw(key, 57)


def block_scale(rng, dims, cuts, least, top_value):
    loudness = 1.0
    for dim, shards_of in cuts:
        heights = jax.random.uniform(jax.random.fold_in(jax.random.fold_in(rng, 6), dim), (shards_of,), jnp.float32, least / len(cuts), top_value / len(cuts))
        loudness = loudness * jnp.repeat(jnp.exp(heights), dims[dim] // shards_of).reshape((-1,) + (1,) * (len(dims) - 1 - dim))
    return loudness


def bell_draw(key, shape, spread, bound, shards=(), kind=jnp.bfloat16):
    drawn = spread * jax.random.normal(key, shape, jnp.float32)
    if shards:
        drawn = drawn * block_scale(key, shape, shards, -0.22, 0.18)
    return jnp.clip(drawn, -bound, bound).astype(kind)


def setup_inputs(seed: int = 0, part: int = 0) -> dict:
    key_of = jax.random.split(jax.random.key(seed), 21)
    part_keys = jax.random.split(jax.random.fold_in(key_of[20], part), 21)
    latent_tokens = bell_draw(part_keys[0], (TOKENS, D_MODEL), 1.0, 6.0, ((0, 16),))
    condition = bell_draw(part_keys[1], (D_MODEL,), 1.0, 6.0, ((0, 4),))
    shift_weight = bell_draw(key_of[2], (D_MODEL, D_MODEL), D_MODEL ** -0.5, 0.125, ((0, 4), (1, 4)))
    scale_weight = bell_draw(key_of[3], (D_MODEL, D_MODEL), D_MODEL ** -0.5, 0.125, ((0, 4), (1, 4)))
    gate_weight = bell_draw(key_of[4], (D_MODEL, D_MODEL), D_MODEL ** -0.5, 0.125, ((0, 4), (1, 4)))
    norm_gain = jnp.clip(1.0 + 0.18 * jax.random.normal(key_of[5], (D_MODEL,), jnp.float32), 0.1, 1.9)
    query_down = bell_draw(key_of[6], (D_MODEL, Q_RANK), D_MODEL ** -0.5, 0.125)
    query_gain = jnp.clip(1.0 + 0.18 * jax.random.normal(key_of[7], (Q_RANK,), jnp.float32), 0.1, 1.9)
    kv_down = bell_draw(key_of[8], (D_MODEL, KV_RANK), D_MODEL ** -0.5, 0.125)
    kv_gain = jnp.clip(1.0 + 0.18 * jax.random.normal(key_of[9], (KV_RANK,), jnp.float32), 0.1, 1.9)
    rope_down = bell_draw(key_of[10], (D_MODEL, ROPE_DIM), D_MODEL ** -0.5, 0.125)
    query_up = bell_draw(key_of[11], (Q_RANK, HEADS * QK_DIM), Q_RANK ** -0.5, 0.25, ((1, 4),))
    key_up = bell_draw(key_of[12], (KV_RANK, HEADS * NOPE_DIM), KV_RANK ** -0.5, 0.375, ((1, 4),))
    value_up = bell_draw(key_of[13], (KV_RANK, HEADS * VALUE_DIM), KV_RANK ** -0.5, 0.375, ((1, 4),))
    query_norm_gain = draw_query_norm_gain(jax.random.fold_in(key_of[20], 71), part)
    key_norm_gain = draw_key_norm_gain(jax.random.fold_in(key_of[20], 71), part)
    out_weight = bell_draw(key_of[16], (HEADS * VALUE_DIM, D_MODEL), (HEADS * VALUE_DIM) ** -0.5, 0.1875, ((0, 4),))
    context_latent = bell_draw(part_keys[17], (CONTEXT, KV_RANK), 1.0, 6.0, ((0, 4),))
    context_rope = bell_draw(part_keys[18], (CONTEXT, ROPE_DIM), 1.0, 6.0, ((0, 4),))
    context_lift = jnp.clip(2.0 * jax.random.uniform(key_of[19], (HEADS,), jnp.float32) ** block_scale(key_of[19], (HEADS,), ((0, 4),), -0.2, 0.2), 0.0, 2.0)
    return {"latent_tokens": latent_tokens, "condition": condition, "shift_weight": shift_weight, "scale_weight": scale_weight, "gate_weight": gate_weight, "norm_gain": norm_gain, "query_down": query_down, "query_gain": query_gain, "kv_down": kv_down, "kv_gain": kv_gain, "rope_down": rope_down, "query_up": query_up, "key_up": key_up, "value_up": value_up, "query_norm_gain": query_norm_gain, "key_norm_gain": key_norm_gain, "out_weight": out_weight, "context_latent": context_latent, "context_rope": context_rope, "context_lift": context_lift}


EPS = 1e-06
THETA = 10000.0

def rms_scaled(values, gain_vector):
    mean_square = lax.optimization_barrier(jnp.mean(values * values, axis=-1, keepdims=True))
    return values * lax.rsqrt(mean_square + EPS) * gain_vector

def rotate(rope_part, positions):
    row_count = rope_part.shape[0]
    freq_count = ROPE_DIM // 4
    inverse = THETA ** (-4.0 * jnp.arange(freq_count, dtype=jnp.float32) / ROPE_DIM)
    grid_row = (positions // GRID_W).astype(jnp.float32)
    grid_col = (positions % GRID_W).astype(jnp.float32)
    angles = jnp.stack([grid_row[:, None] * inverse, grid_col[:, None] * inverse], axis=1)
    cosine_table = jnp.cos(angles)[:, None]
    sine_table = jnp.sin(angles)[:, None]
    split_rows = rope_part.reshape(row_count, rope_part.shape[1], 2, 2, freq_count)
    first_half = split_rows[:, :, :, 0]
    second_half = split_rows[:, :, :, 1]
    turned = jnp.stack([first_half * cosine_table - second_half * sine_table, second_half * cosine_table + first_half * sine_table], axis=3)
    return turned.reshape(rope_part.shape)

def expand(latent_rows, rope_rows, key_up, value_up, key_norm_gain):
    row_count = latent_rows.shape[0]
    nope_part = jnp.dot(latent_rows, key_up, preferred_element_type=jnp.float32).reshape(row_count, HEADS, NOPE_DIM)
    value_rows = jnp.dot(latent_rows, value_up, preferred_element_type=jnp.float32).astype(jnp.bfloat16)
    shared = jnp.broadcast_to(rope_rows.astype(jnp.float32)[:, None, :], (row_count, HEADS, ROPE_DIM))
    normal_keys = rms_scaled(jnp.concatenate([nope_part, shared], axis=-1), key_norm_gain)
    return (normal_keys, value_rows.reshape(row_count, HEADS, VALUE_DIM))

def reference(latent_tokens, condition, shift_weight, scale_weight, gate_weight, norm_gain, query_down, query_gain, kv_down, kv_gain, rope_down, query_up, key_up, value_up, query_norm_gain, key_norm_gain, out_weight, context_latent, context_rope, context_lift):
    activated = jax.nn.silu(condition.astype(jnp.float32)).astype(jnp.bfloat16)[None]
    mod_shift = jnp.dot(activated, shift_weight, preferred_element_type=jnp.float32)[0]
    mod_scale = jnp.dot(activated, scale_weight, preferred_element_type=jnp.float32)[0]
    mod_gate = jnp.dot(activated, gate_weight, preferred_element_type=jnp.float32)[0]
    token_values = latent_tokens.astype(jnp.float32)
    normed = (rms_scaled(token_values, norm_gain) * (1.0 + mod_scale) + mod_shift).astype(jnp.bfloat16)
    query_latent = rms_scaled(jnp.dot(normed, query_down, preferred_element_type=jnp.float32), query_gain).astype(jnp.bfloat16)
    key_latent = rms_scaled(jnp.dot(normed, kv_down, preferred_element_type=jnp.float32), kv_gain).astype(jnp.bfloat16)
    rope_key = jnp.dot(normed, rope_down, preferred_element_type=jnp.float32).astype(jnp.bfloat16)
    positions = jnp.arange(TOKENS, dtype=jnp.int32)
    query_heads = rms_scaled(jnp.dot(query_latent, query_up, preferred_element_type=jnp.float32).reshape(TOKENS, HEADS, QK_DIM), query_norm_gain)
    queries = jnp.concatenate([query_heads[..., :NOPE_DIM], rotate(query_heads[..., NOPE_DIM:], positions)], axis=-1).astype(jnp.bfloat16)
    latent_normal, latent_values = expand(key_latent, rope_key, key_up, value_up, key_norm_gain)
    latent_keys = jnp.concatenate([latent_normal[..., :NOPE_DIM], rotate(latent_normal[..., NOPE_DIM:], positions)], axis=-1).astype(jnp.bfloat16)
    context_normal, context_values = expand(context_latent, context_rope, key_up, value_up, key_norm_gain)
    context_keys = context_normal.astype(jnp.bfloat16)
    all_keys = jnp.concatenate([latent_keys, context_keys], axis=0)
    all_values = jnp.concatenate([latent_values, context_values], axis=0)
    is_context = jnp.arange(TOKENS + CONTEXT, dtype=jnp.int32) >= TOKENS

    def one_head(inputs):
        query_head, key_head, value_head, lift_head = inputs
        scores = jnp.dot(query_head, key_head.T, preferred_element_type=jnp.float32) * QK_DIM ** (-0.5)
        scores = scores + jnp.where(is_context, lift_head, jnp.zeros((), jnp.float32))[None, :]
        top_score = lax.optimization_barrier(jnp.max(scores, axis=-1, keepdims=True))
        weights = jnp.exp(scores - top_score)
        weight_total = lax.optimization_barrier(jnp.sum(weights, axis=-1, keepdims=True))
        summed = jnp.dot(weights.astype(jnp.bfloat16), value_head, preferred_element_type=jnp.float32)
        return (summed / weight_total).astype(jnp.bfloat16)
    attended = lax.map(one_head, (jnp.transpose(queries, (1, 0, 2)), jnp.transpose(all_keys, (1, 0, 2)), jnp.transpose(all_values, (1, 0, 2)), context_lift))
    attended = jnp.transpose(attended, (1, 0, 2)).reshape(TOKENS, HEADS * VALUE_DIM)
    group_width = HEADS // N_TP * VALUE_DIM
    mixed_sum = jnp.zeros((TOKENS, D_MODEL), jnp.float32)
    for head_group in range(N_TP):
        group_term = jnp.dot(attended[:, head_group * group_width:(head_group + 1) * group_width], out_weight[head_group * group_width:(head_group + 1) * group_width], preferred_element_type=jnp.float32)
        rounded = lax.optimization_barrier(group_term.astype(jnp.bfloat16))
        mixed_sum = mixed_sum + rounded.astype(jnp.float32)
    return (token_values + mod_gate * mixed_sum).astype(jnp.bfloat16)
```

```python
import functools

import jax
import jax.numpy as jnp
import numpy as np
from jax import lax
from jax.experimental import pallas as pl
from jax.experimental.pallas import tpu as pltpu
from jax.sharding import PartitionSpec as P

NOPE_DIM = 64
ROPE_DIM = 32
VALUE_DIM = 64
QK_DIM = 96
GRID_W = 64
LANES = 128

EPS = 1e-06
THETA = 10000.0
LOG2E = 1.4426950408889634
MESH = pl.DeviceIdType.MESH
VMEM_SPEC = pl.BlockSpec(memory_space=pltpu.VMEM)
ANY_SPEC = pl.BlockSpec(memory_space=pl.ANY)
BF16 = jnp.bfloat16
F32 = jnp.float32


def partner_order():
    return np.arange(ROPE_DIM) ^ (ROPE_DIM // 4)


def rope_spread():
    spread = np.zeros((ROPE_DIM, LANES), np.float32)
    order = partner_order()
    for j in range(ROPE_DIM):
        spread[j, NOPE_DIM + j] = 1.0
        spread[order[j], QK_DIM + j] = 1.0
    return spread


def query_spread(heads):
    spread = np.zeros((heads * QK_DIM, heads * LANES), np.float32)
    order = partner_order()
    for h in range(heads):
        for j in range(QK_DIM):
            spread[h * QK_DIM + j, h * LANES + j] = 1.0
        for j in range(ROPE_DIM):
            spread[h * QK_DIM + NOPE_DIM + order[j], h * LANES + QK_DIM + j] = 1.0
    return spread


def head_spread(heads, width):
    spread = np.zeros((heads * width, heads * LANES), np.float32)
    for h in range(heads):
        for j in range(width):
            spread[h * width + j, h * LANES + j] = 1.0
    return spread


def turn_tables(count, axis):
    freq_count = ROPE_DIM // 4
    inverse = np.float32(THETA) ** (-np.float32(4.0) * np.arange(freq_count, dtype=np.float32) / np.float32(ROPE_DIM))
    angles = np.arange(count, dtype=np.float32)[:, None] * inverse.astype(np.float32)
    cosine = np.zeros((count, LANES), np.float32)
    sine = np.zeros((count, LANES), np.float32)
    start = NOPE_DIM + axis * 2 * freq_count
    mid = start + freq_count
    cosine[:, start:mid] = np.cos(angles.astype(np.float64))
    cosine[:, mid : mid + freq_count] = np.cos(angles.astype(np.float64))
    sine[:, start:mid] = -np.sin(angles.astype(np.float64))
    sine[:, mid : mid + freq_count] = np.sin(angles.astype(np.float64))
    if axis == 0:
        cosine[:, :NOPE_DIM] = 1.0
    return cosine, sine


def norm_factor(values):
    return lax.rsqrt(jnp.mean(values * values, axis=-1, keepdims=True) + EPS)


def partner(tp, index, d):
    if tp & (tp - 1):
        return lax.rem(index + d, tp)
    result = 0 * index
    bit = 1
    while bit < tp:
        here = lax.rem(index // bit, 2)
        result = result + bit * (lax.rem(here + 1, 2) if d & bit else here)
        bit *= 2
    return result


def fused_kernel(
    sp, tp, dp, heads,
    cond_ref, gain_ref, qg_ref, kg_ref, qgain_ref, kgain_ref, lift_ref, row_a, row_b, col_a, col_b, spread_ref,
    shift_hbm, scale_hbm, gate_hbm, tokens_hbm, qd_hbm, kd_hbm, rd_hbm, cl_hbm, cr_hbm,
    qu_hbm, ku_hbm, vu_hbm, qe_hbm, ke_hbm, ve_hbm, w_hbm,
    out_ref,
    mods, q_lat, kv, ctx, ctx_rope, gate_buf, tab_a, tab_b, gains, q_all, k_buf, v_buf, k_ctx, v_ctx, top_ref, acc_ref, att, held,
    w_all, shift_w, scale_w, gate_w, tokens_ref, qd_ref, kd_ref, rd_ref,
    qu_raw, ku_raw, vu_raw, qe_ref, ke_ref, ve_ref, qu_ref, ku_ref, vu_ref,
    load_sem, mod_send, mod_recv, q_send, q_recv, kv_send, kv_recv, c_send, c_recv, w_send, w_recv,
    x_send, x_recv, a_send, a_recv,
):
    s_me = lax.axis_index("sp")
    t_me = lax.axis_index("tp")
    d_me = lax.axis_index("dp")
    me = s_me * tp + t_me
    half = mods.shape[2]
    rows = tokens_ref.shape[0]
    rank = ku_raw.shape[0]
    group = tp * rows
    ctx_rows = cl_hbm.shape[0]
    share = w_hbm.shape[0] // dp
    width = w_hbm.shape[1]
    pieces = rank // rows

    def load(i, src, dst):
        cp = pltpu.make_async_copy(src, dst, load_sem.at[i])
        cp.start()
        return cp

    first = [
        load(i, src, dst)
        for i, (src, dst) in enumerate(((shift_hbm, shift_w), (scale_hbm, scale_w), (gate_hbm, gate_w)))
    ]
    ctx_load = [
        load(3, cl_hbm, ctx.at[0]),
        load(4, cr_hbm, ctx_rope.at[0]),
    ]
    w_load = load(5, w_hbm, w_all.at[0])
    token_load = load(6, tokens_hbm, tokens_ref)
    down_load = [load(7, qd_hbm, qd_ref), load(8, kd_hbm, kd_ref), load(9, rd_hbm, rd_ref)]
    up_load = [
        load(10 + i, src, dst)
        for i, (src, dst) in enumerate((
            (qu_hbm, qu_raw), (ku_hbm, ku_raw), (vu_hbm, vu_raw), (qe_hbm, qe_ref), (ke_hbm, ke_ref), (ve_hbm, ve_ref),
        ))
    ]

    def peer(ds, dt):
        return {"sp": lax.rem(s_me + ds, sp), "tp": lax.rem(t_me + dt, tp)}

    def column(ds):
        return {"sp": lax.rem(s_me + ds, sp)}

    def mate(d):
        return {"tp": partner(tp, t_me, d)}

    def twin(e):
        return {"dp": lax.rem(d_me + e, dp)}

    def remote(src, dst, send, recv, device):
        return pltpu.make_async_remote_copy(
            src_ref=src, dst_ref=dst, send_sem=send, recv_sem=recv, device_id=device, device_id_type=MESH
        )

    others = [(ds, dt) for ds in range(sp) for dt in range(tp) if ds or dt]
    barrier = pltpu.get_barrier_semaphore()
    for ds, dt in others:
        pl.semaphore_signal(barrier, inc=1, device_id=peer(ds, dt), device_id_type=MESH)
    for e in range(1, dp):
        pl.semaphore_signal(barrier, inc=1, device_id=twin(e), device_id_type=MESH)

    with jax.named_scope("modmm"):
        c = cond_ref[...].astype(F32)
        act = (c / (1.0 + jnp.exp(-c))).astype(BF16)
        act = jnp.broadcast_to(act, (16, act.shape[1]))
        terms = []
        for i, w in enumerate((shift_w, scale_w, gate_w)):
            first[i].wait()
            term = jnp.dot(act, w[...], preferred_element_type=F32)[0:1]
            terms += [term[:, :half], term[:, half:]]
        mods[me] = jnp.concatenate(terms + [terms[0], terms[0]], axis=0)
        for cp in ctx_load:
            cp.wait()
        w_load.wait()

    with jax.named_scope("barrier"):
        pl.semaphore_wait(barrier, len(others) + dp - 1)
    mod_copies = []
    for i, (ds, dt) in enumerate(others):
        mod_copies.append(remote(mods.at[me], mods.at[me], mod_send.at[i], mod_recv.at[i], peer(ds, dt)))
        mod_copies[-1].start()
    ctx_copies = []
    for ds in range(1, sp):
        for k, buf in enumerate((ctx, ctx_rope)):
            i = 2 * ds - 2 + k
            ctx_copies.append(remote(buf.at[0], buf.at[ds], c_send.at[i], c_recv.at[i], column(ds)))
            ctx_copies[-1].start()

    cut = share // 2
    my_start = pl.multiple_of(d_me * share, share)

    def w_copy(d, part):
        span = pl.ds(pl.multiple_of(my_start + part * cut, cut), cut)
        i = (d - 1) * 2 + part
        return remote(w_all.at[0, span], w_all.at[d, span], w_send.at[i], w_recv.at[i], mate(d))

    early = [(d, 0) for d in range(1, tp - 1)]
    late = [(d, part) for d in range(1, tp) for part in range(2) if (d, part) not in early]
    for d, part in early:
        w_copy(d, part).start()

    with jax.named_scope("prep"):
        gains[...] = jnp.zeros(gains.shape, F32)
        gains[0:1, :QK_DIM] = qgain_ref[...]
        gains[1:2, :QK_DIM] = kgain_ref[...]
        lane = lax.broadcasted_iota(jnp.int32, (1, LANES), 1)
        freq = ROPE_DIM // 4
        low = lax.rem(lane, 2 * freq) < freq
        live = lane < QK_DIM
        ones_lane = jnp.where(lane == VALUE_DIM, 1.0, 0.0).astype(F32)
        qgain = gains[0:1, :]
        kgain = gains[1:2, :]

        def swap(g):
            return jnp.where(low, pltpu.roll(g, LANES - freq, 1), pltpu.roll(g, freq, 1))

        qgain_swap = swap(qgain)
        kgain_swap = swap(kgain)

        def fill_tables(r, carry):
            span = pl.ds(pl.multiple_of(r * GRID_W, GRID_W), GRID_W)
            tab_a[span, :] = row_a[pl.ds(r, 1), :] + col_a[...]
            tab_b[span, :] = row_b[pl.ds(r, 1), :] + col_b[...]
            return carry

        lax.fori_loop(0, tab_a.shape[0] // GRID_W, fill_tables, 0)
        for cp in up_load:
            cp.wait()
        factor = LOG2E * QK_DIM ** (-0.5)
        qu_ref[...] = jnp.dot(qu_raw[...], qe_ref[...], preferred_element_type=F32).astype(BF16)
        ku_ref[...] = jnp.dot(ku_raw[...], ke_ref[...], preferred_element_type=F32).astype(BF16)
        vu_ref[...] = jnp.dot(vu_raw[...], ve_ref[...], preferred_element_type=F32).astype(BF16)
        spread = spread_ref[...]
        token_load.wait()
        for cp in down_load:
            cp.wait()
        x = tokens_ref[...].astype(F32)
        xn = x * norm_factor(x) * gain_ref[...]

    with jax.named_scope("waitmods"):
        for cp in mod_copies:
            cp.wait_recv()
    with jax.named_scope("stageB"):
        parts = [[], [], []]
        for t in range(tp):
            total = mods[t]
            for s in range(1, sp):
                total = total + mods[s * tp + t]
            for k in range(3):
                parts[k] += [total[2 * k : 2 * k + 1], total[2 * k + 1 : 2 * k + 2]]
        shift, scale, gate = [jnp.concatenate(p, axis=1) for p in parts]
        gate_buf[...] = gate
        normed = (xn * (1.0 + scale) + shift).astype(BF16)
        q = jnp.dot(normed, qd_ref[...], preferred_element_type=F32)
        q_lat[0] = (q * norm_factor(q) * qg_ref[...]).astype(BF16)
        lat = jnp.dot(normed, kd_ref[...], preferred_element_type=F32)
        kv[0, 0, :rows, :] = (lat * norm_factor(lat) * kg_ref[...]).astype(BF16)
        rope = lax.dot_general(
            rd_ref[...], normed, (((1,), (1,)), ((), ())), preferred_element_type=F32
        ).astype(BF16)
        piece = ROPE_DIM // pieces
        for p in range(pieces):
            kv[0, 0, rows:, p * rows : (p + 1) * rows] = rope[p * piece : (p + 1) * piece]

    def q_copy(d):
        return remote(q_lat.at[0], q_lat.at[d], q_send.at[d - 1], q_recv.at[d - 1], mate(d))

    def kv_column(ds):
        return remote(kv.at[0, 0], kv.at[ds, 0], kv_send.at[ds, 0], kv_recv.at[ds, 0], column(ds))

    def kv_mate(ds, d):
        return remote(kv.at[ds, 0], kv.at[ds, d], kv_send.at[ds, d], kv_recv.at[ds, d], mate(d))

    for d in range(1, tp):
        q_copy(d).start()
    for ds in range(1, sp):
        kv_column(ds).start()
    for d in range(1, tp):
        kv_mate(0, d).start()

    contract = (((1,), (1,)), ((), ()))

    def expand(lat, rope_t, a, b, store):
        rope = lax.dot_general(rope_t, spread, (((0,), (0,)), ((), ())), preferred_element_type=F32)
        rope_square = jnp.sum(jnp.where(live, rope * rope, 0.0), axis=-1, keepdims=True)
        turned = rope * a if b is None else rope * a + pltpu.roll(rope, QK_DIM, 1) * b
        k = jnp.dot(lat, ku_ref[...], preferred_element_type=F32)
        v = jnp.dot(lat, vu_ref[...], preferred_element_type=F32)
        for h in range(heads):
            cols = slice(h * LANES, (h + 1) * LANES)
            kh = k[:, cols]
            square = jnp.sum(kh * kh, axis=-1, keepdims=True) + rope_square
            scale_h = lax.rsqrt(square * (1.0 / QK_DIM) + EPS)
            store(h, ((kh * kgain + turned) * scale_h).astype(BF16), (v[:, cols] + ones_lane).astype(BF16))

    def attend(start, count, keys, values, h, lift, fresh):
        span = pl.ds(start, count)
        s = lax.dot_general(q_all[h, span, :], keys, contract, preferred_element_type=F32)
        peak = jnp.max(s, axis=-1, keepdims=True)
        if lift is not None:
            peak = peak + lift
        if fresh:
            top = jnp.broadcast_to(peak, (count, LANES))
        else:
            old = top_ref[h, span, :]
            top = jnp.maximum(old, peak)
        top_ref[h, span, :] = top
        floor = top if lift is None else top - lift
        p = jnp.exp2(s - jnp.concatenate([floor] * (keys.shape[0] // LANES), axis=1)).astype(BF16)
        add = jnp.dot(p, values, preferred_element_type=F32)
        if not fresh:
            add = acc_ref[h, span, :] * jnp.exp2(old - top) + add
        acc_ref[h, span, :] = add

    with jax.named_scope("ctxwait"):
        for cp in ctx_copies:
            cp.wait_recv()
    with jax.named_scope("ctxexpand"):
        def context_block(i, carry):
            lat = ctx[i]
            rope_t = ctx_rope[i]

            def store(h, k, v):
                span = pl.ds(pl.multiple_of(i * ctx_rows, ctx_rows), ctx_rows)
                k_ctx[h, span, :] = k
                v_ctx[h, span, :] = v

            expand(lat, rope_t, kgain, None, store)
            return carry

        lax.fori_loop(0, sp, context_block, 0)

    for d in range(tp):
        slot = (tp - 1 - d) * rows
        with jax.named_scope("qwait"):
            if d:
                q_copy(d).wait_recv()
        with jax.named_scope("qctx"):
            start = pl.multiple_of((s_me * tp + (partner(tp, t_me, d) if d else t_me)) * rows, rows)
            a = tab_a[pl.ds(start, rows), :] * qgain
            b = tab_b[pl.ds(start, rows), :] * qgain_swap
            qx = jnp.dot(q_lat[d], qu_ref[...], preferred_element_type=F32)
            for h in range(heads):
                v = qx[:, h * LANES : (h + 1) * LANES]
                square = jnp.sum(jnp.where(live, v * v, 0.0), axis=-1, keepdims=True)
                scale_h = lax.rsqrt(square * (1.0 / QK_DIM) + EPS) * factor
                q_all[h, slot : slot + rows, :] = ((v * a + pltpu.roll(v, QK_DIM, 1) * b) * scale_h).astype(BF16)
            for h in range(heads):
                attend(slot, rows, k_ctx[h], v_ctx[h], h, lift_ref[h] * LOG2E, True)

    with jax.named_scope("zwait"):
        for ds in range(1, sp):
            kv_column(ds).wait_recv()
            for d in range(1, tp):
                kv_mate(ds, d).start()
    for d, part in late:
        w_copy(d, part).start()

    def x_copy(d, e):
        i = (d - 1) * (dp - 1) + e - 1
        span = pl.ds(my_start, share)
        return remote(w_all.at[d, span], w_all.at[d, span], x_send.at[i], x_recv.at[i], twin(e))

    q_rows = 2 * rows if tp % 2 == 0 else rows

    def group_step(i, carry):
        ds = lax.rem(lax.rem(i, 2) * ((i + 1) // 2) + lax.rem(i + 1, 2) * (sp - i // 2), sp)
        source = lax.rem(s_me + sp - ds, sp)
        with jax.named_scope("kvwait"):
            for d in range(1, tp):
                kv_mate(ds, d).wait_recv()
        with jax.named_scope("kvexpand"):
            for d in range(tp):
                start = pl.multiple_of((source * tp + (partner(tp, t_me, d) if d else t_me)) * rows, rows)
                a = tab_a[pl.ds(start, rows), :] * kgain
                b = tab_b[pl.ds(start, rows), :] * kgain_swap
                lat = kv[ds, d, pl.ds(0, rows), :]
                tail = kv[ds, d, pl.ds(rows, ROPE_DIM // pieces), :]
                rope_t = jnp.concatenate([tail[:, p * rows : (p + 1) * rows] for p in range(pieces)], axis=0)

                def store(h, k, v):
                    k_buf[h, d * rows : (d + 1) * rows, :] = k
                    v_buf[h, d * rows : (d + 1) * rows, :] = v

                expand(lat, rope_t, a, b, store)

        with jax.named_scope("attend"):

            def rows_step(j, inner):
                start = pl.multiple_of(j * q_rows, q_rows)
                for h in range(heads):
                    attend(start, q_rows, k_buf[h], v_buf[h], h, None, False)
                return inner

            lax.fori_loop(0, group // q_rows, rows_step, 0)

        @pl.when(i == sp - 2)
        def _():
            with jax.named_scope("wswap"):
                for d in range(1, tp):
                    for part in range(2):
                        w_copy(d, part).wait_recv()
                    for e in range(1, dp):
                        x_copy(d, e).start()

        return carry

    lax.fori_loop(0, sp, group_step, 0)

    def a_copy(d):
        return remote(att.at[d], held.at[d - 1], a_send.at[d - 1], a_recv.at[d - 1], mate(d))

    with jax.named_scope("finish"):
        for d in range(tp - 1, -1, -1):
            slot = (tp - 1 - d) * rows
            outs = []
            for h in range(heads):
                total = acc_ref[h, slot : slot + rows, :]
                outs.append((total[:, :VALUE_DIM] / total[:, VALUE_DIM : VALUE_DIM + 1]).astype(BF16))
            att[d] = jnp.concatenate(outs, axis=1)
            if d:
                a_copy(d).start()

    with jax.named_scope("tail"):
        chunk = 512
        spans = [slice(n * chunk, (n + 1) * chunk) for n in range(width // chunk)]
        mixed = [
            jnp.dot(att[0], w_all[0, :, cols], preferred_element_type=F32).astype(BF16).astype(F32) for cols in spans
        ]
        for d in range(1, tp):
            with jax.named_scope("xwait"):
                for e in range(1, dp):
                    x_copy(d, e).wait_recv()
            with jax.named_scope("await"):
                a_copy(d).wait_recv()
            for n, cols in enumerate(spans):
                term = jnp.dot(held[d - 1], w_all[d, :, cols], preferred_element_type=F32)
                mixed[n] = mixed[n] + term.astype(BF16).astype(F32)
        for n, cols in enumerate(spans):
            out_ref[:, cols] = (tokens_ref[:, cols].astype(F32) + gate_buf[:, cols] * mixed[n]).astype(BF16)

    with jax.named_scope("drain"):
        for cp in mod_copies + ctx_copies:
            cp.wait_send()
        for d in range(1, tp):
            q_copy(d).wait_send()
            a_copy(d).wait_send()
            for part in range(2):
                w_copy(d, part).wait_send()
            for e in range(1, dp):
                x_copy(d, e).wait_send()
            for ds in range(sp):
                kv_mate(ds, d).wait_send()
        for ds in range(1, sp):
            kv_column(ds).wait_send()


def local(
    sp, tp, dp,
    latent_tokens, condition, shift_weight, scale_weight, gate_weight, norm_gain,
    query_down, query_gain, kv_down, kv_gain, rope_down, query_up, key_up, value_up,
    query_norm_gain, key_norm_gain, out_weight, context_latent, context_rope, context_lift,
):
    rows, width = latent_tokens.shape
    q_rank = query_down.shape[1]
    rank = kv_down.shape[1]
    heads = query_up.shape[1] // QK_DIM
    ctx_rows = context_latent.shape[0]
    group = rows * tp
    tokens = group * sp
    context = sp * ctx_rows
    n_dev = sp * tp
    row_a, row_b = turn_tables(tokens // GRID_W, 0)
    col_a, col_b = turn_tables(GRID_W, 1)
    q_spread = jnp.asarray(query_spread(heads), BF16)
    k_spread = jnp.asarray(head_spread(heads, NOPE_DIM), BF16)
    v_spread = jnp.asarray(head_spread(heads, VALUE_DIM), BF16)
    dma = pltpu.SemaphoreType.DMA
    vmem = pltpu.VMEM
    return pl.pallas_call(
        functools.partial(fused_kernel, sp, tp, dp, heads),
        out_shape=jax.ShapeDtypeStruct((rows, width), BF16),
        in_specs=[VMEM_SPEC] * 6 + [pl.BlockSpec(memory_space=pltpu.SMEM)] + [VMEM_SPEC] * 5 + [ANY_SPEC] * 16,
        out_specs=VMEM_SPEC,
        scratch_shapes=[
            vmem((n_dev, 8, width // tp // 2), F32),
            vmem((tp, rows, q_rank), BF16),
            vmem((sp, tp, rows + ROPE_DIM * rows // rank, rank), BF16),
            vmem((sp, ctx_rows, rank), BF16),
            vmem((sp, ROPE_DIM, ctx_rows), BF16),
            vmem((1, width), F32),
            vmem((tokens, LANES), F32),
            vmem((tokens, LANES), F32),
            vmem((8, LANES), F32),
            vmem((heads, group, LANES), BF16),
            vmem((heads, group, LANES), BF16),
            vmem((heads, group, LANES), BF16),
            vmem((heads, context, LANES), BF16),
            vmem((heads, context, LANES), BF16),
            vmem((heads, group, LANES), F32),
            vmem((heads, group, LANES), F32),
            vmem((tp, rows, heads * VALUE_DIM), BF16),
            vmem((tp - 1, rows, heads * VALUE_DIM), BF16),
            vmem((tp,) + out_weight.shape, BF16),
            vmem(shift_weight.shape, BF16),
            vmem(scale_weight.shape, BF16),
            vmem(gate_weight.shape, BF16),
            vmem(latent_tokens.shape, BF16),
            vmem(query_down.shape, BF16),
            vmem(kv_down.shape, BF16),
            vmem(rope_down.shape[::-1], BF16),
            vmem(query_up.shape, BF16),
            vmem(key_up.shape, BF16),
            vmem(value_up.shape, BF16),
            vmem(q_spread.shape, BF16),
            vmem(k_spread.shape, BF16),
            vmem(v_spread.shape, BF16),
            vmem((q_rank, heads * LANES), BF16),
            vmem((rank, heads * LANES), BF16),
            vmem((rank, heads * LANES), BF16),
            dma((16,)),
            dma((n_dev - 1,)), dma((n_dev - 1,)),
            dma((tp - 1,)), dma((tp - 1,)),
            dma((sp, tp)), dma((sp, tp)),
            dma((2 * (sp - 1),)), dma((2 * (sp - 1),)),
            dma((2 * (tp - 1),)), dma((2 * (tp - 1),)),
            dma(((tp - 1) * (dp - 1),)), dma(((tp - 1) * (dp - 1),)),
            dma((tp - 1,)), dma((tp - 1,)),
        ],
        compiler_params=pltpu.CompilerParams(
            collective_id=0, has_side_effects=True, vmem_limit_bytes=60 * 1024 * 1024
        ),
        name="fused",
    )(
        condition[None], norm_gain[None], query_gain[None], kv_gain[None], query_norm_gain[None], key_norm_gain[None],
        context_lift, jnp.asarray(row_a), jnp.asarray(row_b), jnp.asarray(col_a), jnp.asarray(col_b),
        jnp.asarray(rope_spread(), BF16),
        shift_weight, scale_weight, gate_weight, latent_tokens, query_down, kv_down, rope_down.T,
        context_latent, context_rope.T, query_up, key_up, value_up, q_spread, k_spread, v_spread, out_weight,
    )


def solution(mesh):
    in_specs = (
        P(("dp", "sp", "tp"), None), P(("dp", "sp")), P("sp", "tp"), P("sp", "tp"), P("sp", "tp"),
        P(), P(), P(), P(), P(), P(), P(None, "tp"), P(None, "tp"), P(None, "tp"), P(), P(),
        P("tp", None), P(("dp", "sp"), None), P(("dp", "sp"), None), P("tp"),
    )
    out_specs = P(("dp", "sp", "tp"), None)
    body = functools.partial(local, mesh.shape["sp"], mesh.shape["tp"], mesh.shape["dp"])
    return jax.shard_map(body, mesh=mesh, in_specs=in_specs, out_specs=out_specs, check_vma=False)
```

```python
import functools

import jax
import jax.numpy as jnp
import numpy as np
from jax import lax
from jax.experimental import pallas as pl
from jax.experimental.pallas import tpu as pltpu
from jax.sharding import PartitionSpec as P

NOPE_DIM = 64
ROPE_DIM = 32
VALUE_DIM = 64
QK_DIM = 96
GRID_W = 64
LANES = 128

EPS = 1e-06
THETA = 10000.0
LOG2E = 1.4426950408889634
MESH = pl.DeviceIdType.MESH
VMEM_SPEC = pl.BlockSpec(memory_space=pltpu.VMEM)
HBM_SPEC = pl.BlockSpec(memory_space=pltpu.HBM)
BF16 = jnp.bfloat16
F32 = jnp.float32


def partner_order():
    return np.arange(ROPE_DIM) ^ (ROPE_DIM // 4)


def rope_spread():
    spread = np.zeros((ROPE_DIM, LANES), np.float32)
    order = partner_order()
    for j in range(ROPE_DIM):
        spread[j, NOPE_DIM + j] = 1.0
        spread[order[j], QK_DIM + j] = 1.0
    return spread


def query_spread(heads):
    spread = np.zeros((heads * QK_DIM, heads * LANES), np.float32)
    order = partner_order()
    for h in range(heads):
        for j in range(QK_DIM):
            spread[h * QK_DIM + j, h * LANES + j] = 1.0
        for j in range(ROPE_DIM):
            spread[h * QK_DIM + NOPE_DIM + order[j], h * LANES + QK_DIM + j] = 1.0
    return spread


def head_spread(heads, width):
    spread = np.zeros((heads * width, heads * LANES), np.float32)
    for h in range(heads):
        for j in range(width):
            spread[h * width + j, h * LANES + j] = 1.0
    return spread


def turn_tables(count, axis):
    freq_count = ROPE_DIM // 4
    inverse = np.float32(THETA) ** (-np.float32(4.0) * np.arange(freq_count, dtype=np.float32) / np.float32(ROPE_DIM))
    angles = np.arange(count, dtype=np.float32)[:, None] * inverse.astype(np.float32)
    cosine = np.zeros((count, LANES), np.float32)
    sine = np.zeros((count, LANES), np.float32)
    start = NOPE_DIM + axis * 2 * freq_count
    mid = start + freq_count
    cosine[:, start:mid] = np.cos(angles.astype(np.float64))
    cosine[:, mid : mid + freq_count] = np.cos(angles.astype(np.float64))
    sine[:, start:mid] = -np.sin(angles.astype(np.float64))
    sine[:, mid : mid + freq_count] = np.sin(angles.astype(np.float64))
    if axis == 0:
        cosine[:, :NOPE_DIM] = 1.0
    return cosine, sine


def norm_factor(values):
    return lax.rsqrt(jnp.mean(values * values, axis=-1, keepdims=True) + EPS)


def partner(tp, index, d):
    if tp & (tp - 1):
        return lax.rem(index + d, tp)
    result = 0 * index
    bit = 1
    while bit < tp:
        here = lax.rem(index // bit, 2)
        result = result + bit * (lax.rem(here + 1, 2) if d & bit else here)
        bit *= 2
    return result


def fused_kernel(
    sp, tp, dp, heads,
    cond_ref, gain_ref, qg_ref, kg_ref, qgain_ref, kgain_ref, lift_ref, row_a, row_b, col_a, col_b, spread_ref,
    shift_hbm, scale_hbm, gate_hbm, tokens_hbm, qd_hbm, kd_hbm, rd_hbm, cl_hbm, cr_hbm,
    qu_hbm, ku_hbm, vu_hbm, qe_hbm, ke_hbm, ve_hbm, w_hbm,
    out_ref,
    mods, gates, q_lat, kv, ctx, ctx_rope, gate_buf, tab_a, tab_b, gains, q_all, k_buf, v_buf, k_ctx, v_ctx, att, held,
    w_all, shift_w, scale_w, gate_w, tokens_ref, qd_ref, kd_ref, rd_ref,
    qu_raw, ku_raw, vu_raw, qe_ref, ke_ref, ve_ref, qu_ref, ku_ref, vu_ref,
    load_sem, mod_send, mod_recv, g_send, g_recv, q_send, q_recv, kv_send, kv_recv, c_send, c_recv, w_send, w_recv,
    z_send, z_recv, x_send, x_recv, a_send, a_recv, *state,
):
    top_refs, acc_refs = state[:heads], state[heads:]
    s_me = lax.axis_index("sp")
    t_me = lax.axis_index("tp")
    d_me = lax.axis_index("dp")
    me = s_me * tp + t_me
    rows = tokens_ref.shape[0]
    rank = ku_raw.shape[0]
    group = tp * rows
    ctx_rows = cl_hbm.shape[0]
    pair = 2 - sp % 2
    share = w_hbm.shape[0] // (pair * dp)
    width = w_hbm.shape[1]
    pieces = rank // rows

    def load(i, src, dst):
        cp = pltpu.make_async_copy(src, dst, load_sem.at[i])
        cp.start()
        return cp

    first = [
        load(i, src, dst)
        for i, (src, dst) in enumerate(((shift_hbm, shift_w), (scale_hbm, scale_w), (gate_hbm, gate_w)))
    ]
    ctx_load = [
        load(3, cl_hbm, ctx.at[0]),
        load(4, cr_hbm, ctx_rope.at[0]),
    ]
    w_load = load(5, w_hbm, w_all.at[0])
    token_load = load(6, tokens_hbm, tokens_ref)
    down_load = [load(7, qd_hbm, qd_ref), load(8, kd_hbm, kd_ref), load(9, rd_hbm, rd_ref)]
    up_load = [
        load(10 + i, src, dst)
        for i, (src, dst) in enumerate((
            (qu_hbm, qu_raw), (ku_hbm, ku_raw), (vu_hbm, vu_raw), (qe_hbm, qe_ref), (ke_hbm, ke_ref), (ve_hbm, ve_ref),
        ))
    ]

    def peer(ds, dt):
        return {"sp": lax.rem(s_me + ds, sp), "tp": lax.rem(t_me + dt, tp)}

    def column(ds):
        return {"sp": lax.rem(s_me + ds, sp)}

    def mate(d):
        return {"tp": partner(tp, t_me, d)}

    def twin(e):
        return {"dp": lax.rem(d_me + e, dp)}

    def remote(src, dst, send, recv, device):
        return pltpu.make_async_remote_copy(
            src_ref=src, dst_ref=dst, send_sem=send, recv_sem=recv, device_id=device, device_id_type=MESH
        )

    others = [(ds, dt) for ds in range(sp) for dt in range(tp) if ds or dt]
    barrier = pltpu.get_barrier_semaphore()
    for ds, dt in others:
        pl.semaphore_signal(barrier, inc=1, device_id=peer(ds, dt), device_id_type=MESH)
    for e in range(1, dp):
        pl.semaphore_signal(barrier, inc=1, device_id=twin(e), device_id_type=MESH)

    with jax.named_scope("modmm"):
        c = cond_ref[...].reshape(1, cond_ref.shape[0]).astype(F32)
        act = (c / (1.0 + jnp.exp(-c))).astype(BF16)
        act = jnp.broadcast_to(act, (16, act.shape[1]))
        terms = []
        for i, w in enumerate((shift_w, scale_w, gate_w)):
            first[i].wait()
            term = jnp.dot(act, w[...], preferred_element_type=F32)[0:1]
            terms.append([term[:, c : c + LANES] for c in range(0, term.shape[1], LANES)])
        mods[me] = jnp.concatenate(terms[0] + terms[1], axis=0)
        gates[me] = jnp.concatenate(terms[2], axis=0)
        for cp in ctx_load:
            cp.wait()
        w_load.wait()

    with jax.named_scope("barrier"):
        pl.semaphore_wait(barrier, len(others) + dp - 1)
    mod_copies = []
    for i, (ds, dt) in enumerate(others):
        mod_copies.append(remote(mods.at[me], mods.at[me], mod_send.at[i], mod_recv.at[i], peer(ds, dt)))
        mod_copies[-1].start()

    def gate_copy(i):
        return remote(gates.at[me], gates.at[me], g_send.at[i], g_recv.at[i], peer(*others[i]))

    def ctx_up(k):
        device = {"sp": lax.rem(s_me + 1, sp)}
        return [
            remote(buf.at[k - 1], buf.at[k], c_send.at[j, k - 1], c_recv.at[j, k], device)
            for j, buf in enumerate((ctx, ctx_rope))
        ]

    def ctx_down(k):
        device = {"sp": lax.rem(s_me + sp - 1, sp)}
        src = (sp - k + 1) % sp
        return [
            remote(buf.at[src], buf.at[sp - k], c_send.at[j, sp - 2 + k], c_recv.at[j, sp - k], device)
            for j, buf in enumerate((ctx, ctx_rope))
        ]

    def ctx_phase(k, arrive=True, depart=True):
        @pl.when(s_me >= k - 1)
        def _():
            if arrive and k > 1:
                for cp in ctx_up(k - 1):
                    cp.wait_recv()

            @pl.when(s_me < sp - 1)
            def _():
                if depart and k < sp:
                    for cp in ctx_up(k):
                        cp.start()

        @pl.when(s_me + k - 1 <= sp - 1)
        def _():
            if arrive and k > 1:
                for cp in ctx_down(k - 1):
                    cp.wait_recv()

            @pl.when(s_me > 0)
            def _():
                if depart and k < sp:
                    for cp in ctx_down(k):
                        cp.start()

    ctx_phase(1)

    parity = lax.rem(s_me, pair)

    def w_span(k):
        return pl.ds(pl.multiple_of((k * dp + d_me) * share, share), share)

    def w_copy(d):
        return remote(
            w_all.at[0, w_span(parity)], w_all.at[d, w_span(parity)], w_send.at[d - 1], w_recv.at[d - 1], mate(d)
        )

    def z_copy(d):
        span = w_span(parity)
        device = {"sp": s_me + 1 - 2 * parity}
        return remote(w_all.at[d, span], w_all.at[d, span], z_send.at[d - 1], z_recv.at[d - 1], device)

    def x_copy(d, e, k):
        i = ((d - 1) * (dp - 1) + e - 1) * pair + k
        span = w_span(k)
        return remote(w_all.at[d, span], w_all.at[d, span], x_send.at[i], x_recv.at[i], twin(e))

    early = range(1, tp - 1)
    late = range(tp - 1, tp)
    for d in early:
        w_copy(d).start()

    with jax.named_scope("prep"):
        gains[...] = jnp.zeros(gains.shape, F32)
        gains[0:1, :QK_DIM] = qgain_ref[...]
        gains[1:2, :QK_DIM] = kgain_ref[...]
        lane = lax.broadcasted_iota(jnp.int32, (1, LANES), 1)
        freq = ROPE_DIM // 4
        low = lax.rem(lane, 2 * freq) < freq
        live = lane < QK_DIM
        ones_lane = jnp.where(lane == VALUE_DIM, 1.0, 0.0).astype(F32)
        qgain = gains[0:1, :]
        kgain = gains[1:2, :]

        def swap(g):
            return jnp.where(low, pltpu.roll(g, LANES - freq, 1), pltpu.roll(g, freq, 1))

        qgain_swap = swap(qgain)
        kgain_swap = swap(kgain)

        def fill_tables(r, carry):
            span = pl.ds(pl.multiple_of(r * GRID_W, GRID_W), GRID_W)
            tab_a[span, :] = row_a[pl.ds(r, 1), :] + col_a[...]
            tab_b[span, :] = row_b[pl.ds(r, 1), :] + col_b[...]
            return carry

        lax.fori_loop(0, tab_a.shape[0] // GRID_W, fill_tables, 0)
        for cp in up_load:
            cp.wait()
        factor = LOG2E * QK_DIM ** (-0.5)
        qu_ref[...] = jnp.dot(qu_raw[...], qe_ref[...], preferred_element_type=F32).astype(BF16)
        ku_ref[...] = jnp.dot(ku_raw[...], ke_ref[...], preferred_element_type=F32).astype(BF16)
        vu_ref[...] = jnp.dot(vu_raw[...], ve_ref[...], preferred_element_type=F32).astype(BF16)
        spread = spread_ref[...]
        token_load.wait()
        for cp in down_load:
            cp.wait()
        x = tokens_ref[...].astype(F32)
        xn = x * norm_factor(x) * gain_ref[...]

    with jax.named_scope("waitmods"):
        for cp in mod_copies:
            cp.wait_recv()
    with jax.named_scope("stageB"):

        def gathered(buf):
            rows_of = []
            for t in range(tp):
                total = buf[t]
                for s in range(1, sp):
                    total = total + buf[s * tp + t]
                rows_of.append(total)
            return rows_of

        def joined(totals, start):
            count = width // tp // LANES
            return jnp.concatenate([t[start + c : start + c + 1] for t in totals for c in range(count)], axis=1)

        totals = gathered(mods)
        shift = joined(totals, 0)
        scale = joined(totals, width // tp // LANES)
        normed = (xn * (1.0 + scale) + shift).astype(BF16)
        q = jnp.dot(normed, qd_ref[...], preferred_element_type=F32)
        q_lat[0] = (q * norm_factor(q) * qg_ref[...]).astype(BF16)
        lat = jnp.dot(normed, kd_ref[...], preferred_element_type=F32)
        kv[0, 0, :rows, :] = (lat * norm_factor(lat) * kg_ref[...]).astype(BF16)
        rope = lax.dot_general(
            rd_ref[...], normed, (((1,), (1,)), ((), ())), preferred_element_type=F32
        ).astype(BF16)
        piece = ROPE_DIM // pieces
        for p in range(pieces):
            kv[0, 0, rows:, p * rows : (p + 1) * rows] = rope[p * piece : (p + 1) * piece]

    def q_copy(d):
        return remote(q_lat.at[0], q_lat.at[d], q_send.at[d - 1], q_recv.at[d - 1], mate(d))

    def kv_column(ds):
        return remote(kv.at[0, 0], kv.at[ds, 0], kv_send.at[ds, 0], kv_recv.at[ds, 0], column(ds))

    def kv_mate(ds, d):
        return remote(kv.at[ds, 0], kv.at[ds, d], kv_send.at[ds, d], kv_recv.at[ds, d], mate(d))

    for d in range(1, tp):
        q_copy(d).start()
    for ds in range(1, sp):
        kv_column(ds).start()
    for d in range(1, tp):
        kv_mate(0, d).start()

    contract = (((1,), (1,)), ((), ()))

    def expand(lats, ropes, a, b, store):
        rope = [
            lax.dot_general(r, spread, (((0,), (0,)), ((), ())), preferred_element_type=F32) for r in ropes
        ]
        rope = jnp.concatenate(rope, axis=0)
        lat = jnp.concatenate(lats, axis=0)
        k = jnp.dot(lat, ku_ref[...], preferred_element_type=F32)
        v = jnp.dot(lat, vu_ref[...], preferred_element_type=F32)
        k = [k[:, h * LANES : (h + 1) * LANES] for h in range(heads)]
        rope_square = jnp.sum(jnp.where(live, rope * rope, 0.0), axis=-1, keepdims=True)
        squares = [jnp.sum(kh * kh, axis=-1, keepdims=True) + rope_square for kh in k]
        turned = rope * a if b is None else rope * a + pltpu.roll(rope, QK_DIM, 1) * b
        scales = [lax.rsqrt(square * (1.0 / QK_DIM) + EPS) for square in squares]
        for h in range(heads):
            store(
                h, ((k[h] * kgain + turned) * scales[h]).astype(BF16),
                (v[:, h * LANES : (h + 1) * LANES] + ones_lane).astype(BF16),
            )

    def attend(starts, k_ref, v_ref, first_key, keys, lift, fresh):
        key_span = pl.ds(first_key, keys)
        items = [(pl.ds(start, q_rows), h) for start in starts for h in range(heads)]

        def product(span, h):
            return lax.dot_general(q_all[h, span, :], k_ref[h, key_span, :], contract, preferred_element_type=F32)

        ahead = 2
        scores = [product(*item) for item in items[:ahead]]
        for i, (span, h) in enumerate(items):
            if i + ahead < len(items):
                scores.append(product(*items[i + ahead]))
            s = scores[i]
            peak = jnp.max(s, axis=-1, keepdims=True)
            if lift:
                lift_h = lift_ref[h] * LOG2E
                peak = peak + lift_h
            if fresh:
                top = jnp.broadcast_to(peak, (q_rows, LANES))
            else:
                old = top_refs[h][span, :]
                top = jnp.maximum(old, peak)
            floor = top - lift_h if lift else top
            p = jnp.exp2(s - jnp.concatenate([floor] * (keys // LANES), axis=1)).astype(BF16)
            add = jnp.dot(p, v_ref[h, key_span, :], preferred_element_type=F32)
            if not fresh:
                add = acc_refs[h][span, :] * jnp.exp2(old - top) + add
            top_refs[h][span, :] = top
            acc_refs[h][span, :] = add

    def expand_context(first, count):
        slots = []
        for i in range(first, first + count):
            if i == 0:
                slots.append(0)
            elif i == 1:
                slots.append(jnp.where(s_me == 0, sp - 1, 1))
            else:
                slots.append(jnp.where(s_me == 0, i - 1, i))

        def store(h, k, v):
            k_ctx[h, first * ctx_rows : (first + count) * ctx_rows, :] = k
            v_ctx[h, first * ctx_rows : (first + count) * ctx_rows, :] = v

        expand([ctx[slot] for slot in slots], [ctx_rope[slot] for slot in slots], kgain, None, store)

    def tables(source, d, gain, gain_swap):
        start = pl.multiple_of((source * tp + (partner(tp, t_me, d) if d else t_me)) * rows, rows)
        return tab_a[pl.ds(start, rows), :] * gain, tab_b[pl.ds(start, rows), :] * gain_swap

    def stacked(pieces_of):
        return [jnp.concatenate(p, axis=0) for p in zip(*pieces_of)]

    def queries(mates):
        a, b = stacked([tables(s_me, d, qgain, qgain_swap) for d in mates])
        qx = jnp.dot(jnp.concatenate([q_lat[d] for d in mates], axis=0), qu_ref[...], preferred_element_type=F32)
        qx = [qx[:, h * LANES : (h + 1) * LANES] for h in range(heads)]
        squares = [jnp.sum(jnp.where(live, v * v, 0.0), axis=-1, keepdims=True) for v in qx]
        turned = [v * a + pltpu.roll(v, QK_DIM, 1) * b for v in qx]
        scales = [lax.rsqrt(square * (1.0 / QK_DIM) + EPS) * factor for square in squares]
        slot = (tp - 1 - mates[0]) * rows
        for h in range(heads):
            q_all[h, slot : slot + len(mates) * rows, :] = (turned[h] * scales[h]).astype(BF16)

    near = min(2, sp)
    near_keys = near * ctx_rows
    far_keys = (sp - near) * ctx_rows
    q_rows = 2 * rows if tp % 2 == 0 else rows

    with jax.named_scope("ctxwait"):
        ctx_phase(2)
    with jax.named_scope("ctxexpand"):
        expand_context(0, near)
    for first_mate in range(0, tp, q_rows // rows):
        mates = list(range(first_mate + q_rows // rows - 1, first_mate - 1, -1))
        with jax.named_scope("qwait"):
            for d in reversed(mates):
                if d:
                    q_copy(d).wait_recv()
        with jax.named_scope("queries"):
            queries(mates)
        with jax.named_scope("ctxattend"):
            attend([(tp - 1 - mates[0]) * rows], k_ctx, v_ctx, 0, near_keys, True, True)
        if first_mate == 0:
            with jax.named_scope("ctxwait3"):
                ctx_phase(3)
            with jax.named_scope("zwait"):
                for ds in range(1, sp):
                    kv_column(ds).wait_recv()
                    for m in range(1, tp):
                        kv_mate(ds, m).start()
    for i in range(len(others)):
        gate_copy(i).start()
    for d in late:
        w_copy(d).start()
    with jax.named_scope("ctxwait4"):
        for k in range(4, sp + 1):
            ctx_phase(k)
    if pair > 1:
        with jax.named_scope("wearly"):
            for d in early:
                w_copy(d).wait_recv()
                z_copy(d).start()
    if far_keys:
        with jax.named_scope("ctxexpand"):
            expand_context(near, sp - near)

    def group_step(i, carry):
        ds = lax.rem(lax.rem(i, 2) * ((i + 1) // 2) + lax.rem(i + 1, 2) * (sp - i // 2), sp)
        source = lax.rem(s_me + sp - ds, sp)
        with jax.named_scope("kvwait"):
            for d in range(1, tp):
                kv_mate(ds, d).wait_recv()
        with jax.named_scope("kvexpand"):
            a, b = stacked([tables(source, d, kgain, kgain_swap) for d in range(tp)])
            tails = [kv[ds, d, pl.ds(rows, ROPE_DIM // pieces), :] for d in range(tp)]
            ropes = [
                jnp.concatenate([t[:, p * rows : (p + 1) * rows] for p in range(pieces)], axis=0) for t in tails
            ]

            def store(h, k, v):
                k_buf[h] = k
                v_buf[h] = v

            expand([kv[ds, d, pl.ds(0, rows), :] for d in range(tp)], ropes, a, b, store)

        with jax.named_scope("attend"):
            attend(range(0, group, q_rows), k_buf, v_buf, 0, group, False, False)

        if far_keys:

            @pl.when(i == 0)
            def _():
                with jax.named_scope("ctxattend"):
                    attend(range(0, group, q_rows), k_ctx, v_ctx, near_keys, far_keys, True, False)

        @pl.when(i == sp - 2)
        def _():
            with jax.named_scope("wswap"):
                for d in late:
                    w_copy(d).wait_recv()
                    if pair > 1:
                        z_copy(d).start()
                if pair == 1:
                    for d in early:
                        w_copy(d).wait_recv()

        return carry

    lax.fori_loop(0, sp, group_step, 0)

    with jax.named_scope("wtwin"):
        for d in range(1, tp):
            if pair > 1:
                z_copy(d).wait_recv()
            for e in range(1, dp):
                for k in range(pair):
                    x_copy(d, e, k).start()

    def a_copy(d):
        return remote(att.at[d], held.at[d - 1], a_send.at[d - 1], a_recv.at[d - 1], mate(d))

    with jax.named_scope("finish"):
        for d in range(tp - 1, -1, -1):
            slot = (tp - 1 - d) * rows
            outs = []
            for h in range(heads):
                total = acc_refs[h][slot : slot + rows, :]
                outs.append((total[:, :VALUE_DIM] / total[:, VALUE_DIM : VALUE_DIM + 1]).astype(BF16))
            att[d] = jnp.concatenate(outs, axis=1)
            if d:
                a_copy(d).start()

    with jax.named_scope("tail"):
        chunk = 512
        spans = [slice(n * chunk, (n + 1) * chunk) for n in range(width // chunk)]
        mixed = [
            jnp.dot(att[0], w_all[0, :, cols], preferred_element_type=F32).astype(BF16).astype(F32) for cols in spans
        ]
        for d in range(1, tp):
            with jax.named_scope("xwait"):
                for e in range(1, dp):
                    for k in range(pair):
                        x_copy(d, e, k).wait_recv()
            with jax.named_scope("await"):
                a_copy(d).wait_recv()
            for n, cols in enumerate(spans):
                term = jnp.dot(held[d - 1], w_all[d, :, cols], preferred_element_type=F32)
                mixed[n] = mixed[n] + term.astype(BF16).astype(F32)
        for i in range(len(others)):
            gate_copy(i).wait_recv()
        gate_buf[...] = joined(gathered(gates), 0)
        for n, cols in enumerate(spans):
            out_ref[:, cols] = (tokens_ref[:, cols].astype(F32) + gate_buf[:, cols] * mixed[n]).astype(BF16)

    with jax.named_scope("drain"):
        for cp in mod_copies:
            cp.wait_send()
        for i in range(len(others)):
            gate_copy(i).wait_send()
        for k in range(1, sp):

            @pl.when((s_me >= k - 1) & (s_me < sp - 1))
            def _():
                for cp in ctx_up(k):
                    cp.wait_send()

            @pl.when((s_me + k - 1 <= sp - 1) & (s_me > 0))
            def _():
                for cp in ctx_down(k):
                    cp.wait_send()

        for d in range(1, tp):
            q_copy(d).wait_send()
            a_copy(d).wait_send()
            w_copy(d).wait_send()
            if pair > 1:
                z_copy(d).wait_send()
            for e in range(1, dp):
                for k in range(pair):
                    x_copy(d, e, k).wait_send()
            for ds in range(sp):
                kv_mate(ds, d).wait_send()
        for ds in range(1, sp):
            kv_column(ds).wait_send()


def local(
    sp, tp, dp,
    latent_tokens, condition, shift_weight, scale_weight, gate_weight, norm_gain,
    query_down, query_gain, kv_down, kv_gain, rope_down, query_up, key_up, value_up,
    query_norm_gain, key_norm_gain, out_weight, context_latent, context_rope, context_lift,
):
    rows, width = latent_tokens.shape
    q_rank = query_down.shape[1]
    rank = kv_down.shape[1]
    heads = query_up.shape[1] // QK_DIM
    ctx_rows = context_latent.shape[0]
    group = rows * tp
    tokens = group * sp
    context = sp * ctx_rows
    n_dev = sp * tp
    row_a, row_b = turn_tables(tokens // GRID_W, 0)
    col_a, col_b = turn_tables(GRID_W, 1)
    q_spread = jnp.asarray(query_spread(heads), BF16)
    k_spread = jnp.asarray(head_spread(heads, NOPE_DIM), BF16)
    v_spread = jnp.asarray(head_spread(heads, VALUE_DIM), BF16)
    dma = pltpu.SemaphoreType.DMA
    vmem = pltpu.VMEM
    return pl.pallas_call(
        functools.partial(fused_kernel, sp, tp, dp, heads),
        out_shape=pltpu.VMEM((rows, width), BF16),
        in_specs=[VMEM_SPEC] * 6 + [pl.BlockSpec(memory_space=pltpu.SMEM)] + [VMEM_SPEC] * 5 + [HBM_SPEC] * 16,
        out_specs=VMEM_SPEC,
        scratch_shapes=[
            vmem((n_dev, 2 * width // tp // LANES, LANES), F32),
            vmem((n_dev, width // tp // LANES, LANES), F32),
            vmem((tp, rows, q_rank), BF16),
            vmem((sp, tp, rows + ROPE_DIM * rows // rank, rank), BF16),
            vmem((sp, ctx_rows, rank), BF16),
            vmem((sp, ROPE_DIM, ctx_rows), BF16),
            vmem((1, width), F32),
            vmem((tokens, LANES), F32),
            vmem((tokens, LANES), F32),
            vmem((8, LANES), F32),
            vmem((heads, group, LANES), BF16),
            vmem((heads, group, LANES), BF16),
            vmem((heads, group, LANES), BF16),
            vmem((heads, context, LANES), BF16),
            vmem((heads, context, LANES), BF16),
            vmem((tp, rows, heads * VALUE_DIM), BF16),
            vmem((tp - 1, rows, heads * VALUE_DIM), BF16),
            vmem((tp,) + out_weight.shape, BF16),
            vmem(shift_weight.shape, BF16),
            vmem(scale_weight.shape, BF16),
            vmem(gate_weight.shape, BF16),
            vmem(latent_tokens.shape, BF16),
            vmem(query_down.shape, BF16),
            vmem(kv_down.shape, BF16),
            vmem(rope_down.shape[::-1], BF16),
            vmem(query_up.shape, BF16),
            vmem(key_up.shape, BF16),
            vmem(value_up.shape, BF16),
            vmem(q_spread.shape, BF16),
            vmem(k_spread.shape, BF16),
            vmem(v_spread.shape, BF16),
            vmem((q_rank, heads * LANES), BF16),
            vmem((rank, heads * LANES), BF16),
            vmem((rank, heads * LANES), BF16),
            dma((16,)),
            dma((n_dev - 1,)), dma((n_dev - 1,)),
            dma((n_dev - 1,)), dma((n_dev - 1,)),
            dma((tp - 1,)), dma((tp - 1,)),
            dma((sp, tp)), dma((sp, tp)),
            dma((2, 2 * sp)), dma((2, sp)),
            dma((tp - 1,)), dma((tp - 1,)),
            dma((tp - 1,)), dma((tp - 1,)),
            dma((2 * (tp - 1) * (dp - 1),)), dma((2 * (tp - 1) * (dp - 1),)),
            dma((tp - 1,)), dma((tp - 1,)),
        ]
        + [vmem((group, LANES), F32)] * (2 * heads),
        compiler_params=pltpu.CompilerParams(
            collective_id=0, has_side_effects=True, vmem_limit_bytes=58 * 1024 * 1024
        ),
        name="fused",
    )(
        condition, norm_gain[None], query_gain[None], kv_gain[None], query_norm_gain[None], key_norm_gain[None],
        context_lift, jnp.asarray(row_a), jnp.asarray(row_b), jnp.asarray(col_a), jnp.asarray(col_b),
        jnp.asarray(rope_spread(), BF16),
        shift_weight, scale_weight, gate_weight, latent_tokens, query_down, kv_down, rope_down.T,
        context_latent, context_rope.T, query_up, key_up, value_up, q_spread, k_spread, v_spread, out_weight,
    )


def solution(mesh):
    in_specs = (
        P(("dp", "sp", "tp"), None), P(("dp", "sp")), P("sp", "tp"), P("sp", "tp"), P("sp", "tp"),
        P(), P(), P(), P(), P(), P(), P(None, "tp"), P(None, "tp"), P(None, "tp"), P(), P(),
        P("tp", None), P(("dp", "sp"), None), P(("dp", "sp"), None), P("tp"),
    )
    out_specs = P(("dp", "sp", "tp"), None)
    body = functools.partial(local, mesh.shape["sp"], mesh.shape["tp"], mesh.shape["dp"])
    return jax.shard_map(body, mesh=mesh, in_specs=in_specs, out_specs=out_specs, check_vma=False)
```

```python
import functools

import jax
import jax.numpy as jnp
import numpy as np
from jax import lax
from jax.experimental import pallas as pl
from jax.experimental.pallas import tpu as pltpu
from jax.sharding import PartitionSpec as P

NOPE_DIM = 64
ROPE_DIM = 32
VALUE_DIM = 64
QK_DIM = 96
GRID_W = 64
LANES = 128

EPS = 1e-06
THETA = 10000.0
LOG2E = 1.4426950408889634
MESH = pl.DeviceIdType.MESH
VMEM_SPEC = pl.BlockSpec(memory_space=pltpu.VMEM)
HBM_SPEC = pl.BlockSpec(memory_space=pltpu.HBM)
BF16 = jnp.bfloat16
F32 = jnp.float32


def partner_order():
    return np.arange(ROPE_DIM) ^ (ROPE_DIM // 4)


def rope_spread():
    spread = np.zeros((ROPE_DIM, LANES), np.float32)
    order = partner_order()
    for j in range(ROPE_DIM):
        spread[j, NOPE_DIM + j] = 1.0
        spread[order[j], QK_DIM + j] = 1.0
    return spread


def query_spread(heads):
    spread = np.zeros((heads * QK_DIM, heads * LANES), np.float32)
    order = partner_order()
    for h in range(heads):
        for j in range(QK_DIM):
            spread[h * QK_DIM + j, h * LANES + j] = 1.0
        for j in range(ROPE_DIM):
            spread[h * QK_DIM + NOPE_DIM + order[j], h * LANES + QK_DIM + j] = 1.0
    return spread


def head_spread(heads, width):
    spread = np.zeros((heads * width, heads * LANES), np.float32)
    for h in range(heads):
        for j in range(width):
            spread[h * width + j, h * LANES + j] = 1.0
    return spread


def turn_tables(count, axis):
    freq_count = ROPE_DIM // 4
    inverse = np.float32(THETA) ** (-np.float32(4.0) * np.arange(freq_count, dtype=np.float32) / np.float32(ROPE_DIM))
    angles = np.arange(count, dtype=np.float32)[:, None] * inverse.astype(np.float32)
    cosine = np.zeros((count, LANES), np.float32)
    sine = np.zeros((count, LANES), np.float32)
    start = NOPE_DIM + axis * 2 * freq_count
    mid = start + freq_count
    cosine[:, start:mid] = np.cos(angles.astype(np.float64))
    cosine[:, mid : mid + freq_count] = np.cos(angles.astype(np.float64))
    sine[:, start:mid] = -np.sin(angles.astype(np.float64))
    sine[:, mid : mid + freq_count] = np.sin(angles.astype(np.float64))
    if axis == 0:
        cosine[:, :NOPE_DIM] = 1.0
    return cosine, sine


def norm_factor(values):
    return lax.rsqrt(jnp.mean(values * values, axis=-1, keepdims=True) + EPS)


def partner(tp, index, d):
    if tp & (tp - 1):
        return lax.rem(index + d, tp)
    result = 0 * index
    bit = 1
    while bit < tp:
        here = lax.rem(index // bit, 2)
        result = result + bit * (lax.rem(here + 1, 2) if d & bit else here)
        bit *= 2
    return result


def fused_kernel(
    sp, tp, dp, heads,
    lift_ref, cond_hbm, gain_hbm, qg_hbm, kg_hbm, qgain_hbm, kgain_hbm, row_a_hbm, row_b_hbm, col_a_hbm, col_b_hbm,
    spread_hbm,
    shift_hbm, scale_hbm, gate_hbm, tokens_hbm, qd_hbm, kd_hbm, rd_hbm, cl_hbm, cr_hbm,
    qu_hbm, ku_hbm, vu_hbm, qe_hbm, ke_hbm, ve_hbm, w_hbm,
    out_ref,
    mods, gates, q_lat, kv, ctx, ctx_rope, gate_buf, tab_a, tab_b, gains, q_all, k_buf, v_buf, k_ctx, v_ctx, att, held,
    w_all, shift_w, scale_w, gate_w, tokens_ref, qd_ref, kd_ref, rd_ref,
    qu_raw, ku_raw, vu_raw, qe_ref, ke_ref, ve_ref, qu_ref, ku_ref, vu_ref,
    cond_ref, gain_ref, qg_ref, kg_ref, qgain_ref, kgain_ref, row_a, row_b, col_a, col_b, spread_ref,
    load_sem, mod_send, mod_recv, g_send, g_recv, q_send, q_recv, kv_send, kv_recv, c_send, c_recv, w_send, w_recv,
    r_send, r_recv, z_send, z_recv, x_send, x_recv, a_send, a_recv, *state,
):
    top_refs, acc_refs = state[:heads], state[heads:]
    s_me = lax.axis_index("sp")
    t_me = lax.axis_index("tp")
    d_me = lax.axis_index("dp")
    me = s_me * tp + t_me
    rows = tokens_ref.shape[0]
    rank = ku_raw.shape[0]
    group = tp * rows
    ctx_rows = cl_hbm.shape[0]
    pair = 2 - sp % 2
    share = w_hbm.shape[0] // dp
    unit = share // 4
    relay = tp == 4
    direct = range(1, 3) if relay else range(1, tp)
    width = w_hbm.shape[1]
    pieces = rank // rows

    def load(i, src, dst):
        cp = pltpu.make_async_copy(src, dst, load_sem.at[i])
        cp.start()
        return cp

    cond_load = load(16, cond_hbm, cond_ref)
    first = [
        load(i, src, dst)
        for i, (src, dst) in enumerate(((shift_hbm, shift_w), (scale_hbm, scale_w), (gate_hbm, gate_w)))
    ]
    ctx_load = [
        load(3, cl_hbm, ctx.at[0]),
        load(4, cr_hbm, ctx_rope.at[0]),
    ]

    def later_loads():
        w_load = load(5, w_hbm, w_all.at[0])
        small_load = [
            load(17 + i, src, dst)
            for i, (src, dst) in enumerate((
                (gain_hbm, gain_ref), (qg_hbm, qg_ref), (kg_hbm, kg_ref), (qgain_hbm, qgain_ref),
                (kgain_hbm, kgain_ref), (row_a_hbm, row_a), (row_b_hbm, row_b), (col_a_hbm, col_a),
                (col_b_hbm, col_b), (spread_hbm, spread_ref),
            ))
        ]
        token_load = load(6, tokens_hbm, tokens_ref)
        up_load = [
            load(10 + i, src, dst)
            for i, (src, dst) in enumerate((
                (qu_hbm, qu_raw), (ku_hbm, ku_raw), (vu_hbm, vu_raw), (qe_hbm, qe_ref), (ke_hbm, ke_ref), (ve_hbm, ve_ref),
            ))
        ]
        down_load = [load(7, qd_hbm, qd_ref), load(8, kd_hbm, kd_ref), load(9, rd_hbm, rd_ref)]
        return w_load, small_load, token_load, up_load, down_load

    def peer(ds, dt):
        return {"sp": lax.rem(s_me + ds, sp), "tp": lax.rem(t_me + dt, tp)}

    def column(ds):
        return {"sp": lax.rem(s_me + ds, sp)}

    def mate(d):
        return {"tp": partner(tp, t_me, d)}

    def twin(e):
        return {"dp": lax.rem(d_me + e, dp)}

    def remote(src, dst, send, recv, device):
        return pltpu.make_async_remote_copy(
            src_ref=src, dst_ref=dst, send_sem=send, recv_sem=recv, device_id=device, device_id_type=MESH
        )

    others = [(ds, dt) for ds in range(sp) for dt in range(tp) if ds or dt]
    barrier = pltpu.get_barrier_semaphore()
    for ds, dt in others:
        pl.semaphore_signal(barrier, inc=1, device_id=peer(ds, dt), device_id_type=MESH)
    for e in range(1, dp):
        pl.semaphore_signal(barrier, inc=1, device_id=twin(e), device_id_type=MESH)

    with jax.named_scope("modmm"):
        cond_load.wait()
        c = cond_ref[...].reshape(1, cond_ref.shape[0]).astype(F32)
        act = (c / (1.0 + jnp.exp(-c))).astype(BF16)
        act = jnp.broadcast_to(act, (16, act.shape[1]))
        terms = []
        for i, w in enumerate((shift_w, scale_w, gate_w)):
            first[i].wait()
            if i == 2:
                w_load, small_load, token_load, up_load, down_load = later_loads()
            term = jnp.dot(act, w[...], preferred_element_type=F32)[0:1]
            terms.append([term[:, c : c + LANES] for c in range(0, term.shape[1], LANES)])
        mods[me] = jnp.concatenate(terms[0] + terms[1], axis=0)
        gates[me] = jnp.concatenate(terms[2], axis=0)
        for cp in ctx_load:
            cp.wait()

    with jax.named_scope("barrier"):
        pl.semaphore_wait(barrier, len(others) + dp - 1)
    mod_copies = []
    for i, (ds, dt) in enumerate(others):
        mod_copies.append(remote(mods.at[me], mods.at[me], mod_send.at[i], mod_recv.at[i], peer(ds, dt)))
        mod_copies[-1].start()

    def gate_copy(i):
        return remote(gates.at[me], gates.at[me], g_send.at[i], g_recv.at[i], peer(*others[i]))

    def ctx_up(k):
        device = {"sp": lax.rem(s_me + 1, sp)}
        return [
            remote(buf.at[k - 1], buf.at[k], c_send.at[j, k - 1], c_recv.at[j, k], device)
            for j, buf in enumerate((ctx, ctx_rope))
        ]

    def ctx_down(k):
        device = {"sp": lax.rem(s_me + sp - 1, sp)}
        src = (sp - k + 1) % sp
        return [
            remote(buf.at[src], buf.at[sp - k], c_send.at[j, sp - 2 + k], c_recv.at[j, sp - k], device)
            for j, buf in enumerate((ctx, ctx_rope))
        ]

    def ctx_phase(k, arrive=True, depart=True):
        @pl.when(s_me >= k - 1)
        def _():
            if arrive and k > 1:
                for cp in ctx_up(k - 1):
                    cp.wait_recv()

            @pl.when(s_me < sp - 1)
            def _():
                if depart and k < sp:
                    for cp in ctx_up(k):
                        cp.start()

        @pl.when(s_me + k - 1 <= sp - 1)
        def _():
            if arrive and k > 1:
                for cp in ctx_down(k - 1):
                    cp.wait_recv()

            @pl.when(s_me > 0)
            def _():
                if depart and k < sp:
                    for cp in ctx_down(k):
                        cp.start()

    ctx_phase(1)

    parity = lax.rem(s_me, pair)
    base = d_me * share
    mine = [parity * 3 * unit, unit, 2 * unit] if pair > 1 else [k * unit for k in range(4)]

    def w_rows(offset):
        return pl.ds(pl.multiple_of(base + offset, unit), unit)

    def w_copy(d, j):
        span = w_rows(mine[j])
        return remote(w_all.at[0, span], w_all.at[d, span], w_send.at[d - 1, j], w_recv.at[d - 1, j], mate(d))

    def w_relay(j, k):
        span = w_rows(mine[j])
        cols = pl.ds(k * (width // 2), width // 2)
        return remote(
            w_all.at[1 + k, span, cols], w_all.at[3, span, cols], r_send.at[j, k], r_recv.at[j, k], mate(2 - k)
        )

    def z_copy(d):
        span = w_rows(mine[0])
        device = {"sp": s_me + 1 - 2 * parity}
        return remote(w_all.at[d, span], w_all.at[d, span], z_send.at[d - 1], z_recv.at[d - 1], device)

    def x_copy(d, e, j):
        span = w_rows(mine[j] if j < len(mine) else (1 - parity) * 3 * unit)
        i = (d - 1) * (dp - 1) + e - 1
        return remote(w_all.at[d, span], w_all.at[d, span], x_send.at[i, j], x_recv.at[i, j], twin(e))

    def w_arrive(d, j):
        if relay and d == 3:
            for k in range(2):
                w_relay(j, k).wait_recv()
        else:
            w_copy(d, j).wait_recv()

    early = range(2)
    late = range(2, len(mine))
    w_load.wait()
    for d in direct:
        w_copy(d, 0).start()

    with jax.named_scope("prep"):
        for cp in small_load:
            cp.wait()
        gains[...] = jnp.zeros(gains.shape, F32)
        gains[0:1, :QK_DIM] = qgain_ref[...]
        gains[1:2, :QK_DIM] = kgain_ref[...]
        lane = lax.broadcasted_iota(jnp.int32, (1, LANES), 1)
        freq = ROPE_DIM // 4
        low = lax.rem(lane, 2 * freq) < freq
        live = lane < QK_DIM
        ones_lane = jnp.where(lane == VALUE_DIM, 1.0, 0.0).astype(F32)
        qgain = gains[0:1, :]
        kgain = gains[1:2, :]

        def swap(g):
            return jnp.where(low, pltpu.roll(g, LANES - freq, 1), pltpu.roll(g, freq, 1))

        qgain_swap = swap(qgain)
        kgain_swap = swap(kgain)

        def fill_tables(r, carry):
            span = pl.ds(pl.multiple_of(r * GRID_W, GRID_W), GRID_W)
            tab_a[span, :] = row_a[pl.ds(r, 1), :] + col_a[...]
            tab_b[span, :] = row_b[pl.ds(r, 1), :] + col_b[...]
            return carry

        lax.fori_loop(0, tab_a.shape[0] // GRID_W, fill_tables, 0)
        for cp in up_load:
            cp.wait()
        factor = LOG2E * QK_DIM ** (-0.5)
        qu_ref[...] = jnp.dot(qu_raw[...], qe_ref[...], preferred_element_type=F32).astype(BF16)
        ku_ref[...] = jnp.dot(ku_raw[...], ke_ref[...], preferred_element_type=F32).astype(BF16)
        vu_ref[...] = jnp.dot(vu_raw[...], ve_ref[...], preferred_element_type=F32).astype(BF16)
        spread = spread_ref[...]
        token_load.wait()
        for cp in down_load:
            cp.wait()
        x = tokens_ref[...].astype(F32)
        xn = x * norm_factor(x) * gain_ref[...]

    with jax.named_scope("waitmods"):
        for cp in mod_copies:
            cp.wait_recv()
    def q_copy(d):
        return remote(q_lat.at[0], q_lat.at[d], q_send.at[d - 1], q_recv.at[d - 1], mate(d))

    def q_relay(k):
        cols = pl.ds(k * (q_lat.shape[2] // 2), q_lat.shape[2] // 2)
        return remote(
            q_lat.at[1 + k, :, cols], q_lat.at[3, :, cols], q_send.at[2 + k], q_recv.at[2 + k], mate(2 - k)
        )

    with jax.named_scope("stageB"):

        def gathered(buf):
            rows_of = []
            for t in range(tp):
                total = buf[t]
                for s in range(1, sp):
                    total = total + buf[s * tp + t]
                rows_of.append(total)
            return rows_of

        def joined(totals, start):
            count = width // tp // LANES
            return jnp.concatenate([t[start + c : start + c + 1] for t in totals for c in range(count)], axis=1)

        totals = gathered(mods)
        shift = joined(totals, 0)
        scale = joined(totals, width // tp // LANES)
        normed = (xn * (1.0 + scale) + shift).astype(BF16)
        q = jnp.dot(normed, qd_ref[...], preferred_element_type=F32)
        q_lat[0] = (q * norm_factor(q) * qg_ref[...]).astype(BF16)
        for d in direct:
            q_copy(d).start()
        lat = jnp.dot(normed, kd_ref[...], preferred_element_type=F32)
        kv[0, 0, :rows, :] = (lat * norm_factor(lat) * kg_ref[...]).astype(BF16)
        rope = lax.dot_general(
            rd_ref[...], normed, (((1,), (1,)), ((), ())), preferred_element_type=F32
        ).astype(BF16)
        piece = ROPE_DIM // pieces
        for p in range(pieces):
            kv[0, 0, rows:, p * rows : (p + 1) * rows] = rope[p * piece : (p + 1) * piece]

    def kv_column(ds):
        return remote(kv.at[0, 0], kv.at[ds, 0], kv_send.at[ds, 0], kv_recv.at[ds, 0], column(ds))

    def kv_mate(ds, d):
        return remote(kv.at[ds, 0], kv.at[ds, d], kv_send.at[ds, d], kv_recv.at[ds, d], mate(d))

    def kv_relay(ds, k):
        cols = pl.ds(k * (rank // 2), rank // 2)
        return remote(
            kv.at[ds, 1 + k, :, cols], kv.at[ds, 3, :, cols], kv_send.at[ds, 3 + k], kv_recv.at[ds, 3 + k], mate(2 - k)
        )

    def middle(i):
        return (i + 1) // 2 if i % 2 else sp - i // 2

    def source_step(i):
        return jnp.where(s_me == 0, sp - i, jnp.where(s_me == sp - 1, i, middle(i)))

    def target_step(i):
        return jnp.where(s_me == 0, i, jnp.where(s_me == sp - 1, sp - i, middle(i)))

    for i in range(1, sp):
        kv_column(target_step(i)).start()
    for d in direct:
        kv_mate(0, d).start()

    contract = (((1,), (1,)), ((), ()))

    def expand(lats, ropes, a, b, store):
        rope = [
            lax.dot_general(r, spread, (((0,), (0,)), ((), ())), preferred_element_type=F32) for r in ropes
        ]
        rope = jnp.concatenate(rope, axis=0)
        lat = jnp.concatenate(lats, axis=0)
        k = jnp.dot(lat, ku_ref[...], preferred_element_type=F32)
        v = jnp.dot(lat, vu_ref[...], preferred_element_type=F32)
        k = [k[:, h * LANES : (h + 1) * LANES] for h in range(heads)]
        rope_square = jnp.sum(jnp.where(live, rope * rope, 0.0), axis=-1, keepdims=True)
        squares = [jnp.sum(kh * kh, axis=-1, keepdims=True) + rope_square for kh in k]
        turned = rope * a if b is None else rope * a + pltpu.roll(rope, QK_DIM, 1) * b
        scales = [lax.rsqrt(square * (1.0 / QK_DIM) + EPS) for square in squares]
        for h in range(heads):
            store(
                h, ((k[h] * kgain + turned) * scales[h]).astype(BF16),
                (v[:, h * LANES : (h + 1) * LANES] + ones_lane).astype(BF16),
            )

    def attend(starts, k_ref, v_ref, first_key, keys, lift, fresh):
        key_span = pl.ds(first_key, keys)
        items = [(pl.ds(start, q_rows), h) for start in starts for h in range(heads)]

        def product(span, h):
            return lax.dot_general(q_all[h, span, :], k_ref[h, key_span, :], contract, preferred_element_type=F32)

        ahead = 2
        scores = [product(*item) for item in items[:ahead]]
        for i, (span, h) in enumerate(items):
            if i + ahead < len(items):
                scores.append(product(*items[i + ahead]))
            s = scores[i]
            peak = jnp.max(s, axis=-1, keepdims=True)
            if lift:
                lift_h = lift_ref[h] * LOG2E
                peak = peak + lift_h
            if fresh:
                top = jnp.broadcast_to(peak, (q_rows, LANES))
            else:
                old = top_refs[h][span, :]
                top = jnp.maximum(old, peak)
            floor = top - lift_h if lift else top
            p = jnp.exp2(s - jnp.concatenate([floor] * (keys // LANES), axis=1)).astype(BF16)
            add = jnp.dot(p, v_ref[h, key_span, :], preferred_element_type=F32)
            if not fresh:
                add = acc_refs[h][span, :] * jnp.exp2(old - top) + add
            top_refs[h][span, :] = top
            acc_refs[h][span, :] = add

    def expand_context(first, count):
        slots = []
        for i in range(first, first + count):
            if i == 0:
                slots.append(0)
            elif i == 1:
                slots.append(jnp.where(s_me == 0, sp - 1, 1))
            else:
                slots.append(jnp.where(s_me == 0, i - 1, i))

        def store(h, k, v):
            k_ctx[h, first * ctx_rows : (first + count) * ctx_rows, :] = k
            v_ctx[h, first * ctx_rows : (first + count) * ctx_rows, :] = v

        expand([ctx[slot] for slot in slots], [ctx_rope[slot] for slot in slots], kgain, None, store)

    def tables(source, d, gain, gain_swap):
        start = pl.multiple_of((source * tp + (partner(tp, t_me, d) if d else t_me)) * rows, rows)
        return tab_a[pl.ds(start, rows), :] * gain, tab_b[pl.ds(start, rows), :] * gain_swap

    def stacked(pieces_of):
        return [jnp.concatenate(p, axis=0) for p in zip(*pieces_of)]

    def queries(mates):
        a, b = stacked([tables(s_me, d, qgain, qgain_swap) for d in mates])
        qx = jnp.dot(jnp.concatenate([q_lat[d] for d in mates], axis=0), qu_ref[...], preferred_element_type=F32)
        qx = [qx[:, h * LANES : (h + 1) * LANES] for h in range(heads)]
        squares = [jnp.sum(jnp.where(live, v * v, 0.0), axis=-1, keepdims=True) for v in qx]
        turned = [v * a + pltpu.roll(v, QK_DIM, 1) * b for v in qx]
        scales = [lax.rsqrt(square * (1.0 / QK_DIM) + EPS) * factor for square in squares]
        slot = (tp - 1 - mates[0]) * rows
        for h in range(heads):
            q_all[h, slot : slot + len(mates) * rows, :] = (turned[h] * scales[h]).astype(BF16)

    near = min(2, sp)
    near_keys = near * ctx_rows
    far_keys = (sp - near) * ctx_rows
    q_rows = 2 * rows if tp % 2 == 0 else rows

    with jax.named_scope("ctxwait"):
        ctx_phase(2)
    with jax.named_scope("ctxexpand"):
        expand_context(0, near)
    def kv_relays(ds):
        if relay:
            for k in range(2):
                kv_mate(ds, 1 + k).wait_recv()
                kv_relay(ds, k).start()

    def queries_attend(first_mate):
        mates = list(range(first_mate + q_rows // rows - 1, first_mate - 1, -1))
        with jax.named_scope("queries"):
            queries(mates)
        with jax.named_scope("ctxattend"):
            attend([(tp - 1 - mates[0]) * rows], k_ctx, v_ctx, 0, near_keys, True, True)

    with jax.named_scope("qwait"):
        for d in direct:
            q_copy(d).wait_recv()
            if relay:
                q_relay(d - 1).start()
        if relay:
            for k in range(2):
                w_copy(1 + k, 0).wait_recv()
                w_relay(0, k).start()
    for d in direct:
        w_copy(d, 1).start()
    queries_attend(0)
    with jax.named_scope("kvwait0"):
        kv_relays(0)
    with jax.named_scope("zwait"):
        for i in range(1, sp):
            ds = source_step(i)
            kv_column(ds).wait_recv()
            for d in direct:
                kv_mate(ds, d).start()
    for i in range(len(others)):
        gate_copy(i).start()
    with jax.named_scope("qwait3"):
        if relay:
            for k in range(2):
                q_relay(k).wait_recv()
    for first_mate in range(q_rows // rows, tp, q_rows // rows):
        queries_attend(first_mate)
    with jax.named_scope("ctxwait3"):
        ctx_phase(3)
    if pair > 1:
        with jax.named_scope("pairwait"):
            for d in direct:
                if not relay:
                    w_copy(d, 0).wait_recv()
                z_copy(d).start()
    with jax.named_scope("relaywait"):
        for i in range(1, min(3, sp)):
            kv_relays(source_step(i))
        if relay:
            for k in range(2):
                w_copy(1 + k, 1).wait_recv()
                w_relay(1, k).start()
    for j in late:
        for d in direct:
            w_copy(d, j).start()

    def a_copy(d):
        return remote(att.at[d], held.at[d - 1], a_send.at[d - 1], a_recv.at[d - 1], mate(d))

    def finish(mates):
        for d in mates:
            slot = (tp - 1 - d) * rows
            outs = []
            for h in range(heads):
                total = acc_refs[h][slot : slot + rows, :]
                outs.append((total[:, :VALUE_DIM] / total[:, VALUE_DIM : VALUE_DIM + 1]).astype(BF16))
            att[d] = jnp.concatenate(outs, axis=1)
            if d:
                a_copy(d).start()

    def group_step(i, carry):
        ds = jnp.where(
            s_me == 0,
            lax.rem(sp - i, sp),
            jnp.where(
                s_me == sp - 1,
                i,
                lax.rem(lax.rem(i, 2) * ((i + 1) // 2) + lax.rem(i + 1, 2) * (sp - i // 2), sp),
            ),
        )
        source = lax.rem(s_me + sp - ds, sp)
        with jax.named_scope("kvwait"):
            if relay:
                for k in range(2):
                    kv_relay(ds, k).wait_recv()
            else:
                for d in direct:
                    kv_mate(ds, d).wait_recv()
        with jax.named_scope("kvexpand"):
            a, b = stacked([tables(source, d, kgain, kgain_swap) for d in range(tp)])
            tails = [kv[ds, d, pl.ds(rows, ROPE_DIM // pieces), :] for d in range(tp)]
            ropes = [
                jnp.concatenate([t[:, p * rows : (p + 1) * rows] for p in range(pieces)], axis=0) for t in tails
            ]

            def store(h, k, v):
                k_buf[h] = k
                v_buf[h] = v

            expand([kv[ds, d, pl.ds(0, rows), :] for d in range(tp)], ropes, a, b, store)

        @pl.when(i < sp - 1)
        def _():
            with jax.named_scope("attend"):
                attend(range(0, group, q_rows), k_buf, v_buf, 0, group, False, False)

        @pl.when(i == sp - 1)
        def _():
            with jax.named_scope("attendlast"):
                count = q_rows // rows
                for start in range(0, group, q_rows):
                    attend([start], k_buf, v_buf, 0, group, False, False)
                    top_mate = tp - 1 - start // rows
                    finish(range(top_mate, top_mate - count, -1))

        if sp > 3:

            @pl.when(i < sp - 3)
            def _():
                with jax.named_scope("relaywait"):
                    n = i + 3
                    step = lax.rem(n, 2) * ((n + 1) // 2) + lax.rem(n + 1, 2) * (sp - n // 2)
                    kv_relays(jnp.where(s_me == 0, sp - n, jnp.where(s_me == sp - 1, n, step)))

        @pl.when(i == 0)
        def _():
            with jax.named_scope("w0"):
                if relay and pair > 1:
                    w_arrive(3, 0)
                    z_copy(3).start()

        if far_keys:

            @pl.when(i == 1)
            def _():
                with jax.named_scope("ctxwait4"):
                    for k in range(4, sp + 1):
                        ctx_phase(k)
                with jax.named_scope("ctxexpand"):
                    expand_context(near, sp - near)
                with jax.named_scope("ctxattend"):
                    attend(range(0, group, q_rows), k_ctx, v_ctx, near_keys, far_keys, True, False)

        @pl.when(i == min(1, sp - 2))
        def _():
            with jax.named_scope("wlate"):
                if relay:
                    for j in late:
                        for k in range(2):
                            w_copy(1 + k, j).wait_recv()
                            w_relay(j, k).start()

        @pl.when(i == sp - 2)
        def _():
            with jax.named_scope("w1"):
                for d in range(1, tp):
                    for j in range(len(mine)):
                        if j in early or (relay and d < 3):
                            if relay and d == 3 and (j == 1 or pair == 1):
                                w_arrive(d, j)
                            if not relay and not (j == 0 and pair > 1):
                                w_arrive(d, j)
                            for e in range(1, dp):
                                x_copy(d, e, j).start()
                    if pair > 1 and d < 3:
                        z_copy(d).wait_recv()
                        for e in range(1, dp):
                            x_copy(d, e, len(mine)).start()

        return carry

    lax.fori_loop(0, sp, group_step, 0)

    with jax.named_scope("wtwin"):
        for d in range(1, tp):
            for j in late:
                if not relay or d == 3:
                    w_arrive(d, j)
                    for e in range(1, dp):
                        x_copy(d, e, j).start()
            if pair > 1 and d >= 3:
                z_copy(d).wait_recv()
                for e in range(1, dp):
                    x_copy(d, e, len(mine)).start()

    with jax.named_scope("tail"):
        chunk = 512
        spans = [slice(n * chunk, (n + 1) * chunk) for n in range(width // chunk)]
        mixed = [
            jnp.dot(att[0], w_all[0, :, cols], preferred_element_type=F32).astype(BF16).astype(F32) for cols in spans
        ]
        for d in list(range(2, tp)) + [1]:
            with jax.named_scope("xwait"):
                for e in range(1, dp):
                    for j in range(4):
                        x_copy(d, e, j).wait_recv()
            with jax.named_scope("await"):
                a_copy(d).wait_recv()
            for n, cols in enumerate(spans):
                term = jnp.dot(held[d - 1], w_all[d, :, cols], preferred_element_type=F32)
                mixed[n] = mixed[n] + term.astype(BF16).astype(F32)
        for i in range(len(others)):
            gate_copy(i).wait_recv()
        gate_buf[...] = joined(gathered(gates), 0)
        for n, cols in enumerate(spans):
            out_ref[:, cols] = (tokens_ref[:, cols].astype(F32) + gate_buf[:, cols] * mixed[n]).astype(BF16)

    with jax.named_scope("drain"):
        for cp in mod_copies:
            cp.wait_send()
        for i in range(len(others)):
            gate_copy(i).wait_send()
        for k in range(1, sp):

            @pl.when((s_me >= k - 1) & (s_me < sp - 1))
            def _():
                for cp in ctx_up(k):
                    cp.wait_send()

            @pl.when((s_me + k - 1 <= sp - 1) & (s_me > 0))
            def _():
                for cp in ctx_down(k):
                    cp.wait_send()

        for d in direct:
            q_copy(d).wait_send()
            for j in range(len(mine)):
                w_copy(d, j).wait_send()
            for ds in range(sp):
                kv_mate(ds, d).wait_send()
        if relay:
            for k in range(2):
                q_relay(k).wait_send()
                for j in range(len(mine)):
                    w_relay(j, k).wait_send()
                for ds in range(sp):
                    kv_relay(ds, k).wait_send()
        for d in range(1, tp):
            a_copy(d).wait_send()
            if pair > 1:
                z_copy(d).wait_send()
            for e in range(1, dp):
                for j in range(4):
                    x_copy(d, e, j).wait_send()
        for ds in range(1, sp):
            kv_column(ds).wait_send()


def local(
    sp, tp, dp,
    latent_tokens, condition, shift_weight, scale_weight, gate_weight, norm_gain,
    query_down, query_gain, kv_down, kv_gain, rope_down, query_up, key_up, value_up,
    query_norm_gain, key_norm_gain, out_weight, context_latent, context_rope, context_lift,
):
    rows, width = latent_tokens.shape
    q_rank = query_down.shape[1]
    rank = kv_down.shape[1]
    heads = query_up.shape[1] // QK_DIM
    ctx_rows = context_latent.shape[0]
    group = rows * tp
    tokens = group * sp
    context = sp * ctx_rows
    n_dev = sp * tp
    row_a, row_b = turn_tables(tokens // GRID_W, 0)
    col_a, col_b = turn_tables(GRID_W, 1)
    q_spread = jnp.asarray(query_spread(heads), BF16)
    k_spread = jnp.asarray(head_spread(heads, NOPE_DIM), BF16)
    v_spread = jnp.asarray(head_spread(heads, VALUE_DIM), BF16)
    dma = pltpu.SemaphoreType.DMA
    vmem = pltpu.VMEM
    return pl.pallas_call(
        functools.partial(fused_kernel, sp, tp, dp, heads),
        out_shape=pltpu.VMEM((rows, width), BF16),
        in_specs=[pl.BlockSpec(memory_space=pltpu.SMEM)] + [HBM_SPEC] * 27,
        out_specs=VMEM_SPEC,
        scratch_shapes=[
            vmem((n_dev, 2 * width // tp // LANES, LANES), F32),
            vmem((n_dev, width // tp // LANES, LANES), F32),
            vmem((tp, rows, q_rank), BF16),
            vmem((sp, tp, rows + ROPE_DIM * rows // rank, rank), BF16),
            vmem((sp, ctx_rows, rank), BF16),
            vmem((sp, ROPE_DIM, ctx_rows), BF16),
            vmem((1, width), F32),
            vmem((tokens, LANES), F32),
            vmem((tokens, LANES), F32),
            vmem((8, LANES), F32),
            vmem((heads, group, LANES), BF16),
            vmem((heads, group, LANES), BF16),
            vmem((heads, group, LANES), BF16),
            vmem((heads, context, LANES), BF16),
            vmem((heads, context, LANES), BF16),
            vmem((tp, rows, heads * VALUE_DIM), BF16),
            vmem((tp - 1, rows, heads * VALUE_DIM), BF16),
            vmem((tp,) + out_weight.shape, BF16),
            vmem(shift_weight.shape, BF16),
            vmem(scale_weight.shape, BF16),
            vmem(gate_weight.shape, BF16),
            vmem(latent_tokens.shape, BF16),
            vmem(query_down.shape, BF16),
            vmem(kv_down.shape, BF16),
            vmem(rope_down.shape[::-1], BF16),
            vmem(query_up.shape, BF16),
            vmem(key_up.shape, BF16),
            vmem(value_up.shape, BF16),
            vmem(q_spread.shape, BF16),
            vmem(k_spread.shape, BF16),
            vmem(v_spread.shape, BF16),
            vmem((q_rank, heads * LANES), BF16),
            vmem((rank, heads * LANES), BF16),
            vmem((rank, heads * LANES), BF16),
            vmem(condition.shape, BF16),
            vmem((1, width), F32),
            vmem((1, q_rank), F32),
            vmem((1, rank), F32),
            vmem((1, QK_DIM), F32),
            vmem((1, QK_DIM), F32),
            vmem(row_a.shape, F32),
            vmem(row_a.shape, F32),
            vmem(col_a.shape, F32),
            vmem(col_a.shape, F32),
            vmem((ROPE_DIM, LANES), BF16),
            dma((27,)),
            dma((n_dev - 1,)), dma((n_dev - 1,)),
            dma((n_dev - 1,)), dma((n_dev - 1,)),
            dma((tp,)), dma((tp,)),
            dma((sp, tp + 1)), dma((sp, tp + 1)),
            dma((2, 2 * sp)), dma((2, sp)),
            dma((tp - 1, 4)), dma((tp - 1, 4)),
            dma((4, 2)), dma((4, 2)),
            dma((tp - 1,)), dma((tp - 1,)),
            dma(((tp - 1) * (dp - 1), 4)), dma(((tp - 1) * (dp - 1), 4)),
            dma((tp - 1,)), dma((tp - 1,)),
        ]
        + [vmem((group, LANES), F32)] * (2 * heads),
        compiler_params=pltpu.CompilerParams(
            collective_id=0, has_side_effects=True, vmem_limit_bytes=58 * 1024 * 1024
        ),
        name="fused",
    )(
        context_lift, condition, norm_gain[None], query_gain[None], kv_gain[None], query_norm_gain[None],
        key_norm_gain[None], jnp.asarray(row_a), jnp.asarray(row_b), jnp.asarray(col_a), jnp.asarray(col_b),
        jnp.asarray(rope_spread(), BF16),
        shift_weight, scale_weight, gate_weight, latent_tokens, query_down, kv_down, rope_down.T,
        context_latent, context_rope.T, query_up, key_up, value_up, q_spread, k_spread, v_spread, out_weight,
    )


def solution(mesh):
    in_specs = (
        P(("dp", "sp", "tp"), None), P(("dp", "sp")), P("sp", "tp"), P("sp", "tp"), P("sp", "tp"),
        P(), P(), P(), P(), P(), P(), P(None, "tp"), P(None, "tp"), P(None, "tp"), P(), P(),
        P("tp", None), P(("dp", "sp"), None), P(("dp", "sp"), None), P("tp"),
    )
    out_specs = P(("dp", "sp", "tp"), None)
    body = functools.partial(local, mesh.shape["sp"], mesh.shape["tp"], mesh.shape["dp"])
    return jax.shard_map(body, mesh=mesh, in_specs=in_specs, out_specs=out_specs, check_vma=False)
```

```python
import functools

import jax
import jax.numpy as jnp
import numpy as np
from jax import lax
from jax.experimental import pallas as pl
from jax.experimental.pallas import tpu as pltpu
from jax.sharding import PartitionSpec as P

NOPE_DIM = 64
ROPE_DIM = 32
VALUE_DIM = 64
QK_DIM = 96
GRID_W = 64
LANES = 128

EPS = 1e-06
THETA = 10000.0
LOG2E = 1.4426950408889634
MESH = pl.DeviceIdType.MESH
VMEM_SPEC = pl.BlockSpec(memory_space=pltpu.VMEM)
HBM_SPEC = pl.BlockSpec(memory_space=pltpu.HBM)
BF16 = jnp.bfloat16
F32 = jnp.float32


def partner_order():
    return np.arange(ROPE_DIM) ^ (ROPE_DIM // 4)


def rope_spread():
    spread = np.zeros((ROPE_DIM, LANES), np.float32)
    order = partner_order()
    for j in range(ROPE_DIM):
        spread[j, NOPE_DIM + j] = 1.0
        spread[order[j], QK_DIM + j] = 1.0
    return spread


def query_spread(heads):
    spread = np.zeros((heads * QK_DIM, heads * LANES), np.float32)
    order = partner_order()
    for h in range(heads):
        for j in range(QK_DIM):
            spread[h * QK_DIM + j, h * LANES + j] = 1.0
        for j in range(ROPE_DIM):
            spread[h * QK_DIM + NOPE_DIM + order[j], h * LANES + QK_DIM + j] = 1.0
    return spread


def head_spread(heads, width):
    spread = np.zeros((heads * width, heads * LANES), np.float32)
    for h in range(heads):
        for j in range(width):
            spread[h * width + j, h * LANES + j] = 1.0
    return spread


def turn_tables(count, axis):
    freq_count = ROPE_DIM // 4
    inverse = np.float32(THETA) ** (-np.float32(4.0) * np.arange(freq_count, dtype=np.float32) / np.float32(ROPE_DIM))
    angles = np.arange(count, dtype=np.float32)[:, None] * inverse.astype(np.float32)
    cosine = np.zeros((count, LANES), np.float32)
    sine = np.zeros((count, LANES), np.float32)
    start = NOPE_DIM + axis * 2 * freq_count
    mid = start + freq_count
    cosine[:, start:mid] = np.cos(angles.astype(np.float64))
    cosine[:, mid : mid + freq_count] = np.cos(angles.astype(np.float64))
    sine[:, start:mid] = -np.sin(angles.astype(np.float64))
    sine[:, mid : mid + freq_count] = np.sin(angles.astype(np.float64))
    if axis == 0:
        cosine[:, :NOPE_DIM] = 1.0
    return cosine, sine


def norm_factor(values):
    return lax.rsqrt(jnp.mean(values * values, axis=-1, keepdims=True) + EPS)


def partner(tp, index, d):
    if tp & (tp - 1):
        return lax.rem(index + d, tp)
    result = 0 * index
    bit = 1
    while bit < tp:
        here = lax.rem(index // bit, 2)
        result = result + bit * (lax.rem(here + 1, 2) if d & bit else here)
        bit *= 2
    return result


def fused_kernel(
    sp, tp, dp, heads,
    lift_ref, cond_hbm, gain_hbm, qg_hbm, kg_hbm, qgain_hbm, kgain_hbm, row_a_hbm, row_b_hbm, col_a_hbm, col_b_hbm,
    spread_hbm,
    shift_hbm, scale_hbm, gate_hbm, tokens_hbm, qd_hbm, kd_hbm, rd_hbm, cl_hbm, cr_hbm,
    qu_hbm, ku_hbm, vu_hbm, qe_hbm, ke_hbm, ve_hbm, w_hbm,
    out_ref,
    mods, gates, q_lat, kv, ctx, ctx_rope, gate_buf, tab_a, tab_b, gains, q_all, k_buf, v_buf, k_ctx, v_ctx, att, held,
    w_all, shift_w, scale_w, gate_w, tokens_ref, qd_ref, kd_ref, rd_ref,
    qu_raw, ku_raw, vu_raw, qe_ref, ke_ref, ve_ref, qu_ref, ku_ref, vu_ref,
    cond_ref, gain_ref, qg_ref, kg_ref, qgain_ref, kgain_ref, row_a, row_b, col_a, col_b, spread_ref,
    load_sem, mod_send, mod_recv, g_send, g_recv, q_send, q_recv, kv_send, kv_recv, c_send, c_recv, w_send, w_recv,
    r_send, r_recv, z_send, z_recv, x_send, x_recv, a_send, a_recv, *state,
):
    top_refs, acc_refs = state[:heads], state[heads:]
    s_me = lax.axis_index("sp")
    t_me = lax.axis_index("tp")
    d_me = lax.axis_index("dp")
    me = s_me * tp + t_me
    rows = tokens_ref.shape[0]
    rank = ku_raw.shape[0]
    group = tp * rows
    ctx_rows = cl_hbm.shape[0]
    pair = 2 - sp % 2
    share = w_hbm.shape[0] // dp
    unit = share // 8
    relay = tp == 4
    direct = range(1, 3) if relay else range(1, tp)
    width = w_hbm.shape[1]
    pieces = rank // rows

    def load(i, src, dst):
        cp = pltpu.make_async_copy(src, dst, load_sem.at[i])
        cp.start()
        return cp

    cond_load = load(16, cond_hbm, cond_ref)
    first = [
        load(i, src, dst)
        for i, (src, dst) in enumerate(((shift_hbm, shift_w), (scale_hbm, scale_w), (gate_hbm, gate_w)))
    ]
    ctx_load = [
        load(3, cl_hbm, ctx.at[0]),
        load(4, cr_hbm, ctx_rope.at[0]),
    ]

    def later_loads():
        w_load = load(5, w_hbm, w_all.at[0])
        small_load = [
            load(17 + i, src, dst)
            for i, (src, dst) in enumerate((
                (gain_hbm, gain_ref), (qg_hbm, qg_ref), (kg_hbm, kg_ref), (qgain_hbm, qgain_ref),
                (kgain_hbm, kgain_ref), (row_a_hbm, row_a), (row_b_hbm, row_b), (col_a_hbm, col_a),
                (col_b_hbm, col_b), (spread_hbm, spread_ref),
            ))
        ]
        token_load = load(6, tokens_hbm, tokens_ref)
        up_load = [
            load(10 + i, src, dst)
            for i, (src, dst) in enumerate((
                (qu_hbm, qu_raw), (ku_hbm, ku_raw), (vu_hbm, vu_raw), (qe_hbm, qe_ref), (ke_hbm, ke_ref), (ve_hbm, ve_ref),
            ))
        ]
        down_load = [load(7, qd_hbm, qd_ref), load(8, kd_hbm, kd_ref), load(9, rd_hbm, rd_ref)]
        return w_load, small_load, token_load, up_load, down_load

    def peer(ds, dt):
        return {"sp": lax.rem(s_me + ds, sp), "tp": lax.rem(t_me + dt, tp)}

    def column(ds):
        return {"sp": lax.rem(s_me + ds, sp)}

    def mate(d):
        return {"tp": partner(tp, t_me, d)}

    def twin(e):
        return {"dp": lax.rem(d_me + e, dp)}

    def remote(src, dst, send, recv, device):
        return pltpu.make_async_remote_copy(
            src_ref=src, dst_ref=dst, send_sem=send, recv_sem=recv, device_id=device, device_id_type=MESH
        )

    others = [(ds, dt) for ds in range(sp) for dt in range(tp) if ds or dt]
    barrier = pltpu.get_barrier_semaphore()
    for ds, dt in others:
        pl.semaphore_signal(barrier, inc=1, device_id=peer(ds, dt), device_id_type=MESH)
    for e in range(1, dp):
        pl.semaphore_signal(barrier, inc=1, device_id=twin(e), device_id_type=MESH)

    with jax.named_scope("modmm"):
        cond_load.wait()
        c = cond_ref[...].reshape(1, cond_ref.shape[0]).astype(F32)
        act = (c / (1.0 + jnp.exp(-c))).astype(BF16)
        act = jnp.broadcast_to(act, (16, act.shape[1]))

        def product(i, w):
            first[i].wait()
            term = jnp.dot(act, w[...], preferred_element_type=F32)[0:1]
            return [term[:, c : c + LANES] for c in range(0, term.shape[1], LANES)]

        mods[me] = jnp.concatenate(product(0, shift_w) + product(1, scale_w), axis=0)
        w_load, small_load, token_load, up_load, down_load = later_loads()
        for cp in ctx_load:
            cp.wait()

    with jax.named_scope("barrier"):
        pl.semaphore_wait(barrier, len(others) + dp - 1)
    mod_copies = []
    for i, (ds, dt) in enumerate(others):
        mod_copies.append(remote(mods.at[me], mods.at[me], mod_send.at[i], mod_recv.at[i], peer(ds, dt)))
        mod_copies[-1].start()

    def gate_copy(i):
        return remote(gates.at[me], gates.at[me], g_send.at[i], g_recv.at[i], peer(*others[i]))

    def ctx_up(k):
        device = {"sp": lax.rem(s_me + 1, sp)}
        return [
            remote(buf.at[k - 1], buf.at[k], c_send.at[j, k - 1], c_recv.at[j, k], device)
            for j, buf in enumerate((ctx, ctx_rope))
        ]

    def ctx_down(k):
        device = {"sp": lax.rem(s_me + sp - 1, sp)}
        src = (sp - k + 1) % sp
        return [
            remote(buf.at[src], buf.at[sp - k], c_send.at[j, sp - 2 + k], c_recv.at[j, sp - k], device)
            for j, buf in enumerate((ctx, ctx_rope))
        ]

    def ctx_phase(k, arrive=True, depart=True):
        @pl.when(s_me >= k - 1)
        def _():
            if arrive and k > 1:
                for cp in ctx_up(k - 1):
                    cp.wait_recv()

            @pl.when(s_me < sp - 1)
            def _():
                if depart and k < sp:
                    for cp in ctx_up(k):
                        cp.start()

        @pl.when(s_me + k - 1 <= sp - 1)
        def _():
            if arrive and k > 1:
                for cp in ctx_down(k - 1):
                    cp.wait_recv()

            @pl.when(s_me > 0)
            def _():
                if depart and k < sp:
                    for cp in ctx_down(k):
                        cp.start()

    ctx_phase(1)

    parity = lax.rem(s_me, pair)
    base = d_me * share
    mine = [(parity * 5 * unit, 3 * unit), (3 * unit, 2 * unit)]
    if pair == 1:
        mine = [(0, 3 * unit), (3 * unit, 2 * unit), (5 * unit, 3 * unit)]

    def w_rows(piece):
        offset, size = piece
        return pl.ds(pl.multiple_of(base + offset, unit), size)

    def w_copy(d, j):
        span = w_rows(mine[j])
        return remote(w_all.at[0, span], w_all.at[d, span], w_send.at[d - 1, j], w_recv.at[d - 1, j], mate(d))

    def w_relay(j, k):
        span = w_rows(mine[j])
        cols = pl.ds(k * (width // 2), width // 2)
        return remote(
            w_all.at[1 + k, span, cols], w_all.at[3, span, cols], r_send.at[j, k], r_recv.at[j, k], mate(2 - k)
        )

    def z_copy(d):
        span = w_rows(mine[0])
        device = {"sp": s_me + 1 - 2 * parity}
        return remote(w_all.at[d, span], w_all.at[d, span], z_send.at[d - 1], z_recv.at[d - 1], device)

    def x_copy(d, e, j):
        span = w_rows(mine[j] if j < len(mine) else ((1 - parity) * 5 * unit, 3 * unit))
        i = (d - 1) * (dp - 1) + e - 1
        return remote(w_all.at[d, span], w_all.at[d, span], x_send.at[i, j], x_recv.at[i, j], twin(e))

    def w_arrive(d, j):
        if relay and d == 3:
            for k in range(2):
                w_relay(j, k).wait_recv()
        else:
            w_copy(d, j).wait_recv()

    w_load.wait()
    for d in direct:
        w_copy(d, 0).start()

    with jax.named_scope("prep"):
        gates[me] = jnp.concatenate(product(2, gate_w), axis=0)
        for cp in small_load:
            cp.wait()
        gains[...] = jnp.zeros(gains.shape, F32)
        gains[0:1, :QK_DIM] = qgain_ref[...]
        gains[1:2, :QK_DIM] = kgain_ref[...]
        lane = lax.broadcasted_iota(jnp.int32, (1, LANES), 1)
        freq = ROPE_DIM // 4
        low = lax.rem(lane, 2 * freq) < freq
        live = lane < QK_DIM
        ones_lane = jnp.where(lane == VALUE_DIM, 1.0, 0.0).astype(F32)
        qgain = gains[0:1, :]
        kgain = gains[1:2, :]

        def swap(g):
            return jnp.where(low, pltpu.roll(g, LANES - freq, 1), pltpu.roll(g, freq, 1))

        qgain_swap = swap(qgain)
        kgain_swap = swap(kgain)

        def fill_tables(r, carry):
            span = pl.ds(pl.multiple_of(r * GRID_W, GRID_W), GRID_W)
            tab_a[span, :] = row_a[pl.ds(r, 1), :] + col_a[...]
            tab_b[span, :] = row_b[pl.ds(r, 1), :] + col_b[...]
            return carry

        lax.fori_loop(0, tab_a.shape[0] // GRID_W, fill_tables, 0)
        for cp in up_load:
            cp.wait()
        factor = LOG2E * QK_DIM ** (-0.5)
        qu_ref[...] = jnp.dot(qu_raw[...], qe_ref[...], preferred_element_type=F32).astype(BF16)
        ku_ref[...] = jnp.dot(ku_raw[...], ke_ref[...], preferred_element_type=F32).astype(BF16)
        vu_ref[...] = jnp.dot(vu_raw[...], ve_ref[...], preferred_element_type=F32).astype(BF16)
        spread = spread_ref[...]
        token_load.wait()
        for cp in down_load:
            cp.wait()
        x = tokens_ref[...].astype(F32)
        xn = x * norm_factor(x) * gain_ref[...]

    with jax.named_scope("waitmods"):
        for cp in mod_copies:
            cp.wait_recv()
    def q_copy(d):
        return remote(q_lat.at[0], q_lat.at[d], q_send.at[d - 1], q_recv.at[d - 1], mate(d))

    def q_relay(k):
        cols = pl.ds(k * (q_lat.shape[2] // 2), q_lat.shape[2] // 2)
        return remote(
            q_lat.at[1 + k, :, cols], q_lat.at[3, :, cols], q_send.at[2 + k], q_recv.at[2 + k], mate(2 - k)
        )

    with jax.named_scope("stageB"):

        def gathered(buf):
            rows_of = []
            for t in range(tp):
                total = buf[t]
                for s in range(1, sp):
                    total = total + buf[s * tp + t]
                rows_of.append(total)
            return rows_of

        def joined(totals, start):
            count = width // tp // LANES
            return jnp.concatenate([t[start + c : start + c + 1] for t in totals for c in range(count)], axis=1)

        totals = gathered(mods)
        shift = joined(totals, 0)
        scale = joined(totals, width // tp // LANES)
        normed = (xn * (1.0 + scale) + shift).astype(BF16)
        q = jnp.dot(normed, qd_ref[...], preferred_element_type=F32)
        q_lat[0] = (q * norm_factor(q) * qg_ref[...]).astype(BF16)
        for d in direct:
            q_copy(d).start()
        lat = jnp.dot(normed, kd_ref[...], preferred_element_type=F32)
        kv[0, 0, :rows, :] = (lat * norm_factor(lat) * kg_ref[...]).astype(BF16)
        rope = lax.dot_general(
            rd_ref[...], normed, (((1,), (1,)), ((), ())), preferred_element_type=F32
        ).astype(BF16)
        piece = ROPE_DIM // pieces
        for p in range(pieces):
            kv[0, 0, rows:, p * rows : (p + 1) * rows] = rope[p * piece : (p + 1) * piece]

    def kv_column(ds):
        return remote(kv.at[0, 0], kv.at[ds, 0], kv_send.at[ds, 0], kv_recv.at[ds, 0], column(ds))

    def kv_mate(ds, d):
        return remote(kv.at[ds, 0], kv.at[ds, d], kv_send.at[ds, d], kv_recv.at[ds, d], mate(d))

    def kv_relay(ds, k):
        cols = pl.ds(k * (rank // 2), rank // 2)
        return remote(
            kv.at[ds, 1 + k, :, cols], kv.at[ds, 3, :, cols], kv_send.at[ds, 3 + k], kv_recv.at[ds, 3 + k], mate(2 - k)
        )

    def middle(i):
        return (i + 1) // 2 if i % 2 else sp - i // 2

    def source_step(i):
        return jnp.where(s_me == 0, sp - i, jnp.where(s_me == sp - 1, i, middle(i)))

    def target_step(i):
        return jnp.where(s_me == 0, i, jnp.where(s_me == sp - 1, sp - i, middle(i)))

    for i in range(1, sp):
        kv_column(target_step(i)).start()
    for d in direct:
        kv_mate(0, d).start()

    contract = (((1,), (1,)), ((), ()))

    def expand(lats, ropes, a, b, store):
        rope = [
            lax.dot_general(r, spread, (((0,), (0,)), ((), ())), preferred_element_type=F32) for r in ropes
        ]
        rope = jnp.concatenate(rope, axis=0)
        lat = jnp.concatenate(lats, axis=0)
        k = jnp.dot(lat, ku_ref[...], preferred_element_type=F32)
        v = jnp.dot(lat, vu_ref[...], preferred_element_type=F32)
        k = [k[:, h * LANES : (h + 1) * LANES] for h in range(heads)]
        rope_square = jnp.sum(jnp.where(live, rope * rope, 0.0), axis=-1, keepdims=True)
        squares = [jnp.sum(kh * kh, axis=-1, keepdims=True) + rope_square for kh in k]
        turned = rope * a if b is None else rope * a + pltpu.roll(rope, QK_DIM, 1) * b
        scales = [lax.rsqrt(square * (1.0 / QK_DIM) + EPS) for square in squares]
        for h in range(heads):
            store(
                h, ((k[h] * kgain + turned) * scales[h]).astype(BF16),
                (v[:, h * LANES : (h + 1) * LANES] + ones_lane).astype(BF16),
            )

    def attend(starts, k_ref, v_ref, first_key, keys, lift, fresh, count=None):
        count = count or q_rows
        key_span = pl.ds(first_key, keys)
        items = [(pl.ds(start, count), h) for start in starts for h in range(heads)]

        def product(span, h):
            return lax.dot_general(q_all[h, span, :], k_ref[h, key_span, :], contract, preferred_element_type=F32)

        ahead = 2
        scores = [product(*item) for item in items[:ahead]]
        for i, (span, h) in enumerate(items):
            if i + ahead < len(items):
                scores.append(product(*items[i + ahead]))
            s = scores[i]
            peak = jnp.max(s, axis=-1, keepdims=True)
            if lift:
                lift_h = lift_ref[h] * LOG2E
                peak = peak + lift_h
            if fresh:
                top = jnp.broadcast_to(peak, (count, LANES))
            else:
                old = top_refs[h][span, :]
                top = jnp.maximum(old, peak)
            floor = top - lift_h if lift else top
            p = jnp.exp2(s - jnp.concatenate([floor] * (keys // LANES), axis=1)).astype(BF16)
            add = jnp.dot(p, v_ref[h, key_span, :], preferred_element_type=F32)
            if not fresh:
                add = acc_refs[h][span, :] * jnp.exp2(old - top) + add
            top_refs[h][span, :] = top
            acc_refs[h][span, :] = add

    def expand_context(first, count):
        slots = []
        for i in range(first, first + count):
            if i == 0:
                slots.append(0)
            elif i == 1:
                slots.append(jnp.where(s_me == 0, sp - 1, 1))
            else:
                slots.append(jnp.where(s_me == 0, i - 1, i))

        def store(h, k, v):
            k_ctx[h, first * ctx_rows : (first + count) * ctx_rows, :] = k
            v_ctx[h, first * ctx_rows : (first + count) * ctx_rows, :] = v

        expand([ctx[slot] for slot in slots], [ctx_rope[slot] for slot in slots], kgain, None, store)

    def tables(source, d, gain, gain_swap):
        start = pl.multiple_of((source * tp + (partner(tp, t_me, d) if d else t_me)) * rows, rows)
        return tab_a[pl.ds(start, rows), :] * gain, tab_b[pl.ds(start, rows), :] * gain_swap

    def stacked(pieces_of):
        return [jnp.concatenate(p, axis=0) for p in zip(*pieces_of)]

    def queries(mates):
        a, b = stacked([tables(s_me, d, qgain, qgain_swap) for d in mates])
        qx = jnp.dot(jnp.concatenate([q_lat[d] for d in mates], axis=0), qu_ref[...], preferred_element_type=F32)
        qx = [qx[:, h * LANES : (h + 1) * LANES] for h in range(heads)]
        squares = [jnp.sum(jnp.where(live, v * v, 0.0), axis=-1, keepdims=True) for v in qx]
        turned = [v * a + pltpu.roll(v, QK_DIM, 1) * b for v in qx]
        scales = [lax.rsqrt(square * (1.0 / QK_DIM) + EPS) * factor for square in squares]
        slot = (tp - 1 - mates[0]) * rows
        for h in range(heads):
            q_all[h, slot : slot + len(mates) * rows, :] = (turned[h] * scales[h]).astype(BF16)

    near = min(2, sp)
    near_keys = near * ctx_rows
    far_keys = (sp - near) * ctx_rows
    q_rows = 2 * rows if tp % 2 == 0 else rows

    def kv_relays(i):
        ds = source_step(i) if i else 0
        if relay:
            with jax.named_scope(f"relay{i}"):
                for k in range(2):
                    kv_mate(ds, 1 + k).wait_recv()
                    kv_relay(ds, k).start()

    def kv_forward(i):
        ds = source_step(i)
        with jax.named_scope(f"forward{i}"):
            kv_column(ds).wait_recv()
            for d in direct:
                kv_mate(ds, d).start()

    def w_relays(j):
        if relay:
            with jax.named_scope(f"wrelay{j}"):
                for k in range(2):
                    if j:
                        w_copy(1 + k, j).wait_recv()
                    w_relay(j, k).start()

    def z_start(d):
        if pair > 1:
            with jax.named_scope(f"zstart{d}"):
                if d not in direct:
                    w_arrive(d, 0)
                z_copy(d).start()

    def context_attend(mates):
        with jax.named_scope("ctxattend"):
            attend([(tp - 1 - mates[0]) * rows], k_ctx, v_ctx, 0, near_keys, True, True, len(mates) * rows)

    def a_copy(d):
        return remote(att.at[d], held.at[d - 1], a_send.at[d - 1], a_recv.at[d - 1], mate(d))

    def finish(mates):
        for d in mates:
            slot = (tp - 1 - d) * rows
            outs = []
            for h in range(heads):
                total = acc_refs[h][slot : slot + rows, :]
                outs.append((total[:, :VALUE_DIM] / total[:, VALUE_DIM : VALUE_DIM + 1]).astype(BF16))
            att[d] = jnp.concatenate(outs, axis=1)
            if d:
                a_copy(d).start()

    order = [(i, 0) for i in range(sp)]
    if relay:
        order += [(i, d) for i in range(sp) for d in direct] + [(i, 3) for i in range(sp)]
    else:
        order += [(i, d) for i in range(1, sp) for d in direct] + [(0, d) for d in direct]
    chunks = [order[c : c + tp] for c in range(0, len(order), tp)]

    def chunk_keys(c):
        blocks = [(source_step(i) if i else 0, i, d) for i, d in chunks[c]]
        with jax.named_scope(f"kvwait{c}"):
            for ds, i, d in blocks:
                if relay and d == 3:
                    for k in range(2):
                        kv_relay(ds, k).wait_recv()
                elif d and not relay:
                    kv_mate(ds, d).wait_recv()
        with jax.named_scope("kvexpand"):
            a, b = stacked([tables(lax.rem(s_me + sp - ds, sp), d, kgain, kgain_swap) for ds, i, d in blocks])
            tails = [kv[ds, d, pl.ds(rows, ROPE_DIM // pieces), :] for ds, i, d in blocks]
            ropes = [
                jnp.concatenate([t[:, p * rows : (p + 1) * rows] for p in range(pieces)], axis=0) for t in tails
            ]

            def store(h, k, v):
                k_buf[h] = k
                v_buf[h] = v

            expand([kv[ds, d, pl.ds(0, rows), :] for ds, i, d in blocks], ropes, a, b, store)

    def chunk_attend():
        with jax.named_scope("attend"):
            attend(range(0, group, q_rows), k_buf, v_buf, 0, group, False, False)

    with jax.named_scope("queries"):
        queries([0])
    with jax.named_scope("ctxwait"):
        ctx_phase(2, depart=False)
    with jax.named_scope("ctxexpand"):
        expand_context(0, near)
    context_attend([0])
    with jax.named_scope("qwait"):
        for d in direct:
            q_copy(d).wait_recv()
            if relay:
                q_relay(d - 1).start()
    ctx_phase(2, arrive=False)
    for d in direct:
        w_copy(d, 0).wait_recv()
    z_start(1)
    with jax.named_scope("queries"):
        queries(list(reversed(direct)))
    kv_relays(0)
    for i in range(1, min(2, sp)):
        kv_forward(i)
    context_attend(list(reversed(direct)))
    if relay:
        with jax.named_scope("qwait3"):
            for k in range(2):
                q_relay(k).wait_recv()
        with jax.named_scope("queries"):
            queries([3])
        context_attend([3])
    for i in range(2, sp):
        kv_forward(i)
    w_relays(0)
    def swap_twin(d, j):
        for e in range(1, dp):
            x_copy(d, e, j).start()

    def swap_pair(d):
        if pair > 1:
            z_copy(d).wait_recv()
            swap_twin(d, len(mine))

    last = len(chunks) - 1
    relayed = [1]

    def relays_to(i):
        while relay and relayed[0] <= i:
            kv_relays(relayed[0])
            relayed[0] += 1

    for c in range(len(chunks)):
        if c:
            relays_to(sp - 1 if any(d == 3 for i, d in chunks[c]) else max(i for i, d in chunks[c]))
        if c == last:
            if far_keys:
                with jax.named_scope("ctxwait4"):
                    for k in range(4, sp + 1):
                        ctx_phase(k)
                with jax.named_scope("ctxexpand"):
                    expand_context(near, sp - near)
                with jax.named_scope("ctxattend"):
                    attend(range(0, group, q_rows), k_ctx, v_ctx, near_keys, far_keys, True, False)
            if relay:
                for j in range(1, len(mine)):
                    w_relays(j)
                    for d in direct:
                        swap_twin(d, j)
            with jax.named_scope("pair1"):
                swap_pair(1)
        chunk_keys(c)
        if c < last:
            chunk_attend()
        if c == 0:
            with jax.named_scope("ctxwait3"):
                ctx_phase(3)
            for d in direct:
                if d > 1:
                    z_start(d)
        if c == min(1, last):
            relays_to(sp - 1)
            for j in range(1, len(mine)):
                for d in direct:
                    w_copy(d, j).start()
            for i in range(len(others)):
                gate_copy(i).start()
            for d in range(1, tp):
                if d in direct:
                    swap_twin(d, 0)
        if c == max(min(1, last), last - 1):
            for d in range(1, tp):
                if d not in direct:
                    z_start(d)

    with jax.named_scope("attendlast"):
        for mates in [list(range(tp - 1, 1, -1)), [1], [0]]:
            attend([(tp - 1 - mates[0]) * rows], k_buf, v_buf, 0, group, False, False, len(mates) * rows)
            finish(mates)

    with jax.named_scope("wtwin"):
        for d in range(1, tp):
            for j in range(len(mine)):
                if d not in direct:
                    if j or pair == 1:
                        w_arrive(d, j)
                    swap_twin(d, j)
                elif j and not relay:
                    w_arrive(d, j)
                    swap_twin(d, j)
            if d > 1:
                swap_pair(d)

    with jax.named_scope("tail"):
        chunk = 512
        spans = [slice(n * chunk, (n + 1) * chunk) for n in range(width // chunk)]
        mixed = [
            jnp.dot(att[0], w_all[0, :, cols], preferred_element_type=F32).astype(BF16).astype(F32) for cols in spans
        ]
        for d in list(range(2, tp)) + [1]:
            with jax.named_scope("xwait"):
                for e in range(1, dp):
                    for j in range(3):
                        x_copy(d, e, j).wait_recv()
            with jax.named_scope("await"):
                a_copy(d).wait_recv()
            for n, cols in enumerate(spans):
                term = jnp.dot(held[d - 1], w_all[d, :, cols], preferred_element_type=F32)
                mixed[n] = mixed[n] + term.astype(BF16).astype(F32)
        for i in range(len(others)):
            gate_copy(i).wait_recv()
        gate_buf[...] = joined(gathered(gates), 0)
        for n, cols in enumerate(spans):
            out_ref[:, cols] = (tokens_ref[:, cols].astype(F32) + gate_buf[:, cols] * mixed[n]).astype(BF16)

    with jax.named_scope("drain"):
        for cp in mod_copies:
            cp.wait_send()
        for i in range(len(others)):
            gate_copy(i).wait_send()
        for k in range(1, sp):

            @pl.when((s_me >= k - 1) & (s_me < sp - 1))
            def _():
                for cp in ctx_up(k):
                    cp.wait_send()

            @pl.when((s_me + k - 1 <= sp - 1) & (s_me > 0))
            def _():
                for cp in ctx_down(k):
                    cp.wait_send()

        for d in direct:
            q_copy(d).wait_send()
            for j in range(len(mine)):
                w_copy(d, j).wait_send()
            for ds in range(sp):
                kv_mate(ds, d).wait_send()
        if relay:
            for k in range(2):
                q_relay(k).wait_send()
                for j in range(len(mine)):
                    w_relay(j, k).wait_send()
                for ds in range(sp):
                    kv_relay(ds, k).wait_send()
        for d in range(1, tp):
            a_copy(d).wait_send()
            if pair > 1:
                z_copy(d).wait_send()
            for e in range(1, dp):
                for j in range(3):
                    x_copy(d, e, j).wait_send()
        for ds in range(1, sp):
            kv_column(ds).wait_send()


def local(
    sp, tp, dp,
    latent_tokens, condition, shift_weight, scale_weight, gate_weight, norm_gain,
    query_down, query_gain, kv_down, kv_gain, rope_down, query_up, key_up, value_up,
    query_norm_gain, key_norm_gain, out_weight, context_latent, context_rope, context_lift,
):
    rows, width = latent_tokens.shape
    q_rank = query_down.shape[1]
    rank = kv_down.shape[1]
    heads = query_up.shape[1] // QK_DIM
    ctx_rows = context_latent.shape[0]
    group = rows * tp
    tokens = group * sp
    context = sp * ctx_rows
    n_dev = sp * tp
    row_a, row_b = turn_tables(tokens // GRID_W, 0)
    col_a, col_b = turn_tables(GRID_W, 1)
    q_spread = jnp.asarray(query_spread(heads), BF16)
    k_spread = jnp.asarray(head_spread(heads, NOPE_DIM), BF16)
    v_spread = jnp.asarray(head_spread(heads, VALUE_DIM), BF16)
    dma = pltpu.SemaphoreType.DMA
    vmem = pltpu.VMEM
    return pl.pallas_call(
        functools.partial(fused_kernel, sp, tp, dp, heads),
        out_shape=pltpu.VMEM((rows, width), BF16),
        in_specs=[pl.BlockSpec(memory_space=pltpu.SMEM)] + [HBM_SPEC] * 27,
        out_specs=VMEM_SPEC,
        scratch_shapes=[
            vmem((n_dev, 2 * width // tp // LANES, LANES), F32),
            vmem((n_dev, width // tp // LANES, LANES), F32),
            vmem((tp, rows, q_rank), BF16),
            vmem((sp, tp, rows + ROPE_DIM * rows // rank, rank), BF16),
            vmem((sp, ctx_rows, rank), BF16),
            vmem((sp, ROPE_DIM, ctx_rows), BF16),
            vmem((1, width), F32),
            vmem((tokens, LANES), F32),
            vmem((tokens, LANES), F32),
            vmem((8, LANES), F32),
            vmem((heads, group, LANES), BF16),
            vmem((heads, group, LANES), BF16),
            vmem((heads, group, LANES), BF16),
            vmem((heads, context, LANES), BF16),
            vmem((heads, context, LANES), BF16),
            vmem((tp, rows, heads * VALUE_DIM), BF16),
            vmem((tp - 1, rows, heads * VALUE_DIM), BF16),
            vmem((tp,) + out_weight.shape, BF16),
            vmem(shift_weight.shape, BF16),
            vmem(scale_weight.shape, BF16),
            vmem(gate_weight.shape, BF16),
            vmem(latent_tokens.shape, BF16),
            vmem(query_down.shape, BF16),
            vmem(kv_down.shape, BF16),
            vmem(rope_down.shape[::-1], BF16),
            vmem(query_up.shape, BF16),
            vmem(key_up.shape, BF16),
            vmem(value_up.shape, BF16),
            vmem(q_spread.shape, BF16),
            vmem(k_spread.shape, BF16),
            vmem(v_spread.shape, BF16),
            vmem((q_rank, heads * LANES), BF16),
            vmem((rank, heads * LANES), BF16),
            vmem((rank, heads * LANES), BF16),
            vmem(condition.shape, BF16),
            vmem((1, width), F32),
            vmem((1, q_rank), F32),
            vmem((1, rank), F32),
            vmem((1, QK_DIM), F32),
            vmem((1, QK_DIM), F32),
            vmem(row_a.shape, F32),
            vmem(row_a.shape, F32),
            vmem(col_a.shape, F32),
            vmem(col_a.shape, F32),
            vmem((ROPE_DIM, LANES), BF16),
            dma((27,)),
            dma((n_dev - 1,)), dma((n_dev - 1,)),
            dma((n_dev - 1,)), dma((n_dev - 1,)),
            dma((tp,)), dma((tp,)),
            dma((sp, tp + 1)), dma((sp, tp + 1)),
            dma((2, 2 * sp)), dma((2, sp)),
            dma((tp - 1, 4)), dma((tp - 1, 4)),
            dma((4, 2)), dma((4, 2)),
            dma((tp - 1,)), dma((tp - 1,)),
            dma(((tp - 1) * (dp - 1), 4)), dma(((tp - 1) * (dp - 1), 4)),
            dma((tp - 1,)), dma((tp - 1,)),
        ]
        + [vmem((group, LANES), F32)] * (2 * heads),
        compiler_params=pltpu.CompilerParams(
            collective_id=0, has_side_effects=True, vmem_limit_bytes=58 * 1024 * 1024
        ),
        name="fused",
    )(
        context_lift, condition, norm_gain[None], query_gain[None], kv_gain[None], query_norm_gain[None],
        key_norm_gain[None], jnp.asarray(row_a), jnp.asarray(row_b), jnp.asarray(col_a), jnp.asarray(col_b),
        jnp.asarray(rope_spread(), BF16),
        shift_weight, scale_weight, gate_weight, latent_tokens, query_down, kv_down, rope_down.T,
        context_latent, context_rope.T, query_up, key_up, value_up, q_spread, k_spread, v_spread, out_weight,
    )


def solution(mesh):
    in_specs = (
        P(("dp", "sp", "tp"), None), P(("dp", "sp")), P("sp", "tp"), P("sp", "tp"), P("sp", "tp"),
        P(), P(), P(), P(), P(), P(), P(None, "tp"), P(None, "tp"), P(None, "tp"), P(), P(),
        P("tp", None), P(("dp", "sp"), None), P(("dp", "sp"), None), P("tp"),
    )
    out_specs = P(("dp", "sp", "tp"), None)
    body = functools.partial(local, mesh.shape["sp"], mesh.shape["tp"], mesh.shape["dp"])
    return jax.shard_map(body, mesh=mesh, in_specs=in_specs, out_specs=out_specs, check_vma=False)
```

```python
import functools

import jax
import jax.numpy as jnp
import numpy as np
from jax import lax
from jax.experimental import pallas as pl
from jax.experimental.pallas import tpu as pltpu
from jax.sharding import PartitionSpec as P

NOPE_DIM = 64
ROPE_DIM = 32
VALUE_DIM = 64
QK_DIM = 96
GRID_W = 64
LANES = 128

EPS = 1e-06
THETA = 10000.0
LOG2E = 1.4426950408889634
MESH = pl.DeviceIdType.MESH
VMEM_SPEC = pl.BlockSpec(memory_space=pltpu.VMEM)
HBM_SPEC = pl.BlockSpec(memory_space=pltpu.HBM)
BF16 = jnp.bfloat16
F32 = jnp.float32


def partner_order():
    return np.arange(ROPE_DIM) ^ (ROPE_DIM // 4)


def rope_spread():
    spread = np.zeros((ROPE_DIM, LANES), np.float32)
    order = partner_order()
    for j in range(ROPE_DIM):
        spread[j, NOPE_DIM + j] = 1.0
        spread[order[j], QK_DIM + j] = 1.0
    return spread


def query_spread(heads):
    spread = np.zeros((heads * QK_DIM, heads * LANES), np.float32)
    order = partner_order()
    for h in range(heads):
        for j in range(QK_DIM):
            spread[h * QK_DIM + j, h * LANES + j] = 1.0
        for j in range(ROPE_DIM):
            spread[h * QK_DIM + NOPE_DIM + order[j], h * LANES + QK_DIM + j] = 1.0
    return spread


def head_spread(heads, width):
    spread = np.zeros((heads * width, heads * LANES), np.float32)
    for h in range(heads):
        for j in range(width):
            spread[h * width + j, h * LANES + j] = 1.0
    return spread


def turn_tables(count, axis):
    freq_count = ROPE_DIM // 4
    inverse = np.float32(THETA) ** (-np.float32(4.0) * np.arange(freq_count, dtype=np.float32) / np.float32(ROPE_DIM))
    angles = np.arange(count, dtype=np.float32)[:, None] * inverse.astype(np.float32)
    cosine = np.zeros((count, LANES), np.float32)
    sine = np.zeros((count, LANES), np.float32)
    start = NOPE_DIM + axis * 2 * freq_count
    mid = start + freq_count
    cosine[:, start:mid] = np.cos(angles.astype(np.float64))
    cosine[:, mid : mid + freq_count] = np.cos(angles.astype(np.float64))
    sine[:, start:mid] = -np.sin(angles.astype(np.float64))
    sine[:, mid : mid + freq_count] = np.sin(angles.astype(np.float64))
    if axis == 0:
        cosine[:, :NOPE_DIM] = 1.0
    return cosine, sine


def norm_factor(values):
    return lax.rsqrt(jnp.mean(values * values, axis=-1, keepdims=True) + EPS)


def partner(tp, index, d):
    if tp & (tp - 1):
        return lax.rem(index + d, tp)
    result = 0 * index
    bit = 1
    while bit < tp:
        here = lax.rem(index // bit, 2)
        result = result + bit * (lax.rem(here + 1, 2) if d & bit else here)
        bit *= 2
    return result


def fused_kernel(
    sp, tp, dp, heads,
    lift_hbm, cond_hbm, gain_hbm, qg_hbm, kg_hbm, qgain_hbm, kgain_hbm, row_a_hbm, row_b_hbm, col_a_hbm, col_b_hbm,
    spread_hbm,
    shift_hbm, scale_hbm, gate_hbm, tokens_hbm, qd_hbm, kd_hbm, rd_hbm, cl_hbm, cr_hbm,
    qu_hbm, ku_hbm, vu_hbm, qe_hbm, ke_hbm, ve_hbm, w_hbm,
    out_ref,
    mods, gates, q_lat, kv, ctx, ctx_rope, gate_buf, tab_a, tab_b, gains, q_all, k_buf, v_buf, k_ctx, v_ctx, att, held,
    w_all, shift_w, scale_w, gate_w, tokens_ref, qd_ref, kd_ref, rd_ref,
    qu_raw, ku_raw, vu_raw, qe_ref, ke_ref, ve_ref, qu_ref, ku_ref, vu_ref,
    lift_ref, cond_ref, gain_ref, qg_ref, kg_ref, qgain_ref, kgain_ref, row_a, row_b, col_a, col_b, spread_ref,
    load_sem, mod_send, mod_recv, g_send, g_recv, q_send, q_recv, kv_send, kv_recv, c_send, c_recv, w_send, w_recv,
    r_send, r_recv, z_send, z_recv, x_send, x_recv, a_send, a_recv, *state,
):
    top_refs, acc_refs = state[:heads], state[heads:]
    s_me = lax.axis_index("sp")
    t_me = lax.axis_index("tp")
    d_me = lax.axis_index("dp")
    me = s_me * tp + t_me
    rows = tokens_ref.shape[0]
    rank = ku_raw.shape[0]
    group = tp * rows
    ctx_rows = cl_hbm.shape[0]
    pair = 2 - sp % 2
    share = w_hbm.shape[0] // dp
    unit = share // 8
    relay = tp == 4
    direct = range(1, 3) if relay else range(1, tp)
    width = w_hbm.shape[1]
    pieces = rank // rows

    def load(i, src, dst):
        cp = pltpu.make_async_copy(src, dst, load_sem.at[i])
        cp.start()
        return cp

    cond_load = load(16, cond_hbm, cond_ref)
    first = [
        load(i, src, dst)
        for i, (src, dst) in enumerate(((shift_hbm, shift_w), (scale_hbm, scale_w), (gate_hbm, gate_w)))
    ]
    ctx_load = [
        load(3, cl_hbm, ctx.at[0]),
        load(4, cr_hbm, ctx_rope.at[0]),
    ]

    def later_loads():
        w_load = load(5, w_hbm, w_all.at[0])
        small_load = [
            load(17 + i, src, dst)
            for i, (src, dst) in enumerate((
                (gain_hbm, gain_ref), (qg_hbm, qg_ref), (kg_hbm, kg_ref), (qgain_hbm, qgain_ref),
                (kgain_hbm, kgain_ref), (row_a_hbm, row_a), (row_b_hbm, row_b), (col_a_hbm, col_a),
                (col_b_hbm, col_b), (spread_hbm, spread_ref), (lift_hbm, lift_ref),
            ))
        ]
        token_load = load(6, tokens_hbm, tokens_ref)
        up_load = [
            load(10 + i, src, dst)
            for i, (src, dst) in enumerate((
                (qu_hbm, qu_raw), (ku_hbm, ku_raw), (vu_hbm, vu_raw), (qe_hbm, qe_ref), (ke_hbm, ke_ref), (ve_hbm, ve_ref),
            ))
        ]
        down_load = [load(7, qd_hbm, qd_ref), load(8, kd_hbm, kd_ref), load(9, rd_hbm, rd_ref)]
        return w_load, small_load, token_load, up_load, down_load

    def peer(ds, dt):
        return {"sp": lax.rem(s_me + ds, sp), "tp": lax.rem(t_me + dt, tp)}

    def column(ds):
        return {"sp": lax.rem(s_me + ds, sp)}

    def mate(d):
        return {"tp": partner(tp, t_me, d)}

    def twin(e):
        return {"dp": lax.rem(d_me + e, dp)}

    def remote(src, dst, send, recv, device):
        return pltpu.make_async_remote_copy(
            src_ref=src, dst_ref=dst, send_sem=send, recv_sem=recv, device_id=device, device_id_type=MESH
        )

    others = [(ds, dt) for ds in range(sp) for dt in range(tp) if ds or dt]
    barrier = pltpu.get_barrier_semaphore()
    for ds, dt in others:
        pl.semaphore_signal(barrier, inc=1, device_id=peer(ds, dt), device_id_type=MESH)
    for e in range(1, dp):
        pl.semaphore_signal(barrier, inc=1, device_id=twin(e), device_id_type=MESH)

    with jax.named_scope("modmm"):
        cond_load.wait()
        c = cond_ref[...].reshape(1, cond_ref.shape[0]).astype(F32)
        act = (c / (1.0 + jnp.exp(-c))).astype(BF16)
        act = jnp.broadcast_to(act, (16, act.shape[1]))

        def product(i, w):
            first[i].wait()
            term = jnp.dot(act, w[...], preferred_element_type=F32)[0:1]
            return [term[:, c : c + LANES] for c in range(0, term.shape[1], LANES)]

        mods[me] = jnp.concatenate(product(0, shift_w) + product(1, scale_w), axis=0)
        w_load, small_load, token_load, up_load, down_load = later_loads()
        for cp in ctx_load:
            cp.wait()

    with jax.named_scope("barrier"):
        pl.semaphore_wait(barrier, len(others) + dp - 1)
    mod_copies = []
    for i, (ds, dt) in enumerate(others):
        mod_copies.append(remote(mods.at[me], mods.at[me], mod_send.at[i], mod_recv.at[i], peer(ds, dt)))
        mod_copies[-1].start()

    def gate_copy(i):
        return remote(gates.at[me], gates.at[me], g_send.at[i], g_recv.at[i], peer(*others[i]))

    def ctx_up(k):
        device = {"sp": lax.rem(s_me + 1, sp)}
        return [
            remote(buf.at[k - 1], buf.at[k], c_send.at[j, k - 1], c_recv.at[j, k], device)
            for j, buf in enumerate((ctx, ctx_rope))
        ]

    def ctx_down(k):
        device = {"sp": lax.rem(s_me + sp - 1, sp)}
        src = (sp - k + 1) % sp
        return [
            remote(buf.at[src], buf.at[sp - k], c_send.at[j, sp - 2 + k], c_recv.at[j, sp - k], device)
            for j, buf in enumerate((ctx, ctx_rope))
        ]

    def ctx_phase(k, arrive=True, depart=True):
        @pl.when(s_me >= k - 1)
        def _():
            if arrive and k > 1:
                for cp in ctx_up(k - 1):
                    cp.wait_recv()

            @pl.when(s_me < sp - 1)
            def _():
                if depart and k < sp:
                    for cp in ctx_up(k):
                        cp.start()

        @pl.when(s_me + k - 1 <= sp - 1)
        def _():
            if arrive and k > 1:
                for cp in ctx_down(k - 1):
                    cp.wait_recv()

            @pl.when(s_me > 0)
            def _():
                if depart and k < sp:
                    for cp in ctx_down(k):
                        cp.start()

    ctx_phase(1)

    parity = lax.rem(s_me, pair)
    base = d_me * share
    mine = [(parity * 5 * unit, 3 * unit), (3 * unit, 2 * unit)]
    if pair == 1:
        mine = [(0, 3 * unit), (3 * unit, 2 * unit), (5 * unit, 3 * unit)]

    def w_rows(piece):
        offset, size = piece
        return pl.ds(pl.multiple_of(base + offset, unit), size)

    def w_copy(d, j):
        span = w_rows(mine[j])
        return remote(w_all.at[0, span], w_all.at[d, span], w_send.at[d - 1, j], w_recv.at[d - 1, j], mate(d))

    def w_relay(j, k):
        span = w_rows(mine[j])
        cols = pl.ds(k * (width // 2), width // 2)
        return remote(
            w_all.at[1 + k, span, cols], w_all.at[3, span, cols], r_send.at[j, k], r_recv.at[j, k], mate(2 - k)
        )

    def z_copy(d):
        span = w_rows(mine[0])
        device = {"sp": s_me + 1 - 2 * parity}
        return remote(w_all.at[d, span], w_all.at[d, span], z_send.at[d - 1], z_recv.at[d - 1], device)

    def x_copy(d, e, j):
        span = w_rows(mine[j] if j < len(mine) else ((1 - parity) * 5 * unit, 3 * unit))
        i = (d - 1) * (dp - 1) + e - 1
        return remote(w_all.at[d, span], w_all.at[d, span], x_send.at[i, j], x_recv.at[i, j], twin(e))

    def w_arrive(d, j):
        if relay and d == 3:
            for k in range(2):
                w_relay(j, k).wait_recv()
        else:
            w_copy(d, j).wait_recv()

    w_load.wait()
    for d in direct:
        w_copy(d, 0).start()

    with jax.named_scope("prep"):
        gates[me] = jnp.concatenate(product(2, gate_w), axis=0)
        for cp in small_load:
            cp.wait()
        gains[...] = jnp.zeros(gains.shape, F32)
        gains[0:1, :QK_DIM] = qgain_ref[...]
        gains[1:2, :QK_DIM] = kgain_ref[...]
        for h in range(heads):
            gains[2 + h : 3 + h, :] = jnp.broadcast_to(lift_ref[0:1, h : h + 1] * LOG2E, (1, LANES))
        lane = lax.broadcasted_iota(jnp.int32, (1, LANES), 1)
        freq = ROPE_DIM // 4
        low = lax.rem(lane, 2 * freq) < freq
        live = lane < QK_DIM
        ones_lane = jnp.where(lane == VALUE_DIM, 1.0, 0.0).astype(F32)
        qgain = gains[0:1, :]
        kgain = gains[1:2, :]

        def swap(g):
            return jnp.where(low, pltpu.roll(g, LANES - freq, 1), pltpu.roll(g, freq, 1))

        qgain_swap = swap(qgain)
        kgain_swap = swap(kgain)

        def fill_tables(r, carry):
            span = pl.ds(pl.multiple_of(r * GRID_W, GRID_W), GRID_W)
            tab_a[span, :] = row_a[pl.ds(r, 1), :] + col_a[...]
            tab_b[span, :] = row_b[pl.ds(r, 1), :] + col_b[...]
            return carry

        lax.fori_loop(0, tab_a.shape[0] // GRID_W, fill_tables, 0)
        for cp in up_load:
            cp.wait()
        factor = LOG2E * QK_DIM ** (-0.5)
        qu_ref[...] = jnp.dot(qu_raw[...], qe_ref[...], preferred_element_type=F32).astype(BF16)
        ku_ref[...] = jnp.dot(ku_raw[...], ke_ref[...], preferred_element_type=F32).astype(BF16)
        vu_ref[...] = jnp.dot(vu_raw[...], ve_ref[...], preferred_element_type=F32).astype(BF16)
        spread = spread_ref[...]
        token_load.wait()
        for cp in down_load:
            cp.wait()
        x = tokens_ref[...].astype(F32)
        xn = x * norm_factor(x) * gain_ref[...]

    with jax.named_scope("waitmods"):
        for cp in mod_copies:
            cp.wait_recv()
    q_half = q_lat.shape[2] // 2

    def q_copy(d, k):
        cols = pl.ds(k * q_half, q_half)
        i = (d - 1) * 2 + k
        return remote(q_lat.at[0, :, cols], q_lat.at[d, :, cols], q_send.at[i], q_recv.at[i], mate(d))

    def q_relay(k):
        cols = pl.ds(k * q_half, q_half)
        return remote(
            q_lat.at[1 + k, :, cols], q_lat.at[3, :, cols], q_send.at[4 + k], q_recv.at[4 + k], mate(2 - k)
        )

    with jax.named_scope("stageB"):

        def gathered(buf):
            rows_of = []
            for t in range(tp):
                total = buf[t]
                for s in range(1, sp):
                    total = total + buf[s * tp + t]
                rows_of.append(total)
            return rows_of

        def joined(totals, start):
            count = width // tp // LANES
            return jnp.concatenate([t[start + c : start + c + 1] for t in totals for c in range(count)], axis=1)

        totals = gathered(mods)
        shift = joined(totals, 0)
        scale = joined(totals, width // tp // LANES)
        normed = (xn * (1.0 + scale) + shift).astype(BF16)
        q = jnp.dot(normed, qd_ref[...], preferred_element_type=F32)
        q_lat[0] = (q * norm_factor(q) * qg_ref[...]).astype(BF16)
        for k in range(2):
            for d in direct:
                q_copy(d, (d - 1 + k) % 2).start()
        lat = jnp.dot(normed, kd_ref[...], preferred_element_type=F32)
        kv[0, 0, :rows, :] = (lat * norm_factor(lat) * kg_ref[...]).astype(BF16)
        rope = lax.dot_general(
            rd_ref[...], normed, (((1,), (1,)), ((), ())), preferred_element_type=F32
        ).astype(BF16)
        piece = ROPE_DIM // pieces
        for p in range(pieces):
            kv[0, 0, rows:, p * rows : (p + 1) * rows] = rope[p * piece : (p + 1) * piece]

    def kv_column(ds):
        return remote(kv.at[0, 0], kv.at[ds, 0], kv_send.at[ds, 0], kv_recv.at[ds, 0], column(ds))

    def kv_mate(ds, d):
        return remote(kv.at[ds, 0], kv.at[ds, d], kv_send.at[ds, d], kv_recv.at[ds, d], mate(d))

    def kv_relay(ds, k):
        cols = pl.ds(k * (rank // 2), rank // 2)
        return remote(
            kv.at[ds, 1 + k, :, cols], kv.at[ds, 3, :, cols], kv_send.at[ds, 3 + k], kv_recv.at[ds, 3 + k], mate(2 - k)
        )

    def middle(i):
        return (i + 1) // 2 if i % 2 else sp - i // 2

    def source_step(i):
        return jnp.where(s_me == 0, sp - i, jnp.where(s_me == sp - 1, i, middle(i)))

    def target_step(i):
        return jnp.where(s_me == 0, i, jnp.where(s_me == sp - 1, sp - i, middle(i)))

    for i in range(1, sp):
        kv_column(target_step(i)).start()
    contract = (((1,), (1,)), ((), ()))

    def expand(lats, ropes, a, b, store):
        rope = [
            lax.dot_general(r, spread, (((0,), (0,)), ((), ())), preferred_element_type=F32) for r in ropes
        ]
        rope = jnp.concatenate(rope, axis=0)
        lat = jnp.concatenate(lats, axis=0)
        k = jnp.dot(lat, ku_ref[...], preferred_element_type=F32)
        v = jnp.dot(lat, vu_ref[...], preferred_element_type=F32)
        k = [k[:, h * LANES : (h + 1) * LANES] for h in range(heads)]
        rope_square = jnp.sum(jnp.where(live, rope * rope, 0.0), axis=-1, keepdims=True)
        squares = [jnp.sum(kh * kh, axis=-1, keepdims=True) + rope_square for kh in k]
        turned = rope * a if b is None else rope * a + pltpu.roll(rope, QK_DIM, 1) * b
        scales = [lax.rsqrt(square * (1.0 / QK_DIM) + EPS) for square in squares]
        for h in range(heads):
            store(
                h, ((k[h] * kgain + turned) * scales[h]).astype(BF16),
                (v[:, h * LANES : (h + 1) * LANES] + ones_lane).astype(BF16),
            )

    def attend(parts_of, k_ref, v_ref, first_key, keys, lift, fresh, after=None):
        key_span = pl.ds(first_key, keys)
        items = [(pl.ds(*part), h) for part in parts_of for h in range(heads)]

        def product(span, h):
            return lax.dot_general(q_all[h, span, :], k_ref[h, key_span, :], contract, preferred_element_type=F32)

        ahead = 2
        scores = [product(*item) for item in items[:ahead]]
        for i, (span, h) in enumerate(items):
            count = span.size
            if i + ahead < len(items):
                scores.append(product(*items[i + ahead]))
            s = scores[i]
            peak = jnp.max(s, axis=-1, keepdims=True)
            if lift:
                lift_h = gains[2 + h : 3 + h, :]
                peak = peak + lift_h
            if fresh:
                top = jnp.broadcast_to(peak, (count, LANES)) if not lift else peak
            else:
                old = top_refs[h][span, :]
                top = jnp.maximum(old, peak)
            floor = top - lift_h if lift else top
            p = jnp.exp2(s - jnp.concatenate([floor] * (keys // LANES), axis=1)).astype(BF16)
            add = jnp.dot(p, v_ref[h, key_span, :], preferred_element_type=F32)
            if not fresh:
                add = acc_refs[h][span, :] * jnp.exp2(old - top) + add
            top_refs[h][span, :] = top
            acc_refs[h][span, :] = add
            if after and h == heads - 1:
                after(i // heads)

    def expand_context(first, count):
        slots = []
        for i in range(first, first + count):
            if i == 0:
                slots.append(0)
            elif i == 1:
                slots.append(jnp.where(s_me == 0, sp - 1, 1))
            else:
                slots.append(jnp.where(s_me == 0, i - 1, i))

        def store(h, k, v):
            k_ctx[h, first * ctx_rows : (first + count) * ctx_rows, :] = k
            v_ctx[h, first * ctx_rows : (first + count) * ctx_rows, :] = v

        expand([ctx[slot] for slot in slots], [ctx_rope[slot] for slot in slots], kgain, None, store)

    def tables(source, d, gain, gain_swap):
        start = pl.multiple_of((source * tp + (partner(tp, t_me, d) if d else t_me)) * rows, rows)
        return tab_a[pl.ds(start, rows), :] * gain, tab_b[pl.ds(start, rows), :] * gain_swap

    def stacked(pieces_of):
        return [jnp.concatenate(p, axis=0) for p in zip(*pieces_of)]

    def queries(mates):
        a, b = stacked([tables(s_me, d, qgain, qgain_swap) for d in mates])
        qx = jnp.dot(jnp.concatenate([q_lat[d] for d in mates], axis=0), qu_ref[...], preferred_element_type=F32)
        qx = [qx[:, h * LANES : (h + 1) * LANES] for h in range(heads)]
        squares = [jnp.sum(jnp.where(live, v * v, 0.0), axis=-1, keepdims=True) for v in qx]
        turned = [v * a + pltpu.roll(v, QK_DIM, 1) * b for v in qx]
        scales = [lax.rsqrt(square * (1.0 / QK_DIM) + EPS) * factor for square in squares]
        slot = (tp - 1 - mates[0]) * rows
        for h in range(heads):
            q_all[h, slot : slot + len(mates) * rows, :] = (turned[h] * scales[h]).astype(BF16)

    near = min(2, sp)
    near_keys = near * ctx_rows
    far_keys = (sp - near) * ctx_rows
    q_rows = 2 * rows if tp % 2 == 0 else rows

    def kv_relays(i):
        ds = source_step(i) if i else 0
        if relay:
            with jax.named_scope(f"relay{i}"):
                for k in range(2):
                    kv_mate(ds, 1 + k).wait_recv()
                    kv_relay(ds, k).start()

    def kv_forward(i):
        ds = source_step(i)
        with jax.named_scope(f"forward{i}"):
            kv_column(ds).wait_recv()
            for d in direct:
                kv_mate(ds, d).start()

    def w_relays(j):
        if relay:
            with jax.named_scope(f"wrelay{j}"):
                for k in range(2):
                    if j:
                        w_copy(1 + k, j).wait_recv()
                    w_relay(j, k).start()

    def z_start(d):
        if pair > 1:
            with jax.named_scope(f"zstart{d}"):
                if d not in direct:
                    w_arrive(d, 0)
                z_copy(d).start()

    def mate_rows(mates):
        return (tp - 1 - mates[0]) * rows, len(mates) * rows

    all_rows = [(start, q_rows) for start in range(0, group, q_rows)]

    def context_attend(mates):
        with jax.named_scope("ctxattend"):
            attend([mate_rows(mates)], k_ctx, v_ctx, 0, near_keys, True, True)

    def a_copy(d):
        return remote(att.at[d], held.at[d - 1], a_send.at[d - 1], a_recv.at[d - 1], mate(d))

    def finish(mates):
        for d in mates:
            slot = (tp - 1 - d) * rows
            outs = []
            for h in range(heads):
                total = acc_refs[h][slot : slot + rows, :]
                outs.append((total[:, :VALUE_DIM] / total[:, VALUE_DIM : VALUE_DIM + 1]).astype(BF16))
            att[d] = jnp.concatenate(outs, axis=1)
            if d:
                a_copy(d).start()

    order = [(i, 0) for i in range(sp)]
    if relay:
        order += [(i, d) for i in range(sp) for d in direct] + [(i, 3) for i in range(sp)]
    else:
        order += [(i, d) for i in range(1, sp) for d in direct] + [(0, d) for d in direct]
    chunks = [order[c : c + tp] for c in range(0, len(order), tp)]

    def chunk_keys(c):
        blocks = [(source_step(i) if i else 0, i, d) for i, d in chunks[c]]
        with jax.named_scope(f"kvwait{c}"):
            for ds, i, d in blocks:
                if relay and d == 3:
                    for k in range(2):
                        kv_relay(ds, k).wait_recv()
                elif d and not relay:
                    kv_mate(ds, d).wait_recv()
        with jax.named_scope("kvexpand"):
            a, b = stacked([tables(lax.rem(s_me + sp - ds, sp), d, kgain, kgain_swap) for ds, i, d in blocks])
            tails = [kv[ds, d, pl.ds(rows, ROPE_DIM // pieces), :] for ds, i, d in blocks]
            ropes = [
                jnp.concatenate([t[:, p * rows : (p + 1) * rows] for p in range(pieces)], axis=0) for t in tails
            ]

            def store(h, k, v):
                k_buf[h] = k
                v_buf[h] = v

            expand([kv[ds, d, pl.ds(0, rows), :] for ds, i, d in blocks], ropes, a, b, store)

    def chunk_attend():
        with jax.named_scope("attend"):
            attend(all_rows, k_buf, v_buf, 0, group, False, False)

    with jax.named_scope("queries"):
        queries([0])
    with jax.named_scope("ctxwait"):
        ctx_phase(2)
    with jax.named_scope("ctxexpand"):
        expand_context(0, near)
    context_attend([0])
    with jax.named_scope("qwait"):
        for d in direct:
            q_copy(d, (d - 1) % 2).wait_recv()
            if relay:
                q_relay(d - 1).start()
        for d in direct:
            kv_mate(0, d).start()
    with jax.named_scope("qwait2"):
        for d in direct:
            q_copy(d, d % 2).wait_recv()
    for d in direct:
        w_copy(d, 0).wait_recv()
    z_start(1)
    with jax.named_scope("queries"):
        queries(list(reversed(direct)))
    for i in range(1, min(2, sp)):
        kv_forward(i)
    w_relays(0)
    context_attend(list(reversed(direct)))
    if relay:
        with jax.named_scope("qwait3"):
            for k in range(2):
                q_relay(k).wait_recv()
        with jax.named_scope("queries"):
            queries([3])
        context_attend([3])
    for i in range(2, sp):
        kv_forward(i)
    kv_relays(0)
    def swap_twin(d, j):
        for e in range(1, dp):
            x_copy(d, e, j).start()

    def swap_pair(d):
        if pair > 1:
            z_copy(d).wait_recv()
            swap_twin(d, len(mine))

    last = len(chunks) - 1
    relayed = [1]

    def relays_to(i):
        while relay and relayed[0] <= i:
            kv_relays(relayed[0])
            relayed[0] += 1

    for c in range(len(chunks)):
        if c:
            relays_to(sp - 1 if any(d == 3 for i, d in chunks[c]) else max(i for i, d in chunks[c]))
        if c == last:
            if far_keys:
                with jax.named_scope("ctxwait4"):
                    for k in range(4, sp + 1):
                        ctx_phase(k)
                with jax.named_scope("ctxexpand"):
                    expand_context(near, sp - near)
            for d in range(1, tp):
                if d not in direct:
                    z_start(d)
            if far_keys:
                with jax.named_scope("ctxattend"):
                    attend(all_rows, k_ctx, v_ctx, near_keys, far_keys, True, False)
            if relay:
                for j in range(1, len(mine)):
                    w_relays(j)
                    for d in direct:
                        swap_twin(d, j)
            with jax.named_scope("pair1"):
                swap_pair(1)
        chunk_keys(c)
        if c == 0:
            with jax.named_scope("ctxwait3"):
                ctx_phase(3)
            for d in direct:
                if d > 1:
                    z_start(d)
        if c < last:
            chunk_attend()
        if c == min(1, last):
            relays_to(min(2, sp - 1))
            for j in range(1, len(mine)):
                for d in direct:
                    w_copy(d, j).start()
            for i in range(len(others)):
                gate_copy(i).start()
            for d in range(1, tp):
                if d in direct:
                    swap_twin(d, 0)

    with jax.named_scope("attendlast"):
        turns = [list(range(tp - 1, 1, -1)), [1], [0]]
        attend(
            [mate_rows(mates) for mates in turns], k_buf, v_buf, 0, group, False, False,
            lambda i: finish(turns[i]),
        )

    with jax.named_scope("wtwin"):
        for d in range(1, tp):
            for j in range(len(mine)):
                if d not in direct:
                    if j or pair == 1:
                        w_arrive(d, j)
                    swap_twin(d, j)
                elif j and not relay:
                    w_arrive(d, j)
                    swap_twin(d, j)
            if d > 1:
                swap_pair(d)

    with jax.named_scope("tail"):
        chunk = 512
        spans = [slice(n * chunk, (n + 1) * chunk) for n in range(width // chunk)]
        mixed = [
            jnp.dot(att[0], w_all[0, :, cols], preferred_element_type=F32).astype(BF16).astype(F32) for cols in spans
        ]
        for d in list(range(2, tp)) + [1]:
            with jax.named_scope("xwait"):
                for e in range(1, dp):
                    for j in range(3):
                        x_copy(d, e, j).wait_recv()
            with jax.named_scope("await"):
                a_copy(d).wait_recv()
            for n, cols in enumerate(spans):
                term = jnp.dot(held[d - 1], w_all[d, :, cols], preferred_element_type=F32)
                mixed[n] = mixed[n] + term.astype(BF16).astype(F32)
        for i in range(len(others)):
            gate_copy(i).wait_recv()
        gate_buf[...] = joined(gathered(gates), 0)
        for n, cols in enumerate(spans):
            out_ref[:, cols] = (tokens_ref[:, cols].astype(F32) + gate_buf[:, cols] * mixed[n]).astype(BF16)

    with jax.named_scope("drain"):
        for cp in mod_copies:
            cp.wait_send()
        for i in range(len(others)):
            gate_copy(i).wait_send()
        for k in range(1, sp):

            @pl.when((s_me >= k - 1) & (s_me < sp - 1))
            def _():
                for cp in ctx_up(k):
                    cp.wait_send()

            @pl.when((s_me + k - 1 <= sp - 1) & (s_me > 0))
            def _():
                for cp in ctx_down(k):
                    cp.wait_send()

        for d in direct:
            for k in range(2):
                q_copy(d, k).wait_send()
            for j in range(len(mine)):
                w_copy(d, j).wait_send()
            for ds in range(sp):
                kv_mate(ds, d).wait_send()
        if relay:
            for k in range(2):
                q_relay(k).wait_send()
                for j in range(len(mine)):
                    w_relay(j, k).wait_send()
                for ds in range(sp):
                    kv_relay(ds, k).wait_send()
        for d in range(1, tp):
            a_copy(d).wait_send()
            if pair > 1:
                z_copy(d).wait_send()
            for e in range(1, dp):
                for j in range(3):
                    x_copy(d, e, j).wait_send()
        for ds in range(1, sp):
            kv_column(ds).wait_send()


def local(
    sp, tp, dp,
    latent_tokens, condition, shift_weight, scale_weight, gate_weight, norm_gain,
    query_down, query_gain, kv_down, kv_gain, rope_down, query_up, key_up, value_up,
    query_norm_gain, key_norm_gain, out_weight, context_latent, context_rope, context_lift,
):
    rows, width = latent_tokens.shape
    q_rank = query_down.shape[1]
    rank = kv_down.shape[1]
    heads = query_up.shape[1] // QK_DIM
    ctx_rows = context_latent.shape[0]
    group = rows * tp
    tokens = group * sp
    context = sp * ctx_rows
    n_dev = sp * tp
    row_a, row_b = turn_tables(tokens // GRID_W, 0)
    col_a, col_b = turn_tables(GRID_W, 1)
    q_spread = jnp.asarray(query_spread(heads), BF16)
    k_spread = jnp.asarray(head_spread(heads, NOPE_DIM), BF16)
    v_spread = jnp.asarray(head_spread(heads, VALUE_DIM), BF16)
    dma = pltpu.SemaphoreType.DMA
    vmem = pltpu.VMEM
    return pl.pallas_call(
        functools.partial(fused_kernel, sp, tp, dp, heads),
        out_shape=pltpu.VMEM((rows, width), BF16),
        in_specs=[HBM_SPEC] * 28,
        out_specs=VMEM_SPEC,
        scratch_shapes=[
            vmem((n_dev, 2 * width // tp // LANES, LANES), F32),
            vmem((n_dev, width // tp // LANES, LANES), F32),
            vmem((tp, rows, q_rank), BF16),
            vmem((sp, tp, rows + ROPE_DIM * rows // rank, rank), BF16),
            vmem((sp, ctx_rows, rank), BF16),
            vmem((sp, ROPE_DIM, ctx_rows), BF16),
            vmem((1, width), F32),
            vmem((tokens, LANES), F32),
            vmem((tokens, LANES), F32),
            vmem((8 * ((heads + 9) // 8), LANES), F32),
            vmem((heads, group, LANES), BF16),
            vmem((heads, group, LANES), BF16),
            vmem((heads, group, LANES), BF16),
            vmem((heads, context, LANES), BF16),
            vmem((heads, context, LANES), BF16),
            vmem((tp, rows, heads * VALUE_DIM), BF16),
            vmem((tp - 1, rows, heads * VALUE_DIM), BF16),
            vmem((tp,) + out_weight.shape, BF16),
            vmem(shift_weight.shape, BF16),
            vmem(scale_weight.shape, BF16),
            vmem(gate_weight.shape, BF16),
            vmem(latent_tokens.shape, BF16),
            vmem(query_down.shape, BF16),
            vmem(kv_down.shape, BF16),
            vmem(rope_down.shape[::-1], BF16),
            vmem(query_up.shape, BF16),
            vmem(key_up.shape, BF16),
            vmem(value_up.shape, BF16),
            vmem(q_spread.shape, BF16),
            vmem(k_spread.shape, BF16),
            vmem(v_spread.shape, BF16),
            vmem((q_rank, heads * LANES), BF16),
            vmem((rank, heads * LANES), BF16),
            vmem((rank, heads * LANES), BF16),
            vmem((1, heads), F32),
            vmem(condition.shape, BF16),
            vmem((1, width), F32),
            vmem((1, q_rank), F32),
            vmem((1, rank), F32),
            vmem((1, QK_DIM), F32),
            vmem((1, QK_DIM), F32),
            vmem(row_a.shape, F32),
            vmem(row_a.shape, F32),
            vmem(col_a.shape, F32),
            vmem(col_a.shape, F32),
            vmem((ROPE_DIM, LANES), BF16),
            dma((28,)),
            dma((n_dev - 1,)), dma((n_dev - 1,)),
            dma((n_dev - 1,)), dma((n_dev - 1,)),
            dma((2 * tp,)), dma((2 * tp,)),
            dma((sp, tp + 1)), dma((sp, tp + 1)),
            dma((2, 2 * sp)), dma((2, sp)),
            dma((tp - 1, 4)), dma((tp - 1, 4)),
            dma((4, 2)), dma((4, 2)),
            dma((tp - 1,)), dma((tp - 1,)),
            dma(((tp - 1) * (dp - 1), 4)), dma(((tp - 1) * (dp - 1), 4)),
            dma((tp - 1,)), dma((tp - 1,)),
        ]
        + [vmem((group, LANES), F32)] * (2 * heads),
        compiler_params=pltpu.CompilerParams(
            collective_id=0, has_side_effects=True, vmem_limit_bytes=58 * 1024 * 1024
        ),
        name="fused",
    )(
        context_lift[None], condition, norm_gain[None], query_gain[None], kv_gain[None], query_norm_gain[None],
        key_norm_gain[None], jnp.asarray(row_a), jnp.asarray(row_b), jnp.asarray(col_a), jnp.asarray(col_b),
        jnp.asarray(rope_spread(), BF16),
        shift_weight, scale_weight, gate_weight, latent_tokens, query_down, kv_down, rope_down.T,
        context_latent, context_rope.T, query_up, key_up, value_up, q_spread, k_spread, v_spread, out_weight,
    )


def solution(mesh):
    in_specs = (
        P(("dp", "sp", "tp"), None), P(("dp", "sp")), P("sp", "tp"), P("sp", "tp"), P("sp", "tp"),
        P(), P(), P(), P(), P(), P(), P(None, "tp"), P(None, "tp"), P(None, "tp"), P(), P(),
        P("tp", None), P(("dp", "sp"), None), P(("dp", "sp"), None), P("tp"),
    )
    out_specs = P(("dp", "sp", "tp"), None)
    body = functools.partial(local, mesh.shape["sp"], mesh.shape["tp"], mesh.shape["dp"])
    return jax.shard_map(body, mesh=mesh, in_specs=in_specs, out_specs=out_specs, check_vma=False)
```

```python
import functools

import jax
import jax.numpy as jnp
import numpy as np
from jax import lax
from jax.experimental import pallas as pl
from jax.experimental.pallas import tpu as pltpu
from jax.sharding import PartitionSpec as P

NOPE_DIM = 64
ROPE_DIM = 32
VALUE_DIM = 64
QK_DIM = 96
GRID_W = 64
LANES = 128

EPS = 1e-06
THETA = 10000.0
LOG2E = 1.4426950408889634
MESH = pl.DeviceIdType.MESH
VMEM_SPEC = pl.BlockSpec(memory_space=pltpu.VMEM)
HBM_SPEC = pl.BlockSpec(memory_space=pltpu.HBM)
BF16 = jnp.bfloat16
F32 = jnp.float32


def partner_order():
    return np.arange(ROPE_DIM) ^ (ROPE_DIM // 4)


def rope_spread():
    spread = np.zeros((ROPE_DIM, LANES), np.float32)
    order = partner_order()
    for j in range(ROPE_DIM):
        spread[j, NOPE_DIM + j] = 1.0
        spread[order[j], QK_DIM + j] = 1.0
    return spread


def query_spread(heads):
    spread = np.zeros((heads * QK_DIM, heads * LANES), np.float32)
    order = partner_order()
    for h in range(heads):
        for j in range(QK_DIM):
            spread[h * QK_DIM + j, h * LANES + j] = 1.0
        for j in range(ROPE_DIM):
            spread[h * QK_DIM + NOPE_DIM + order[j], h * LANES + QK_DIM + j] = 1.0
    return spread


def head_spread(heads, width):
    spread = np.zeros((heads * width, heads * LANES), np.float32)
    for h in range(heads):
        for j in range(width):
            spread[h * width + j, h * LANES + j] = 1.0
    return spread


def turn_tables(count, axis):
    freq_count = ROPE_DIM // 4
    inverse = np.float32(THETA) ** (-np.float32(4.0) * np.arange(freq_count, dtype=np.float32) / np.float32(ROPE_DIM))
    angles = np.arange(count, dtype=np.float32)[:, None] * inverse.astype(np.float32)
    cosine = np.zeros((count, LANES), np.float32)
    sine = np.zeros((count, LANES), np.float32)
    start = NOPE_DIM + axis * 2 * freq_count
    mid = start + freq_count
    cosine[:, start:mid] = np.cos(angles.astype(np.float64))
    cosine[:, mid : mid + freq_count] = np.cos(angles.astype(np.float64))
    sine[:, start:mid] = -np.sin(angles.astype(np.float64))
    sine[:, mid : mid + freq_count] = np.sin(angles.astype(np.float64))
    if axis == 0:
        cosine[:, :NOPE_DIM] = 1.0
    return cosine, sine


def norm_factor(values):
    return lax.rsqrt(jnp.mean(values * values, axis=-1, keepdims=True) + EPS)


def partner(tp, index, d):
    if tp & (tp - 1):
        return lax.rem(index + d, tp)
    result = 0 * index
    bit = 1
    while bit < tp:
        here = lax.rem(index // bit, 2)
        result = result + bit * (lax.rem(here + 1, 2) if d & bit else here)
        bit *= 2
    return result


def fused_kernel(
    sp, tp, dp, heads,
    lift_hbm, cond_hbm, gain_hbm, qg_hbm, kg_hbm, qgain_hbm, kgain_hbm, row_a_hbm, row_b_hbm, col_a_hbm, col_b_hbm,
    spread_hbm,
    shift_hbm, scale_hbm, gate_hbm, tokens_hbm, qd_hbm, kd_hbm, rd_hbm, cl_hbm, cr_hbm,
    qu_hbm, ku_hbm, vu_hbm, qe_hbm, ke_hbm, ve_hbm, w_hbm,
    out_ref,
    mods, gates, q_lat, kv, ctx, ctx_rope, gate_buf, tab_a, tab_b, gains, q_all, k_buf, v_buf, k_ctx, v_ctx, att, held,
    w_all, shift_w, scale_w, gate_w, tokens_ref, qd_ref, kd_ref, rd_ref,
    qu_raw, ku_raw, vu_raw, qe_ref, ke_ref, ve_ref, qu_ref, ku_ref, vu_ref,
    lift_ref, cond_ref, gain_ref, qg_ref, kg_ref, qgain_ref, kgain_ref, row_a, row_b, col_a, col_b, spread_ref,
    load_sem, mod_send, mod_recv, g_send, g_recv, q_send, q_recv, kv_send, kv_recv, c_send, c_recv, w_send, w_recv,
    r_send, r_recv, z_send, z_recv, x_send, x_recv, a_send, a_recv, *state,
):
    top_refs, acc_refs = state[:heads], state[heads:]
    s_me = lax.axis_index("sp")
    t_me = lax.axis_index("tp")
    d_me = lax.axis_index("dp")
    me = s_me * tp + t_me
    rows = tokens_ref.shape[0]
    rank = ku_raw.shape[0]
    group = tp * rows
    ctx_rows = cl_hbm.shape[0]
    pair = 2 - sp % 2
    share = w_hbm.shape[0] // dp
    unit = share // 8
    relay = tp == 4
    direct = range(1, 3) if relay else range(1, tp)
    width = w_hbm.shape[1]
    pieces = rank // rows

    def load(i, src, dst):
        cp = pltpu.make_async_copy(src, dst, load_sem.at[i])
        cp.start()
        return cp

    cond_load = load(16, cond_hbm, cond_ref)
    first = [
        load(i, src, dst)
        for i, (src, dst) in enumerate(((shift_hbm, shift_w), (scale_hbm, scale_w), (gate_hbm, gate_w)))
    ]
    ctx_load = [
        load(3, cl_hbm, ctx.at[0]),
        load(4, cr_hbm, ctx_rope.at[0]),
    ]

    def later_loads():
        w_load = load(5, w_hbm, w_all.at[0])
        small_load = [
            load(17 + i, src, dst)
            for i, (src, dst) in enumerate((
                (gain_hbm, gain_ref), (qg_hbm, qg_ref), (kg_hbm, kg_ref), (qgain_hbm, qgain_ref),
                (kgain_hbm, kgain_ref), (row_a_hbm, row_a), (row_b_hbm, row_b), (col_a_hbm, col_a),
                (col_b_hbm, col_b), (spread_hbm, spread_ref), (lift_hbm, lift_ref),
            ))
        ]
        token_load = load(6, tokens_hbm, tokens_ref)
        up_load = [
            load(10 + i, src, dst)
            for i, (src, dst) in enumerate((
                (qu_hbm, qu_raw), (ku_hbm, ku_raw), (vu_hbm, vu_raw), (qe_hbm, qe_ref), (ke_hbm, ke_ref), (ve_hbm, ve_ref),
            ))
        ]
        down_load = [load(7, qd_hbm, qd_ref), load(8, kd_hbm, kd_ref), load(9, rd_hbm, rd_ref)]
        return w_load, small_load, token_load, up_load, down_load

    def peer(ds, dt):
        return {"sp": lax.rem(s_me + ds, sp), "tp": lax.rem(t_me + dt, tp)}

    def column(ds):
        return {"sp": lax.rem(s_me + ds, sp)}

    def mate(d):
        return {"tp": partner(tp, t_me, d)}

    def twin(e):
        return {"dp": lax.rem(d_me + e, dp)}

    def remote(src, dst, send, recv, device):
        return pltpu.make_async_remote_copy(
            src_ref=src, dst_ref=dst, send_sem=send, recv_sem=recv, device_id=device, device_id_type=MESH
        )

    others = [(ds, dt) for ds in range(sp) for dt in range(tp) if ds or dt]
    barrier = pltpu.get_barrier_semaphore()
    for ds, dt in others:
        pl.semaphore_signal(barrier, inc=1, device_id=peer(ds, dt), device_id_type=MESH)
    for e in range(1, dp):
        pl.semaphore_signal(barrier, inc=1, device_id=twin(e), device_id_type=MESH)

    with jax.named_scope("modmm"):
        cond_load.wait()
        c = cond_ref[...].reshape(1, cond_ref.shape[0]).astype(F32)
        act = (c / (1.0 + jnp.exp(-c))).astype(BF16)
        act = jnp.broadcast_to(act, (16, act.shape[1]))

        def product(i, w):
            first[i].wait()
            term = jnp.dot(act, w[...], preferred_element_type=F32)[0:1]
            return [term[:, c : c + LANES] for c in range(0, term.shape[1], LANES)]

        mods[me] = jnp.concatenate(product(0, shift_w) + product(1, scale_w), axis=0)
        w_load, small_load, token_load, up_load, down_load = later_loads()
        for cp in ctx_load:
            cp.wait()

    with jax.named_scope("barrier"):
        pl.semaphore_wait(barrier, len(others) + dp - 1)
    mod_copies = []
    for i, (ds, dt) in enumerate(others):
        mod_copies.append(remote(mods.at[me], mods.at[me], mod_send.at[0], mod_recv.at[0], peer(ds, dt)))
        mod_copies[-1].start()

    def gate_copy(i):
        return remote(gates.at[me], gates.at[me], g_send.at[0], g_recv.at[0], peer(*others[i]))

    every = pl.ds(0, len(others))

    def all_mods():
        return remote(mods.at[every], mods.at[every], mod_send.at[0], mod_recv.at[0], peer(*others[0]))

    def all_gates():
        return remote(gates.at[every], gates.at[every], g_send.at[0], g_recv.at[0], peer(*others[0]))

    def ctx_up(k):
        device = {"sp": lax.rem(s_me + 1, sp)}
        return [
            remote(buf.at[k - 1], buf.at[k], c_send.at[j, k - 1], c_recv.at[j, k], device)
            for j, buf in enumerate((ctx, ctx_rope))
        ]

    def ctx_down(k):
        device = {"sp": lax.rem(s_me + sp - 1, sp)}
        src = (sp - k + 1) % sp
        return [
            remote(buf.at[src], buf.at[sp - k], c_send.at[j, sp - 2 + k], c_recv.at[j, sp - k], device)
            for j, buf in enumerate((ctx, ctx_rope))
        ]

    def ctx_phase(k, arrive=True, depart=True):
        @pl.when(s_me >= k - 1)
        def _():
            if arrive and k > 1:
                for cp in ctx_up(k - 1):
                    cp.wait_recv()

            @pl.when(s_me < sp - 1)
            def _():
                if depart and k < sp:
                    for cp in ctx_up(k):
                        cp.start()

        @pl.when(s_me + k - 1 <= sp - 1)
        def _():
            if arrive and k > 1:
                for cp in ctx_down(k - 1):
                    cp.wait_recv()

            @pl.when(s_me > 0)
            def _():
                if depart and k < sp:
                    for cp in ctx_down(k):
                        cp.start()

    ctx_phase(1)

    parity = lax.rem(s_me, pair)
    base = d_me * share
    mine = [(parity * 5 * unit, 3 * unit), (3 * unit, 2 * unit)]
    if pair == 1:
        mine = [(0, 3 * unit), (3 * unit, 2 * unit), (5 * unit, 3 * unit)]

    def w_rows(piece):
        offset, size = piece
        return pl.ds(pl.multiple_of(base + offset, unit), size)

    def w_copy(d, j):
        span = w_rows(mine[j])
        return remote(w_all.at[0, span], w_all.at[d, span], w_send.at[d - 1, j], w_recv.at[d - 1, j], mate(d))

    def w_relay(j, k):
        span = w_rows(mine[j])
        cols = pl.ds(k * (width // 2), width // 2)
        return remote(
            w_all.at[1 + k, span, cols], w_all.at[3, span, cols], r_send.at[j, k], r_recv.at[j, k], mate(2 - k)
        )

    def z_copy(d):
        span = w_rows(mine[0])
        device = {"sp": s_me + 1 - 2 * parity}
        return remote(w_all.at[d, span], w_all.at[d, span], z_send.at[d - 1], z_recv.at[d - 1], device)

    def x_copy(d, e, j):
        span = w_rows(mine[j] if j < len(mine) else ((1 - parity) * 5 * unit, 3 * unit))
        i = (d - 1) * (dp - 1) + e - 1
        return remote(w_all.at[d, span], w_all.at[d, span], x_send.at[i, j], x_recv.at[i, j], twin(e))

    def w_arrive(d, j):
        if relay and d == 3:
            for k in range(2):
                w_relay(j, k).wait_recv()
        else:
            w_copy(d, j).wait_recv()

    w_load.wait()
    for d in direct:
        w_copy(d, 0).start()

    with jax.named_scope("prep"):
        gates[me] = jnp.concatenate(product(2, gate_w), axis=0)
        for cp in small_load:
            cp.wait()
        gains[...] = jnp.zeros(gains.shape, F32)
        gains[0:1, :QK_DIM] = qgain_ref[...]
        gains[1:2, :QK_DIM] = kgain_ref[...]
        for h in range(heads):
            gains[2 + h : 3 + h, :] = jnp.broadcast_to(lift_ref[0:1, h : h + 1] * LOG2E, (1, LANES))
        lane = lax.broadcasted_iota(jnp.int32, (1, LANES), 1)
        freq = ROPE_DIM // 4
        low = lax.rem(lane, 2 * freq) < freq
        live = lane < QK_DIM
        ones_lane = jnp.where(lane == VALUE_DIM, 1.0, 0.0).astype(F32)
        qgain = gains[0:1, :]
        kgain = gains[1:2, :]

        def swap(g):
            return jnp.where(low, pltpu.roll(g, LANES - freq, 1), pltpu.roll(g, freq, 1))

        qgain_swap = swap(qgain)
        kgain_swap = swap(kgain)

        def fill_tables(r, carry):
            span = pl.ds(pl.multiple_of(r * GRID_W, GRID_W), GRID_W)
            tab_a[span, :] = row_a[pl.ds(r, 1), :] + col_a[...]
            tab_b[span, :] = row_b[pl.ds(r, 1), :] + col_b[...]
            return carry

        lax.fori_loop(0, tab_a.shape[0] // GRID_W, fill_tables, 0)
        for cp in up_load:
            cp.wait()
        factor = LOG2E * QK_DIM ** (-0.5)
        qu_ref[...] = jnp.dot(qu_raw[...], qe_ref[...], preferred_element_type=F32).astype(BF16)
        ku_ref[...] = jnp.dot(ku_raw[...], ke_ref[...], preferred_element_type=F32).astype(BF16)
        vu_ref[...] = jnp.dot(vu_raw[...], ve_ref[...], preferred_element_type=F32).astype(BF16)
        spread = spread_ref[...]
        token_load.wait()
        for cp in down_load:
            cp.wait()
        x = tokens_ref[...].astype(F32)
        xn = x * norm_factor(x) * gain_ref[...]

    with jax.named_scope("waitmods"):
        all_mods().wait_recv()
    q_half = q_lat.shape[2] // 2

    def q_copy(d, k):
        cols = pl.ds(k * q_half, q_half)
        i = (d - 1) * 2 + k
        return remote(q_lat.at[0, :, cols], q_lat.at[d, :, cols], q_send.at[i], q_recv.at[i], mate(d))

    def q_relay(k):
        cols = pl.ds(k * q_half, q_half)
        return remote(
            q_lat.at[1 + k, :, cols], q_lat.at[3, :, cols], q_send.at[4 + k], q_recv.at[4 + k], mate(2 - k)
        )

    with jax.named_scope("stageB"):

        def gathered(buf):
            rows_of = []
            for t in range(tp):
                total = buf[t]
                for s in range(1, sp):
                    total = total + buf[s * tp + t]
                rows_of.append(total)
            return rows_of

        def joined(totals, start):
            count = width // tp // LANES
            return jnp.concatenate([t[start + c : start + c + 1] for t in totals for c in range(count)], axis=1)

        totals = gathered(mods)
        shift = joined(totals, 0)
        scale = joined(totals, width // tp // LANES)
        normed = (xn * (1.0 + scale) + shift).astype(BF16)
        q = jnp.dot(normed, qd_ref[...], preferred_element_type=F32)
        q_lat[0] = (q * norm_factor(q) * qg_ref[...]).astype(BF16)
        for k in range(2):
            for d in direct:
                q_copy(d, (d - 1 + k) % 2).start()
        lat = jnp.dot(normed, kd_ref[...], preferred_element_type=F32)
        kv[0, 0, :rows, :] = (lat * norm_factor(lat) * kg_ref[...]).astype(BF16)
        rope = lax.dot_general(
            rd_ref[...], normed, (((1,), (1,)), ((), ())), preferred_element_type=F32
        ).astype(BF16)
        piece = ROPE_DIM // pieces
        for p in range(pieces):
            kv[0, 0, rows:, p * rows : (p + 1) * rows] = rope[p * piece : (p + 1) * piece]

    def kv_column(ds):
        return remote(kv.at[0, 0], kv.at[ds, 0], kv_send.at[ds, 0], kv_recv.at[ds, 0], column(ds))

    def kv_mate(ds, d):
        return remote(kv.at[ds, 0], kv.at[ds, d], kv_send.at[ds, d], kv_recv.at[ds, d], mate(d))

    def kv_relay(ds, k):
        cols = pl.ds(k * (rank // 2), rank // 2)
        return remote(
            kv.at[ds, 1 + k, :, cols], kv.at[ds, 3, :, cols], kv_send.at[ds, 3 + k], kv_recv.at[ds, 3 + k], mate(2 - k)
        )

    def middle(i):
        return (i + 1) // 2 if i % 2 else sp - i // 2

    def source_step(i):
        return jnp.where(s_me == 0, sp - i, jnp.where(s_me == sp - 1, i, middle(i)))

    def target_step(i):
        return jnp.where(s_me == 0, i, jnp.where(s_me == sp - 1, sp - i, middle(i)))

    for i in range(1, sp):
        kv_column(target_step(i)).start()
    contract = (((1,), (1,)), ((), ()))

    def expand(lats, ropes, a, b, store):
        rope = [
            lax.dot_general(r, spread, (((0,), (0,)), ((), ())), preferred_element_type=F32) for r in ropes
        ]
        rope = jnp.concatenate(rope, axis=0)
        lat = jnp.concatenate(lats, axis=0)
        k = jnp.dot(lat, ku_ref[...], preferred_element_type=F32)
        v = jnp.dot(lat, vu_ref[...], preferred_element_type=F32)
        k = [k[:, h * LANES : (h + 1) * LANES] for h in range(heads)]
        rope_square = jnp.sum(jnp.where(live, rope * rope, 0.0), axis=-1, keepdims=True)
        squares = [jnp.sum(kh * kh, axis=-1, keepdims=True) + rope_square for kh in k]
        turned = rope * a if b is None else rope * a + pltpu.roll(rope, QK_DIM, 1) * b
        scales = [lax.rsqrt(square * (1.0 / QK_DIM) + EPS) for square in squares]
        for h in range(heads):
            store(
                h, ((k[h] * kgain + turned) * scales[h]).astype(BF16),
                (v[:, h * LANES : (h + 1) * LANES] + ones_lane).astype(BF16),
            )

    def attend(parts_of, k_ref, v_ref, first_key, keys, lift, fresh, after=None):
        key_span = pl.ds(first_key, keys)
        items = [(pl.ds(*part), h) for part in parts_of for h in range(heads)]

        def product(span, h):
            return lax.dot_general(q_all[h, span, :], k_ref[h, key_span, :], contract, preferred_element_type=F32)

        ahead = 3
        scores = [product(*item) for item in items[:ahead]]
        for i, (span, h) in enumerate(items):
            count = span.size
            if i + ahead < len(items):
                scores.append(product(*items[i + ahead]))
            s = scores[i]
            peak = jnp.max(s, axis=-1, keepdims=True)
            if lift:
                lift_h = gains[2 + h : 3 + h, :]
                peak = peak + lift_h
            if fresh:
                top = jnp.broadcast_to(peak, (count, LANES)) if not lift else peak
            else:
                old = top_refs[h][span, :]
                top = jnp.maximum(old, peak)
            floor = top - lift_h if lift else top
            p = jnp.exp2(s - jnp.concatenate([floor] * (keys // LANES), axis=1)).astype(BF16)
            add = jnp.dot(p, v_ref[h, key_span, :], preferred_element_type=F32)
            if not fresh:
                add = acc_refs[h][span, :] * jnp.exp2(old - top) + add
            top_refs[h][span, :] = top
            acc_refs[h][span, :] = add
            if after and h == heads - 1:
                after(i // heads)

    def expand_context(first, count):
        slots = []
        for i in range(first, first + count):
            if i == 0:
                slots.append(0)
            elif i == 1:
                slots.append(jnp.where(s_me == 0, sp - 1, 1))
            else:
                slots.append(jnp.where(s_me == 0, i - 1, i))

        def store(h, k, v):
            k_ctx[h, first * ctx_rows : (first + count) * ctx_rows, :] = k
            v_ctx[h, first * ctx_rows : (first + count) * ctx_rows, :] = v

        expand([ctx[slot] for slot in slots], [ctx_rope[slot] for slot in slots], kgain, None, store)

    def tables(source, d, gain, gain_swap):
        start = pl.multiple_of((source * tp + (partner(tp, t_me, d) if d else t_me)) * rows, rows)
        return tab_a[pl.ds(start, rows), :] * gain, tab_b[pl.ds(start, rows), :] * gain_swap

    def stacked(pieces_of):
        return [jnp.concatenate(p, axis=0) for p in zip(*pieces_of)]

    def queries(mates):
        a, b = stacked([tables(s_me, d, qgain, qgain_swap) for d in mates])
        qx = jnp.dot(jnp.concatenate([q_lat[d] for d in mates], axis=0), qu_ref[...], preferred_element_type=F32)
        qx = [qx[:, h * LANES : (h + 1) * LANES] for h in range(heads)]
        squares = [jnp.sum(jnp.where(live, v * v, 0.0), axis=-1, keepdims=True) for v in qx]
        turned = [v * a + pltpu.roll(v, QK_DIM, 1) * b for v in qx]
        scales = [lax.rsqrt(square * (1.0 / QK_DIM) + EPS) * factor for square in squares]
        slot = (tp - 1 - mates[0]) * rows
        for h in range(heads):
            q_all[h, slot : slot + len(mates) * rows, :] = (turned[h] * scales[h]).astype(BF16)

    near = min(2, sp)
    near_keys = near * ctx_rows
    far_keys = (sp - near) * ctx_rows
    q_rows = 2 * rows if tp % 2 == 0 else rows

    def kv_relays(i):
        ds = source_step(i) if i else 0
        if relay:
            with jax.named_scope(f"relay{i}"):
                for k in range(2):
                    kv_mate(ds, 1 + k).wait_recv()
                    kv_relay(ds, k).start()

    def kv_forward(i):
        ds = source_step(i)
        with jax.named_scope(f"forward{i}"):
            kv_column(ds).wait_recv()
            for d in direct:
                kv_mate(ds, d).start()

    def w_relays(j):
        if relay:
            with jax.named_scope(f"wrelay{j}"):
                for k in range(2):
                    if j:
                        w_copy(1 + k, j).wait_recv()
                    w_relay(j, k).start()

    def z_start(d):
        if pair > 1:
            with jax.named_scope(f"zstart{d}"):
                if d not in direct:
                    w_arrive(d, 0)
                z_copy(d).start()

    def mate_rows(mates):
        return (tp - 1 - mates[0]) * rows, len(mates) * rows

    all_rows = [(start, q_rows) for start in range(0, group, q_rows)]

    def context_attend(mates):
        with jax.named_scope("ctxattend"):
            attend([mate_rows(mates)], k_ctx, v_ctx, 0, near_keys, True, True)

    def a_copy(d):
        return remote(att.at[d], held.at[d - 1], a_send.at[d - 1], a_recv.at[d - 1], mate(d))

    def finish(mates):
        for d in mates:
            slot = (tp - 1 - d) * rows
            outs = []
            for h in range(heads):
                total = acc_refs[h][slot : slot + rows, :]
                outs.append((total[:, :VALUE_DIM] / total[:, VALUE_DIM : VALUE_DIM + 1]).astype(BF16))
            att[d] = jnp.concatenate(outs, axis=1)
            if d:
                a_copy(d).start()

    order = [(i, 0) for i in range(sp)]
    if relay:
        order += [(i, d) for i in range(sp) for d in direct] + [(i, 3) for i in range(sp)]
    else:
        order += [(i, d) for i in range(1, sp) for d in direct] + [(0, d) for d in direct]
    chunks = [order[c : c + tp] for c in range(0, len(order), tp)]

    def chunk_keys(c):
        blocks = [(source_step(i) if i else 0, i, d) for i, d in chunks[c]]
        with jax.named_scope(f"kvwait{c}"):
            for ds, i, d in blocks:
                if relay and d == 3:
                    for k in range(2):
                        kv_relay(ds, k).wait_recv()
                elif d and not relay:
                    kv_mate(ds, d).wait_recv()
        with jax.named_scope("kvexpand"):
            a, b = stacked([tables(lax.rem(s_me + sp - ds, sp), d, kgain, kgain_swap) for ds, i, d in blocks])
            tails = [kv[ds, d, pl.ds(rows, ROPE_DIM // pieces), :] for ds, i, d in blocks]
            ropes = [
                jnp.concatenate([t[:, p * rows : (p + 1) * rows] for p in range(pieces)], axis=0) for t in tails
            ]

            def store(h, k, v):
                k_buf[h] = k
                v_buf[h] = v

            expand([kv[ds, d, pl.ds(0, rows), :] for ds, i, d in blocks], ropes, a, b, store)

    def chunk_attend():
        with jax.named_scope("attend"):
            attend(all_rows, k_buf, v_buf, 0, group, False, False)

    with jax.named_scope("queries"):
        queries([0])
    with jax.named_scope("ctxwait"):
        ctx_phase(2)
    with jax.named_scope("ctxexpand"):
        expand_context(0, near)
    context_attend([0])
    with jax.named_scope("qwait"):
        for d in direct:
            q_copy(d, (d - 1) % 2).wait_recv()
            if relay:
                q_relay(d - 1).start()
        for d in direct:
            kv_mate(0, d).start()
    with jax.named_scope("qwait2"):
        for d in direct:
            q_copy(d, d % 2).wait_recv()
    for d in direct:
        w_copy(d, 0).wait_recv()
    z_start(1)
    with jax.named_scope("queries"):
        queries(list(reversed(direct)))
    for i in range(1, min(2, sp)):
        kv_forward(i)
    context_attend(list(reversed(direct)))
    for i in range(2, min(3, sp)):
        kv_forward(i)
    if relay:
        with jax.named_scope("qwait3"):
            for k in range(2):
                q_relay(k).wait_recv()
        with jax.named_scope("queries"):
            queries([3])
        context_attend([3])
    for i in range(3, sp):
        kv_forward(i)
    kv_relays(0)
    w_relays(0)
    def swap_twin(d, j):
        for e in range(1, dp):
            x_copy(d, e, j).start()

    def swap_pair(d):
        if pair > 1:
            z_copy(d).wait_recv()
            swap_twin(d, len(mine))

    last = len(chunks) - 1
    relayed = [1]

    def relays_to(i):
        while relay and relayed[0] <= i:
            kv_relays(relayed[0])
            relayed[0] += 1

    for c in range(len(chunks)):
        if c:
            relays_to(sp - 1 if any(d == 3 for i, d in chunks[c]) else max(i for i, d in chunks[c]))
        if c == min(1, last):
            for j in range(1, len(mine)):
                for d in direct:
                    w_copy(d, j).start()
        if c == last:
            if far_keys:
                with jax.named_scope("ctxwait4"):
                    for k in range(4, sp + 1):
                        ctx_phase(k)
                with jax.named_scope("ctxexpand"):
                    expand_context(near, sp - near)
            for d in range(1, tp):
                if d not in direct:
                    z_start(d)
                    if pair > 1:
                        swap_twin(d, 0)
            if far_keys:
                with jax.named_scope("ctxattend"):
                    attend(all_rows, k_ctx, v_ctx, near_keys, far_keys, True, False)
            if relay:
                for j in range(1, len(mine)):
                    w_relays(j)
                    for d in direct:
                        swap_twin(d, j)
            with jax.named_scope("pair1"):
                swap_pair(1)
        chunk_keys(c)
        if c == last:
            with jax.named_scope("pair2"):
                for d in direct:
                    if d > 1:
                        swap_pair(d)
        if c == 0:
            with jax.named_scope("ctxwait3"):
                ctx_phase(3)
            for d in direct:
                if d > 1:
                    z_start(d)
        if c < last:
            chunk_attend()
        if c == min(1, last):
            relays_to(min(2, sp - 1))
            for i in range(len(others)):
                gate_copy(i).start()
            for d in range(1, tp):
                if d in direct:
                    swap_twin(d, 0)

    with jax.named_scope("attendlast"):
        turns = [list(range(tp - 1, 1, -1)), [1], [0]]
        attend(
            [mate_rows(mates) for mates in turns], k_buf, v_buf, 0, group, False, False,
            lambda i: finish(turns[i]),
        )

    with jax.named_scope("wtwin"):
        for d in range(1, tp):
            for j in range(len(mine)):
                if d not in direct:
                    if j or pair == 1:
                        w_arrive(d, j)
                        swap_twin(d, j)
                elif j and not relay:
                    w_arrive(d, j)
                    swap_twin(d, j)
            if d not in direct:
                swap_pair(d)

    with jax.named_scope("tail"):
        chunk = 512
        spans = [slice(n * chunk, (n + 1) * chunk) for n in range(width // chunk)]
        mixed = [
            jnp.dot(att[0], w_all[0, :, cols], preferred_element_type=F32).astype(BF16).astype(F32) for cols in spans
        ]
        for d in list(range(2, tp)) + [1]:
            with jax.named_scope("xwait"):
                for e in range(1, dp):
                    for j in range(3):
                        x_copy(d, e, j).wait_recv()
            with jax.named_scope("await"):
                a_copy(d).wait_recv()
            for n, cols in enumerate(spans):
                term = jnp.dot(held[d - 1], w_all[d, :, cols], preferred_element_type=F32)
                mixed[n] = mixed[n] + term.astype(BF16).astype(F32)
        all_gates().wait_recv()
        gate_buf[...] = joined(gathered(gates), 0)
        for n, cols in enumerate(spans):
            out_ref[:, cols] = (tokens_ref[:, cols].astype(F32) + gate_buf[:, cols] * mixed[n]).astype(BF16)

    with jax.named_scope("drain"):
        all_mods().wait_send()
        all_gates().wait_send()
        for k in range(1, sp):

            @pl.when((s_me >= k - 1) & (s_me < sp - 1))
            def _():
                for cp in ctx_up(k):
                    cp.wait_send()

            @pl.when((s_me + k - 1 <= sp - 1) & (s_me > 0))
            def _():
                for cp in ctx_down(k):
                    cp.wait_send()

        for d in direct:
            for k in range(2):
                q_copy(d, k).wait_send()
            for j in range(len(mine)):
                w_copy(d, j).wait_send()
            for ds in range(sp):
                kv_mate(ds, d).wait_send()
        if relay:
            for k in range(2):
                q_relay(k).wait_send()
                for j in range(len(mine)):
                    w_relay(j, k).wait_send()
                for ds in range(sp):
                    kv_relay(ds, k).wait_send()
        for d in range(1, tp):
            a_copy(d).wait_send()
            if pair > 1:
                z_copy(d).wait_send()
            for e in range(1, dp):
                for j in range(3):
                    x_copy(d, e, j).wait_send()
        for ds in range(1, sp):
            kv_column(ds).wait_send()


def local(
    sp, tp, dp,
    latent_tokens, condition, shift_weight, scale_weight, gate_weight, norm_gain,
    query_down, query_gain, kv_down, kv_gain, rope_down, query_up, key_up, value_up,
    query_norm_gain, key_norm_gain, out_weight, context_latent, context_rope, context_lift,
):
    rows, width = latent_tokens.shape
    q_rank = query_down.shape[1]
    rank = kv_down.shape[1]
    heads = query_up.shape[1] // QK_DIM
    ctx_rows = context_latent.shape[0]
    group = rows * tp
    tokens = group * sp
    context = sp * ctx_rows
    n_dev = sp * tp
    row_a, row_b = turn_tables(tokens // GRID_W, 0)
    col_a, col_b = turn_tables(GRID_W, 1)
    q_spread = jnp.asarray(query_spread(heads), BF16)
    k_spread = jnp.asarray(head_spread(heads, NOPE_DIM), BF16)
    v_spread = jnp.asarray(head_spread(heads, VALUE_DIM), BF16)
    dma = pltpu.SemaphoreType.DMA
    vmem = pltpu.VMEM
    return pl.pallas_call(
        functools.partial(fused_kernel, sp, tp, dp, heads),
        out_shape=pltpu.VMEM((rows, width), BF16),
        in_specs=[HBM_SPEC] * 28,
        out_specs=VMEM_SPEC,
        scratch_shapes=[
            vmem((n_dev, 2 * width // tp // LANES, LANES), F32),
            vmem((n_dev, width // tp // LANES, LANES), F32),
            vmem((tp, rows, q_rank), BF16),
            vmem((sp, tp, rows + ROPE_DIM * rows // rank, rank), BF16),
            vmem((sp, ctx_rows, rank), BF16),
            vmem((sp, ROPE_DIM, ctx_rows), BF16),
            vmem((1, width), F32),
            vmem((tokens, LANES), F32),
            vmem((tokens, LANES), F32),
            vmem((8 * ((heads + 9) // 8), LANES), F32),
            vmem((heads, group, LANES), BF16),
            vmem((heads, group, LANES), BF16),
            vmem((heads, group, LANES), BF16),
            vmem((heads, context, LANES), BF16),
            vmem((heads, context, LANES), BF16),
            vmem((tp, rows, heads * VALUE_DIM), BF16),
            vmem((tp - 1, rows, heads * VALUE_DIM), BF16),
            vmem((tp,) + out_weight.shape, BF16),
            vmem(shift_weight.shape, BF16),
            vmem(scale_weight.shape, BF16),
            vmem(gate_weight.shape, BF16),
            vmem(latent_tokens.shape, BF16),
            vmem(query_down.shape, BF16),
            vmem(kv_down.shape, BF16),
            vmem(rope_down.shape[::-1], BF16),
            vmem(query_up.shape, BF16),
            vmem(key_up.shape, BF16),
            vmem(value_up.shape, BF16),
            vmem(q_spread.shape, BF16),
            vmem(k_spread.shape, BF16),
            vmem(v_spread.shape, BF16),
            vmem((q_rank, heads * LANES), BF16),
            vmem((rank, heads * LANES), BF16),
            vmem((rank, heads * LANES), BF16),
            vmem((1, heads), F32),
            vmem(condition.shape, BF16),
            vmem((1, width), F32),
            vmem((1, q_rank), F32),
            vmem((1, rank), F32),
            vmem((1, QK_DIM), F32),
            vmem((1, QK_DIM), F32),
            vmem(row_a.shape, F32),
            vmem(row_a.shape, F32),
            vmem(col_a.shape, F32),
            vmem(col_a.shape, F32),
            vmem((ROPE_DIM, LANES), BF16),
            dma((28,)),
            dma((1,)), dma((1,)),
            dma((1,)), dma((1,)),
            dma((2 * tp,)), dma((2 * tp,)),
            dma((sp, tp + 1)), dma((sp, tp + 1)),
            dma((2, 2 * sp)), dma((2, sp)),
            dma((tp - 1, 4)), dma((tp - 1, 4)),
            dma((4, 2)), dma((4, 2)),
            dma((tp - 1,)), dma((tp - 1,)),
            dma(((tp - 1) * (dp - 1), 4)), dma(((tp - 1) * (dp - 1), 4)),
            dma((tp - 1,)), dma((tp - 1,)),
        ]
        + [vmem((group, LANES), F32)] * (2 * heads),
        compiler_params=pltpu.CompilerParams(
            collective_id=0, has_side_effects=True, vmem_limit_bytes=58 * 1024 * 1024
        ),
        name="fused",
    )(
        context_lift[None], condition, norm_gain[None], query_gain[None], kv_gain[None], query_norm_gain[None],
        key_norm_gain[None], jnp.asarray(row_a), jnp.asarray(row_b), jnp.asarray(col_a), jnp.asarray(col_b),
        jnp.asarray(rope_spread(), BF16),
        shift_weight, scale_weight, gate_weight, latent_tokens, query_down, kv_down, rope_down.T,
        context_latent, context_rope.T, query_up, key_up, value_up, q_spread, k_spread, v_spread, out_weight,
    )


def solution(mesh):
    in_specs = (
        P(("dp", "sp", "tp"), None), P(("dp", "sp")), P("sp", "tp"), P("sp", "tp"), P("sp", "tp"),
        P(), P(), P(), P(), P(), P(), P(None, "tp"), P(None, "tp"), P(None, "tp"), P(), P(),
        P("tp", None), P(("dp", "sp"), None), P(("dp", "sp"), None), P("tp"),
    )
    out_specs = P(("dp", "sp", "tp"), None)
    body = functools.partial(local, mesh.shape["sp"], mesh.shape["tp"], mesh.shape["dp"])
    return jax.shard_map(body, mesh=mesh, in_specs=in_specs, out_specs=out_specs, check_vma=False)
```
